32 devices in a mesh: sp: 8 (over z, x), tp: 4 (over y, core).
Axes of the slice: x: 2, y: 2, z: 4, core: 2. Of those that a mesh axis runs over, the one named last changes fastest.
Arguments:
- residual: bfloat16 [1024, 2048], P('sp'), may hold values from -6 to 6
- query_narrow: bfloat16 [1024, 1024], P('sp', 'tp'), may hold values from -6 to 6
- keys_narrow: bfloat16 [1024, 1024], P('sp', 'tp'), may hold values from -6 to 6
- values_narrow: bfloat16 [1024, 1024], P('sp', 'tp'), may hold values from -6 to 6
- outgate_narrow: bfloat16 [1024, 1024], P('sp', 'tp'), may hold values from -6 to 6
- gates_narrow: float32 [4, 8, 1024], P(None, 'tp', 'sp'), may hold values from -4 to 100
- query_broad: bfloat16 [1024, 1024], P('sp', 'tp'), may hold values from -6 to 6
- keys_broad: bfloat16 [1024, 1024], P('sp', 'tp'), may hold values from -6 to 6
- values_broad: bfloat16 [1024, 1024], P('sp', 'tp'), may hold values from -6 to 6
- outgate_broad: bfloat16 [1024, 1024], P('sp', 'tp'), may hold values from -6 to 6
- gates_broad: float32 [4, 4, 1024], P(None, 'tp', 'sp'), may hold values from -4 to 100
- outproj_narrow: bfloat16 [1024, 2048], P('tp'), may hold values from -0.125 to 0.125
- outproj_broad: bfloat16 [1024, 2048], P('tp'), may hold values from -0.125 to 0.125
- norm_gain: bfloat16 [2048], replicated, may hold values from 0.099609375 to 1.8984375
- gate_weight: bfloat16 [2048, 5632], P('sp', 'tp'), may hold values from -0.125 to 0.125
- up_weight: bfloat16 [2048, 5632], P('sp', 'tp'), may hold values from -0.125 to 0.125
- down_weight: bfloat16 [2048, 5632], P('sp', 'tp'), may hold values from -0.078125 to 0.078125
Outputs:
- layer_out: bfloat16 [1024, 2048], P(('sp', 'tp'))
The draws below stay inside these ranges and needn't reach their ends.
All inputs are finite; a program needn't handle non-finite values.
Results may differ from the reference program's by a relative error of at most 0.0085.
Values may be sent and summed in bfloat16 or wider, within the bound.
A program may use at most 192 MiB of HBM per device.

```python
import jax
import jax.numpy as jnp
from jax import lax

D = 2048
H_A = 8
DH_A = 128
H_B = 4
DH_B = 256
FF = 5632
TOK_DEV = 128
TOKENS = 1024
D_A = 1024
D_B = 1024
N_TP = 4


def gate_draw(key, number_of_heads):
    running_total = TOKENS
    every_key_row = jax.random.split(key, 9)
    in_gate = jnp.clip(jax.random.normal(every_key_row[0], (2, number_of_heads, running_total), jnp.float32), -4.0, 4.0)
    fast_share = 0.5
    fast = jax.random.uniform(every_key_row[4], (2, number_of_heads, 1)) < fast_share
    base_rate = jnp.where(fast, 1.0 / 40.0, 0.25 / running_total)
    block_count = running_total // TOK_DEV
    block_factor = jnp.exp(jax.random.uniform(every_key_row[5], (2, 1, block_count), jnp.float32, -0.7, 0.7))
    block_factor = jnp.repeat(block_factor, TOK_DEV, axis=2)
    rate = base_rate * block_factor * jnp.exp(0.5 * jax.random.normal(every_key_row[6], (2, number_of_heads, running_total), jnp.float32))
    forget_gate = -jnp.log(rate)
    spike_positions = jax.random.randint(every_key_row[7], (3,), 0, running_total)
    spike_flag = jnp.any(jnp.arange(running_total)[:, None] == spike_positions[None, :], axis=1)
    spike_magnitude = jax.random.uniform(every_key_row[8], (2, number_of_heads, running_total), jnp.float32, 0.0, 1.4)
    forget_gate = jnp.where(spike_flag[None, None, :], spike_magnitude, forget_gate)
    forget_gate = jnp.maximum(forget_gate, 0.0)
    return jnp.concatenate([in_gate, forget_gate], axis=0).astype(jnp.float32)


def draw_gates_narrow(key, part):
    return gate_draw(jax.random.fold_in(key, 11), H_A)


def draw_gates_broad(key, part):
    return gate_draw(jax.random.fold_in(key, 12), H_B)


def level_of(own_key, shape, shards, smallest, top_value):
    def one(axis_at, parts):
        heights = jax.random.uniform(jax.random.fold_in(jax.random.fold_in(own_key, 6), axis_at), (parts,), jnp.float32, smallest / len(shards), top_value / len(shards))
        return jnp.repeat(jnp.exp(heights), shape[axis_at] // parts).reshape((-1,) + (1,) * (len(shape) - axis_at - 1))

    level = one(*shards[0])
    for cut in shards[1:]:
        level = level * one(*cut)
    return level


def centred(key, shape, scale, most, cuts=(), kind=jnp.bfloat16):
    drawn = scale * jax.random.normal(key, shape, jnp.float32)
    if cuts:
        drawn = drawn * level_of(key, shape, cuts, -0.22, 0.18)
    return jnp.clip(drawn, -most, most).astype(kind)


def setup_inputs(seed: int = 0) -> dict:
    key_of = jax.random.split(jax.random.key(seed), 18)
    return {
        "residual": centred(key_of[0], (TOKENS, D), 1.0, 6.0, ((0, 8),)),
        "query_narrow": centred(key_of[1], (TOKENS, D_A), 1.0, 6.0, ((0, 8), (1, 4))),
        "keys_narrow": centred(key_of[2], (TOKENS, D_A), 1.0, 6.0, ((0, 8), (1, 4))),
        "values_narrow": centred(key_of[3], (TOKENS, D_A), 1.0, 6.0, ((0, 8), (1, 4))),
        "outgate_narrow": centred(key_of[4], (TOKENS, D_A), 1.0, 6.0, ((0, 8), (1, 4))),
        "gates_narrow": draw_gates_narrow(jax.random.fold_in(key_of[17], 71), 0),
        "query_broad": centred(key_of[6], (TOKENS, D_B), 1.0, 6.0, ((0, 8), (1, 4))),
        "keys_broad": centred(key_of[7], (TOKENS, D_B), 1.0, 6.0, ((0, 8), (1, 4))),
        "values_broad": centred(key_of[8], (TOKENS, D_B), 1.0, 6.0, ((0, 8), (1, 4))),
        "outgate_broad": centred(key_of[9], (TOKENS, D_B), 1.0, 6.0, ((0, 8), (1, 4))),
        "gates_broad": draw_gates_broad(jax.random.fold_in(key_of[17], 71), 0),
        "outproj_narrow": centred(key_of[11], (D_A, D), (D_A + D_B) ** -0.5, 0.125, ((0, 4),)),
        "outproj_broad": centred(key_of[12], (D_B, D), (D_A + D_B) ** -0.5, 0.125, ((0, 4),)),
        "norm_gain": jnp.clip(1.0 + 0.18 * jax.random.normal(key_of[13], (D,), jnp.float32), 0.099609375, 1.8984375).astype(jnp.bfloat16),
        "gate_weight": centred(key_of[14], (D, FF), D ** -0.5, 0.125, ((0, 8), (1, 4))),
        "up_weight": centred(key_of[15], (D, FF), D ** -0.5, 0.125, ((0, 8), (1, 4))),
        "down_weight": centred(key_of[16], (D, FF), FF ** -0.5, 0.078125, ((0, 8), (1, 4))),
    }


EPSILON = 1e-06
START_MAX = -1e+30

def rounded(values_in):
    return lax.optimization_barrier(values_in.astype(jnp.bfloat16)).astype(jnp.float32)

def empty_state(number_of_heads, head_width):
    return (jnp.zeros((number_of_heads, head_width, head_width), jnp.float32), jnp.zeros((number_of_heads, head_width), jnp.float32), jnp.full((number_of_heads,), START_MAX, jnp.float32), jnp.zeros((number_of_heads,), jnp.float32))

def combine(earlier_state, later_state):
    memory_early, normer_early, max_early, total_early = earlier_state
    memory_late, normer_late, max_late, total_late = later_state
    new_max = jnp.maximum(max_early + total_late, max_late)
    keep_early = jnp.exp(max_early + total_late - new_max)
    keep_late = jnp.exp(max_late - new_max)
    return (keep_early[:, None, None] * memory_early + keep_late[:, None, None] * memory_late, keep_early[:, None] * normer_early + keep_late[:, None] * normer_late, new_max, total_early + total_late)

def local_pass(query_rows, key_rows, value_rows, in_gate, log_forget):
    length = query_rows.shape[0]
    scaling = query_rows.shape[2] ** (-0.5)
    cumulative = jnp.cumsum(log_forget, axis=1)
    positions = jnp.arange(length)
    lower_tri = positions[:, None] >= positions[None, :]
    log_weight = jnp.where(lower_tri[None], cumulative[:, :, None] - cumulative[:, None, :] + in_gate[:, None, :], -jnp.inf)
    local_max = lax.optimization_barrier(jnp.max(log_weight, axis=2))
    query_float = query_rows.astype(jnp.float32)
    key_float = key_rows.astype(jnp.float32)
    value_float = value_rows.astype(jnp.float32)
    scores = jnp.einsum('thd,shd->hts', query_float, key_float) * scaling
    weighted = jnp.exp(log_weight - local_max[:, :, None]) * scores
    local_den = lax.optimization_barrier(jnp.sum(weighted, axis=2))
    local_num = jnp.einsum('hts,shd->thd', rounded(weighted), value_float)
    decay_total = cumulative[:, -1]
    toward_end = decay_total[:, None] - cumulative + in_gate
    end_max = lax.optimization_barrier(jnp.max(toward_end, axis=1))
    end_share = jnp.exp(toward_end - end_max[:, None])
    weighted_keys = jnp.transpose(end_share)[:, :, None] * key_float
    memory = jnp.einsum('shv,shk->hvk', value_float, rounded(weighted_keys))
    normer = lax.optimization_barrier(jnp.sum(weighted_keys, axis=0))
    return ((local_num, local_den, local_max, cumulative), (memory, normer, end_max, decay_total))

def finish(local, query_rows, carried):
    local_num, local_den, local_max, cumulative = local
    memory, normer, start_max, decay_total = carried
    scaling = query_rows.shape[2] ** (-0.5)
    query_float = query_rows.astype(jnp.float32)
    reach = cumulative + start_max[:, None]
    new_max = jnp.maximum(local_max, reach)
    own_scale = jnp.transpose(jnp.exp(local_max - new_max))
    past_scale = jnp.transpose(jnp.exp(reach - new_max)) * scaling
    from_memory = jnp.einsum('thk,hvk->thv', query_float, memory, precision=lax.Precision.HIGHEST)
    from_normer = jnp.einsum('thk,hk->th', query_float, normer, precision=lax.Precision.HIGHEST)
    numerator = own_scale[:, :, None] * local_num + past_scale[:, :, None] * from_memory
    denominator = own_scale * jnp.transpose(local_den) + past_scale * from_normer
    return numerator / jnp.maximum(jnp.abs(denominator), 1.0)[:, :, None]

def direction_outputs(query_rows, key_rows, value_rows, in_gate, log_forget):
    count = query_rows.shape[0] // TOK_DEV
    number_of_heads = query_rows.shape[1]
    head_width = query_rows.shape[2]

    def blocks(packed):
        return packed.reshape((count, TOK_DEV) + packed.shape[1:])

    def gate_blocks(packed):
        return jnp.moveaxis(packed.reshape(number_of_heads, count, TOK_DEV), 1, 0)

    def block_step(carried, block_inputs):
        queries, key_block, value_block, gate_block, forget_block = block_inputs
        local, summary = local_pass(queries, key_block, value_block, gate_block, forget_block)
        return (combine(carried, summary), finish(local, queries, carried))
    inputs = (blocks(query_rows), blocks(key_rows), blocks(value_rows), gate_blocks(in_gate), gate_blocks(log_forget))
    final_state, outputs = lax.scan(block_step, empty_state(number_of_heads, head_width), inputs)
    return outputs.reshape(query_rows.shape)

def group_cell(query_all, every_key_row, values_all, outgate_all, gate_pre, head_width):
    token_count = query_all.shape[0]
    queries = query_all.reshape(token_count, -1, head_width)
    key_rows = every_key_row.reshape(token_count, -1, head_width)
    value_rows = values_all.reshape(token_count, -1, head_width)
    forward_out = direction_outputs(queries, key_rows, value_rows, gate_pre[0], jax.nn.log_sigmoid(gate_pre[2]))
    backward_out = direction_outputs(queries[::-1], key_rows[::-1], value_rows[::-1], gate_pre[1][:, ::-1], jax.nn.log_sigmoid(gate_pre[3])[:, ::-1])[::-1]
    summed = forward_out + backward_out
    normed = summed * lax.rsqrt(lax.optimization_barrier(jnp.mean(summed * summed, axis=2, keepdims=True)) + EPSILON)
    return (normed.reshape(token_count, -1) * jax.nn.sigmoid(outgate_all.astype(jnp.float32))).astype(jnp.bfloat16)

def reference(residual, query_narrow, keys_narrow, values_narrow, outgate_narrow, gates_narrow, query_broad, keys_broad, values_broad, outgate_broad, gates_broad, outproj_narrow, outproj_broad, norm_gain, gate_weight, up_weight, down_weight):
    cell_narrow = group_cell(query_narrow, keys_narrow, values_narrow, outgate_narrow, gates_narrow, DH_A)
    cell_broad = group_cell(query_broad, keys_broad, values_broad, outgate_broad, gates_broad, DH_B)
    narrow_part = cell_narrow.shape[1] // N_TP
    broad_part = cell_broad.shape[1] // N_TP
    hidden_part = gate_weight.shape[1] // N_TP
    proj = jnp.zeros(residual.shape, jnp.float32)
    for member in range(N_TP):
        narrow_cols = slice(member * narrow_part, (member + 1) * narrow_part)
        broad_cols = slice(member * broad_part, (member + 1) * broad_part)
        partial_value = jnp.dot(cell_narrow[:, narrow_cols], outproj_narrow[narrow_cols], preferred_element_type=jnp.float32)
        partial_value = partial_value + jnp.dot(cell_broad[:, broad_cols], outproj_broad[broad_cols], preferred_element_type=jnp.float32)
        proj = proj + rounded(partial_value)
    stream = residual.astype(jnp.float32) + proj
    scaled = stream * lax.rsqrt(lax.optimization_barrier(jnp.mean(stream * stream, axis=1, keepdims=True)) + EPSILON)
    normed = (scaled * norm_gain.astype(jnp.float32)).astype(jnp.bfloat16)
    ffn = jnp.zeros(residual.shape, jnp.float32)
    for member in range(N_TP):
        hidden_cols = slice(member * hidden_part, (member + 1) * hidden_part)
        gate = jnp.dot(normed, gate_weight[:, hidden_cols], preferred_element_type=jnp.float32)
        upward = jnp.dot(normed, up_weight[:, hidden_cols], preferred_element_type=jnp.float32)
        hidden = (jax.nn.silu(gate) * upward).astype(jnp.bfloat16)
        partial_value = lax.dot_general(hidden, down_weight[:, hidden_cols], (((1,), (1,)), ((), ())), preferred_element_type=jnp.float32)
        ffn = ffn + rounded(partial_value)
    return (stream + 0.5 * ffn).astype(jnp.bfloat16)
```

```python
import functools

import jax
import jax.numpy as jnp
from jax import lax
from jax.experimental import pallas as pl
from jax.experimental.pallas import tpu as pltpu
from jax.sharding import PartitionSpec as P

DH_A = 128
DH_B = 256

EPSILON = 1e-06
FAR = -1e30
LATE = 1
SHARED = 1
MESH = pl.DeviceIdType.MESH


def direction_columns(in_gate, log_forget, reverse):
    place, length = lax.axis_index("sp"), lax.axis_size("sp")
    cumulative = lax.cumsum(log_forget, axis=1, reverse=reverse)
    total = cumulative[:, 0] if reverse else cumulative[:, -1]
    toward_end = total[:, None] - cumulative + in_gate
    packed = jnp.concatenate([toward_end, total[:, None]], axis=1)
    every = lax.all_gather(packed, "sp")
    ends, totals = every[:, :, :-1], every[:, :, -1]
    index = jnp.arange(length)
    if reverse:
        between = (index[None, :] > place) & (index[None, :] < index[:, None])
        valid = index > place
    else:
        between = (index[None, :] < place) & (index[None, :] > index[:, None])
        valid = index < place
    offset = jnp.sum(jnp.where(between[:, :, None], totals[None], 0.0), axis=1)
    columns = jnp.where(valid[:, None, None], offset[:, :, None] + ends, FAR)
    own = (in_gate - cumulative)[None]
    columns = jnp.where((index == place)[:, None, None], own, columns)
    return jnp.moveaxis(columns, 0, 1).reshape(in_gate.shape[0], -1)


def group_cell(query, keys, values, outgate, gates, width):
    rows, every = query.shape[0], keys.shape[0]
    place = lax.axis_index("sp")
    heads = query.shape[1] // width
    q = query.reshape(rows, heads, width)
    k = keys.reshape(every, heads, width)
    v = values.reshape(every, heads, width)
    scores = jnp.einsum("thd,shd->hts", q, k, preferred_element_type=jnp.float32) * width ** (-0.5)
    t_at = (place * rows + jnp.arange(rows))[:, None]
    s_at = jnp.arange(every)[None, :]
    summed = 0.0
    for direction in range(2):
        columns = direction_columns(
            gates[direction], jax.nn.log_sigmoid(gates[2 + direction]), direction == 1
        )
        mask = s_at >= t_at if direction else s_at <= t_at
        log_weight = jnp.where(mask[None], columns[:, None, :], FAR)
        top = jnp.max(log_weight, axis=2, keepdims=True)
        weighted = jnp.exp(log_weight - top) * scores
        den = jnp.sum(weighted, axis=2)
        num = jnp.einsum(
            "hts,shd->thd", weighted.astype(jnp.bfloat16), v, preferred_element_type=jnp.float32
        )
        summed = summed + num / jnp.maximum(jnp.abs(jnp.transpose(den)), 1.0)[:, :, None]
    normed = summed * lax.rsqrt(jnp.mean(summed * summed, axis=2, keepdims=True) + EPSILON)
    return (normed.reshape(rows, -1) * jax.nn.sigmoid(outgate.astype(jnp.float32))).astype(
        jnp.bfloat16
    )


def shards(
    residual,
    query_narrow,
    keys_narrow,
    values_narrow,
    outgate_narrow,
    gates_narrow,
    query_broad,
    keys_broad,
    values_broad,
    outgate_broad,
    gates_broad,
    outproj_narrow,
    outproj_broad,
    norm_gain,
    gate_weight,
    up_weight,
    down_weight,
):
    spread = lax.axis_size("sp")
    channels, hidden_own = gate_weight.shape
    stacked = jnp.stack([gate_weight.T, up_weight.T, down_weight.T])
    pieces = stacked.reshape(3, spread, hidden_own // spread, channels)
    pieces = lax.all_to_all(pieces, "sp", split_axis=1, concat_axis=1)
    weights = jnp.swapaxes(pieces, 1, 2).reshape(3, hidden_own // spread, -1)

    narrow, broad = keys_narrow.shape[1], keys_broad.shape[1]
    memory = lax.all_gather(
        jnp.concatenate([keys_narrow, values_narrow, keys_broad, values_broad], axis=1),
        "sp",
        axis=0,
        tiled=True,
    )
    kn, vn = memory[:, :narrow], memory[:, narrow : 2 * narrow]
    kb, vb = memory[:, 2 * narrow : 2 * narrow + broad], memory[:, 2 * narrow + broad :]
    cell_narrow = group_cell(query_narrow, kn, vn, outgate_narrow, gates_narrow, DH_A)
    cell_broad = group_cell(query_broad, kb, vb, outgate_broad, gates_broad, DH_B)

    own_count = residual.shape[0] // lax.axis_size("tp")
    proj = lax.psum_scatter(
        (
            jnp.dot(cell_narrow, outproj_narrow, preferred_element_type=jnp.float32)
            + jnp.dot(cell_broad, outproj_broad, preferred_element_type=jnp.float32)
        ).astype(jnp.bfloat16),
        "tp",
        scatter_dimension=0,
        tiled=True,
    ).astype(jnp.float32)
    offset = lax.axis_index("tp") * own_count
    stream = lax.dynamic_slice_in_dim(residual, offset, own_count, 0).astype(jnp.float32) + proj
    scaled = stream * lax.rsqrt(jnp.mean(stream * stream, axis=1, keepdims=True) + EPSILON)
    normed = (scaled * norm_gain.astype(jnp.float32)).astype(jnp.bfloat16)
    normed = lax.all_gather(normed, ("sp", "tp"), axis=0, tiled=True)
    nt = (((1,), (1,)), ((), ()))
    gate = lax.dot_general(normed, weights[0], nt, preferred_element_type=jnp.float32)
    upward = lax.dot_general(normed, weights[1], nt, preferred_element_type=jnp.float32)
    hidden = (jax.nn.silu(gate) * upward).astype(jnp.bfloat16)
    partial_value = jnp.dot(hidden, weights[2], preferred_element_type=jnp.float32)
    ffn = lax.psum_scatter(
        partial_value.astype(jnp.bfloat16), ("sp", "tp"), scatter_dimension=0, tiled=True
    ).astype(jnp.float32)
    return (stream + 0.5 * ffn).astype(jnp.bfloat16)


def fused_kernel(geometry, *refs):
    spread, members, wide, narrow_heads, broad_heads = geometry
    (res, qn, kn, vn, on, gn, qb, kb, vb, ob, gb, opn, opb, gain, gw, uw, dw, out) = refs[:18]
    (kv_all, info, gates, wt, w_all, pp, rs, x_all, part, r1, s2, r3) = refs[18:30]
    (kv_send, kv_recv, in_send, in_recv, w_send, w_recv, f_send, f_recv, g_send, g_recv) = refs[30:40]
    (p_send, p_recv, x_send, x_recv, e_send, e_recv, z_send, z_recv) = refs[40:48]
    rows = res.shape[0]
    own = rows // members
    depth = spread // 2
    chan, hid = gw.shape
    piece = hid // spread
    ca, cb = kn.shape[1], kb.shape[1]
    i, j = lax.axis_index("sp"), lax.axis_index("tp")
    z, x = i // 2, i % 2
    y, c = j // 2, j % 2
    ox = 1 - x
    f32, bf16 = jnp.float32, jnp.bfloat16
    sibling, x_peer = (i, j + 1 - 2 * c), (2 * z + ox, j)
    across = (1 - y) * 2 + c
    y_peer = (i, across)

    def ranked(n):
        pick = 0
        for a in range(depth):
            others = sorted(
                (b for b in range(depth) if b != a),
                key=lambda b: (abs(a - b), (a < depth // 2) == (b < depth // 2)),
            )
            pick = pick + jnp.where(z == a, others[n], 0)
        return pick

    def send(src, dst, s_sem, r_sem, to):
        copy = pltpu.make_async_remote_copy(
            src_ref=src, dst_ref=dst, send_sem=s_sem, recv_sem=r_sem, device_id=to, device_id_type=MESH
        )
        copy.start()
        return copy

    def arrived(ref, sem):
        pltpu.make_async_remote_copy(
            src_ref=ref, dst_ref=ref, send_sem=sem, recv_sem=sem, device_id=(i, j), device_id_type=MESH
        ).wait_recv()

    def sent(ref, sem, cond=None):
        def wait():
            pltpu.make_async_remote_copy(
                src_ref=ref, dst_ref=ref, send_sem=sem, recv_sem=sem, device_id=(i, j), device_id_type=MESH
            ).wait_send()

        if cond is None:
            wait()
        else:
            pl.when(cond)(wait)

    barrier = pltpu.get_barrier_semaphore()
    for k in range(1, spread):
        pl.semaphore_signal(barrier, inc=1, device_id=((i + k) % spread, j), device_id_type=MESH)
    for k in range(1, members):
        pl.semaphore_signal(barrier, inc=1, device_id=(i, (j + k) % members), device_id_type=MESH)

    kv_all[i, :, 0:ca] = kn[...]
    kv_all[i, :, ca : 2 * ca] = vn[...]
    kv_all[i, :, 2 * ca : 2 * ca + cb] = kb[...]
    kv_all[i, :, 2 * ca + cb : 2 * ca + 2 * cb] = vb[...]
    gates[...] = jnp.zeros_like(gates)
    for role in range(4):
        at = 8 * (role % 2)
        gates[role // 2, at : at + narrow_heads, :] = gn[role]
        gates[role // 2, at + narrow_heads : at + narrow_heads + broad_heads, :] = gb[role]
    in_gate, pre = gates[0], gates[1]
    forget = jnp.minimum(pre, 0.0) - jnp.log1p(jnp.exp(-jnp.abs(pre)))
    r_at = lax.broadcasted_iota(jnp.int32, (rows, rows), 0)
    c_at = lax.broadcasted_iota(jnp.int32, (rows, rows), 1)
    run = lambda m: jnp.dot(
        forget, m.astype(f32), preferred_element_type=f32, precision=lax.Precision.HIGHEST
    )
    forward_row = lax.broadcasted_iota(jnp.int32, in_gate.shape, 0) < 8
    cumulative = jnp.where(forward_row, run(r_at <= c_at), run(r_at >= c_at))
    total = jnp.where(
        forward_row,
        jnp.broadcast_to(cumulative[:, rows - 1 : rows], in_gate.shape),
        jnp.broadcast_to(cumulative[:, 0:1], in_gate.shape),
    )
    own_column = in_gate - cumulative
    info[i, 0] = total + own_column
    info[i, 1] = total
    pl.semaphore_wait(barrier, spread + members - 2)

    def pass_kv(slot, way, to):
        send(kv_all.at[slot], kv_all.at[slot], kv_send.at[way, slot], kv_recv.at[slot], to)
        send(info.at[slot], info.at[slot], in_send.at[way, slot], in_recv.at[slot], to)

    def kv_arrived(slot):
        arrived(kv_all.at[slot], kv_recv.at[slot])
        arrived(info.at[slot], in_recv.at[slot])

    @pl.when(z + 1 < depth)
    def _():
        pass_kv(i, 0, (i + 2, j))

    @pl.when(z >= 1)
    def _():
        pass_kv(i, 1, (i - 2, j))

    pass_kv(i, 2, (2 * z + ox, j))

    for m, ref in enumerate((gw, uw, dw)):
        for k in range(hid // 128):
            wt[m, k * 128 : (k + 1) * 128, :] = ref[:, k * 128 : (k + 1) * 128].T
    mine = pl.ds(pl.multiple_of(i * piece, 16), piece)

    def w_slot(jj, p):
        return w_all.at[:, jj, :, pl.ds(pl.multiple_of(p * chan, 128), chan)]

    def send_weights(p):
        theirs = pl.ds(pl.multiple_of(p * piece, 16), piece)
        send(wt.at[:, theirs, :], w_slot(j, i), w_send.at[p], w_recv.at[i], (p, j))

    def share_weights(p):
        slot = w_slot(j, p)
        arrived(slot, w_recv.at[p])
        send(slot, slot, f_send.at[0, p], f_recv.at[0, p], sibling)
        send(slot, slot, g_send.at[p], g_recv.at[p], y_peer)

    def share_across(p):
        slot = w_slot(across, p)
        arrived(slot, g_recv.at[p])
        send(slot, slot, f_send.at[1, p], f_recv.at[1, p], sibling)

    columns = pl.ds(pl.multiple_of(i * chan, 128), chan)
    block = wt.at[:, mine, :]
    send(block, w_slot(j, i), g_send.at[i], g_recv.at[i], y_peer)
    send(block, w_slot(j, i), f_send.at[0, i], f_recv.at[0, i], sibling)
    w_all[:, j, :, columns] = wt[:, mine, :]
    for s in range(1, depth):

        @pl.when(z - s >= 0)
        def _():
            slot = i - 2 * s
            kv_arrived(slot)

            @pl.when(z + 1 < depth)
            def _():
                pass_kv(slot, 0, (i + 2, j))

            pass_kv(slot, 2, (2 * z + ox, j))

        @pl.when(z + s < depth)
        def _():
            slot = i + 2 * s
            kv_arrived(slot)

            @pl.when(z >= 1)
            def _():
                pass_kv(slot, 1, (i - 2, j))

            pass_kv(slot, 2, (2 * z + ox, j))

    straight = [2 * ranked(n) + x for n in range(depth - 1)]
    crossed = [2 * z + ox] + [2 * ranked(n) + ox for n in range(depth - 1)]
    middle = jnp.logical_or(z == depth // 2 - 1, z == depth // 2)

    @pl.when(middle)
    def _():
        send_weights(straight[0])

    def kv_sent(slot, way, cond=None):
        sent(kv_all.at[slot], kv_send.at[way, slot], cond)
        sent(info.at[slot], in_send.at[way, slot], cond)

    for zz in range(depth):
        kv_sent(2 * zz + x, 0, jnp.logical_and(zz <= z, z + 1 < depth))
        kv_sent(2 * zz + x, 1, jnp.logical_and(zz >= z, z >= 1))

    @pl.when(jnp.logical_not(middle))
    def _():
        send_weights(straight[0])

    for p in straight[1:]:
        send_weights(p)
    for zz in range(depth):
        kv_arrived(2 * zz + ox)
    for p in crossed[:LATE]:
        send_weights(p)

    offset = jnp.zeros_like(total)
    pieces = [None] * spread
    forward_sum = jnp.zeros_like(total)
    ahead = [None] * spread
    for k in reversed(range(spread)):
        ahead[k] = forward_sum
        forward_sum = forward_sum + jnp.where(k < i, info[k, 1], 0.0)
    backward_sum = jnp.zeros_like(total)
    for k in range(spread):
        reach = jnp.where(forward_row, ahead[k], backward_sum) + info[k, 0]
        seen = jnp.logical_or(
            jnp.logical_and(forward_row, k < i), jnp.logical_and(jnp.logical_not(forward_row), k > i)
        )
        pieces[k] = jnp.where(k == i, own_column, jnp.where(seen, reach, FAR))
        backward_sum = backward_sum + jnp.where(k > i, info[k, 1], 0.0)
    column = jnp.concatenate(pieces, axis=1)
    t_at = lax.broadcasted_iota(jnp.int32, (rows, spread * rows), 0) + i * rows
    s_at = lax.broadcasted_iota(jnp.int32, (rows, spread * rows), 1)
    masks = (s_at <= t_at, s_at >= t_at)
    nt = (((1,), (1,)), ((), ()))
    proj = jnp.zeros((rows, res.shape[1]), f32)
    heads = [(qn, on, opn, 0, ca, h, ca // narrow_heads, h) for h in range(narrow_heads)]
    heads += [
        (qb, ob, opb, 2 * ca, cb, h, cb // broad_heads, narrow_heads + h) for h in range(broad_heads)
    ]
    for query, outgate, outproj, base, group, h, width, row in heads:
        lanes = slice(h * width, (h + 1) * width)
        keys = kv_all[:, :, base + h * width : base + (h + 1) * width].reshape(spread * rows, width)
        vals = kv_all[:, :, base + group + h * width : base + group + (h + 1) * width].reshape(
            spread * rows, width
        )
        scores = lax.dot_general(query[:, lanes], keys, nt, preferred_element_type=f32) * width ** (-0.5)
        summed = jnp.zeros((rows, width), f32)
        for direction in range(2):
            at = 8 * direction + row
            weight = jnp.where(
                masks[direction],
                jnp.broadcast_to(column[at : at + 1, :], scores.shape),
                FAR,
            )
            top = jnp.max(weight, axis=1, keepdims=True)
            p = jnp.exp(weight - top) * scores
            den = jnp.sum(p, axis=1, keepdims=True)
            num = jnp.dot(p.astype(bf16), vals, preferred_element_type=f32)
            summed = summed + num / jnp.maximum(jnp.abs(den), 1.0)
        normed = summed * lax.rsqrt(jnp.mean(summed * summed, axis=1, keepdims=True) + EPSILON)
        opened = 1.0 / (1.0 + jnp.exp(-outgate[:, lanes].astype(f32)))
        cell = (normed * opened).astype(bf16)
        proj = proj + jnp.dot(cell, outproj[lanes, :], preferred_element_type=f32)
    pp[...] = proj.astype(bf16).reshape(pp.shape)

    for k in range(1, members):
        q = (j + k) % members
        send(pp.at[q], rs.at[j], p_send.at[q], p_recv.at[j], (i, q))
    for p in straight[:SHARED]:
        share_weights(p)
    stream = res[pl.ds(pl.multiple_of(j * own, own), own), :].astype(f32) + pp[j].astype(f32)
    for k in range(1, members):
        q = (j + k) % members
        arrived(rs.at[q], p_recv.at[q])
        stream = stream + rs[q].astype(f32)
    scaled = stream * lax.rsqrt(jnp.mean(stream * stream, axis=1, keepdims=True) + EPSILON)
    x_all[x, z] = (scaled * gain[...].astype(f32).reshape(1, wide)).astype(bf16)

    def pass_x(zz, way, to):
        slot = x_all.at[x, zz]
        send(slot, slot, x_send.at[way, zz], x_recv.at[x, zz], to)

    def x_arrived(xx, zz):
        arrived(x_all.at[xx, zz], x_recv.at[xx, zz])

    @pl.when(z + 1 < depth)
    def _():
        pass_x(z, 0, (i + 2, j))

    @pl.when(z >= 1)
    def _():
        pass_x(z, 1, (i - 2, j))

    pass_x(z, 2, x_peer)
    for p in crossed[LATE:]:
        send_weights(p)
    for s in range(1, depth):

        @pl.when(z - s >= 0)
        def _():
            x_arrived(x, z - s)

            @pl.when(z + 1 < depth)
            def _():
                pass_x(z - s, 0, (i + 2, j))

            pass_x(z - s, 2, x_peer)

        @pl.when(z + s < depth)
        def _():
            x_arrived(x, z + s)

            @pl.when(z >= 1)
            def _():
                pass_x(z + s, 1, (i - 2, j))

            pass_x(z + s, 2, x_peer)

    for p in straight[SHARED:] + crossed:
        share_weights(p)
    for p in [i] + straight + crossed:
        share_across(p)
    for zz in range(depth):
        x_arrived(ox, zz)
    other, other_across = 2 * y + 1 - c, 2 * (1 - y) + 1 - c
    for p in [i] + straight + crossed:
        arrived(w_slot(other, p), f_recv.at[0, p])
        arrived(w_slot(other_across, p), f_recv.at[1, p])

    units = members * piece

    def chunk(xx):
        a = x_all[xx].reshape(depth * own, -1)
        gate = lax.dot_general(a, w_all[0].reshape(units, -1), nt, preferred_element_type=f32)
        up = lax.dot_general(a, w_all[1].reshape(units, -1), nt, preferred_element_type=f32)
        hidden = (gate / (1.0 + jnp.exp(-gate)) * up).astype(bf16)
        got = jnp.dot(hidden, w_all[2].reshape(units, -1), preferred_element_type=f32)
        part[xx] = got.astype(bf16).reshape(depth, own, -1)

    ends = [(z + depth // 2) % depth] + [(z + k) % depth for k in range(1, depth) if 2 * k != depth]
    chunk(ox)
    for zz in ends + [z]:
        send(part.at[ox, zz], r1.at[zz], e_send.at[zz], e_recv.at[zz], x_peer)
    chunk(x)
    for zz in ends:
        arrived(r1.at[zz], e_recv.at[zz])
        s2[zz] = (part[x, zz].astype(f32) + r1[zz].astype(f32)).astype(bf16)
        send(s2.at[zz], r3.at[z], z_send.at[zz], z_recv.at[z], (2 * zz + x, j))
    arrived(r1.at[z], e_recv.at[z])
    ffn = part[x, z].astype(f32) + r1[z].astype(f32)
    for zz in ends:
        arrived(r3.at[zz], z_recv.at[zz])
        ffn = ffn + r3[zz].astype(f32)
    out[...] = (stream + 0.5 * ffn).astype(out.dtype)

    for zz in range(depth):
        kv_sent(2 * zz + x, 2)
        slot = x_all.at[x, zz]
        sent(slot, x_send.at[0, zz], jnp.logical_and(zz <= z, z + 1 < depth))
        sent(slot, x_send.at[1, zz], jnp.logical_and(zz >= z, z >= 1))
        sent(slot, x_send.at[2, zz])
        sent(r1.at[0], e_send.at[zz])
    for p in straight + crossed:
        sent(block, w_send.at[p])
    for p in range(spread):
        sent(block, f_send.at[0, p])
        sent(block, f_send.at[1, p])
        sent(block, g_send.at[p])
    for k in range(1, members):
        sent(rs.at[0], p_send.at[(j + k) % members])
    for zz in ends:
        sent(s2.at[0], z_send.at[zz])


def fused_shards(*args):
    (res, qn, kn, vn, on, gn, qb, kb, vb, ob, gb, opn, opb, gain, gw, uw, dw) = args
    spread, members = lax.axis_size("sp"), lax.axis_size("tp")
    rows, wide = res.shape
    own, depth = rows // members, spread // 2
    chan, hid = gw.shape
    piece = hid // spread
    kvw = 2 * (kn.shape[1] + kb.shape[1])
    bf16, f32 = jnp.bfloat16, jnp.float32
    v = pltpu.VMEM
    dma = pltpu.SemaphoreType.DMA
    scratch = [
        v((spread, rows, kvw), bf16),
        v((spread, 2, 16, rows), f32),
        v((2, 16, rows), f32),
        v((3, hid, chan), bf16),
        v((3, members, piece, wide), bf16),
        v((members, own, wide), bf16),
        v((members, own, wide), bf16),
        v((2, depth, own, wide), bf16),
        v((2, depth, own, wide), bf16),
        v((depth, own, wide), bf16),
        v((depth, own, wide), bf16),
        v((depth, own, wide), bf16),
        dma((3, spread)),
        dma((spread,)),
        dma((3, spread)),
        dma((spread,)),
        dma((spread,)),
        dma((spread,)),
        dma((2, spread)),
        dma((2, spread)),
        dma((spread,)),
        dma((spread,)),
        dma((members,)),
        dma((members,)),
        dma((3, depth)),
        dma((2, depth)),
        dma((depth,)),
        dma((depth,)),
        dma((depth,)),
        dma((depth,)),
    ]
    geometry = (spread, members, wide, gn.shape[1], gb.shape[1])
    return pl.pallas_call(
        functools.partial(fused_kernel, geometry),
        out_shape=jax.ShapeDtypeStruct((own, wide), bf16),
        in_specs=[pl.BlockSpec(memory_space=pltpu.VMEM)] * 17,
        out_specs=pl.BlockSpec(memory_space=pltpu.VMEM),
        scratch_shapes=scratch,
        compiler_params=pltpu.CompilerParams(
            collective_id=0, has_side_effects=True, vmem_limit_bytes=60 * 1024 * 1024
        ),
        name="fused",
    )(res, qn, kn, vn, on, gn, qb, kb, vb, ob, gb, opn, opb, gain, gw, uw, dw)


def pick(*args):
    res, kn, gn, gb, gw = args[0], args[2], args[5], args[10], args[14]
    spread, members = lax.axis_size("sp"), lax.axis_size("tp")
    rows = res.shape[0]
    chan, hid = gw.shape
    fits = (
        spread % 2 == 0
        and spread >= 4
        and members == 4
        and rows == 128
        and spread * rows <= 2048
        and chan % 128 == 0
        and hid % (16 * spread) == 0
        and hid % 128 == 0
        and gn.shape[1] + gb.shape[1] <= 8
    )
    return fused_shards(*args) if fits else shards(*args)


def solution(mesh):
    in_specs = (
        P("sp", None),
        P("sp", "tp"),
        P("sp", "tp"),
        P("sp", "tp"),
        P("sp", "tp"),
        P(None, "tp", "sp"),
        P("sp", "tp"),
        P("sp", "tp"),
        P("sp", "tp"),
        P("sp", "tp"),
        P(None, "tp", "sp"),
        P("tp", None),
        P("tp", None),
        P(),
        P("sp", "tp"),
        P("sp", "tp"),
        P("sp", "tp"),
    )
    out_specs = P(("sp", "tp"), None)
    return jax.shard_map(pick, mesh=mesh, in_specs=in_specs, out_specs=out_specs, check_vma=False)
```

```python
import functools

import jax
import jax.numpy as jnp
from jax import lax
from jax.experimental import pallas as pl
from jax.experimental.pallas import tpu as pltpu
from jax.sharding import PartitionSpec as P

DH_A = 128
DH_B = 256

EPSILON = 1e-06
FAR = -1e30
MESH = pl.DeviceIdType.MESH


def direction_columns(in_gate, log_forget, reverse):
    place, length = lax.axis_index("sp"), lax.axis_size("sp")
    cumulative = lax.cumsum(log_forget, axis=1, reverse=reverse)
    total = cumulative[:, 0] if reverse else cumulative[:, -1]
    toward_end = total[:, None] - cumulative + in_gate
    packed = jnp.concatenate([toward_end, total[:, None]], axis=1)
    every = lax.all_gather(packed, "sp")
    ends, totals = every[:, :, :-1], every[:, :, -1]
    index = jnp.arange(length)
    if reverse:
        between = (index[None, :] > place) & (index[None, :] < index[:, None])
        valid = index > place
    else:
        between = (index[None, :] < place) & (index[None, :] > index[:, None])
        valid = index < place
    offset = jnp.sum(jnp.where(between[:, :, None], totals[None], 0.0), axis=1)
    columns = jnp.where(valid[:, None, None], offset[:, :, None] + ends, FAR)
    own = (in_gate - cumulative)[None]
    columns = jnp.where((index == place)[:, None, None], own, columns)
    return jnp.moveaxis(columns, 0, 1).reshape(in_gate.shape[0], -1)


def group_cell(query, keys, values, outgate, gates, width):
    rows, every = query.shape[0], keys.shape[0]
    place = lax.axis_index("sp")
    heads = query.shape[1] // width
    q = query.reshape(rows, heads, width)
    k = keys.reshape(every, heads, width)
    v = values.reshape(every, heads, width)
    scores = jnp.einsum("thd,shd->hts", q, k, preferred_element_type=jnp.float32) * width ** (-0.5)
    t_at = (place * rows + jnp.arange(rows))[:, None]
    s_at = jnp.arange(every)[None, :]
    summed = 0.0
    for direction in range(2):
        columns = direction_columns(
            gates[direction], jax.nn.log_sigmoid(gates[2 + direction]), direction == 1
        )
        mask = s_at >= t_at if direction else s_at <= t_at
        log_weight = jnp.where(mask[None], columns[:, None, :], FAR)
        top = jnp.max(log_weight, axis=2, keepdims=True)
        weighted = jnp.exp(log_weight - top) * scores
        den = jnp.sum(weighted, axis=2)
        num = jnp.einsum(
            "hts,shd->thd", weighted.astype(jnp.bfloat16), v, preferred_element_type=jnp.float32
        )
        summed = summed + num / jnp.maximum(jnp.abs(jnp.transpose(den)), 1.0)[:, :, None]
    normed = summed * lax.rsqrt(jnp.mean(summed * summed, axis=2, keepdims=True) + EPSILON)
    return (normed.reshape(rows, -1) * jax.nn.sigmoid(outgate.astype(jnp.float32))).astype(
        jnp.bfloat16
    )


def shards(
    residual,
    query_narrow,
    keys_narrow,
    values_narrow,
    outgate_narrow,
    gates_narrow,
    query_broad,
    keys_broad,
    values_broad,
    outgate_broad,
    gates_broad,
    outproj_narrow,
    outproj_broad,
    norm_gain,
    gate_weight,
    up_weight,
    down_weight,
):
    spread = lax.axis_size("sp")
    channels, hidden_own = gate_weight.shape
    stacked = jnp.stack([gate_weight.T, up_weight.T, down_weight.T])
    pieces = stacked.reshape(3, spread, hidden_own // spread, channels)
    pieces = lax.all_to_all(pieces, "sp", split_axis=1, concat_axis=1)
    weights = jnp.swapaxes(pieces, 1, 2).reshape(3, hidden_own // spread, -1)

    narrow, broad = keys_narrow.shape[1], keys_broad.shape[1]
    memory = lax.all_gather(
        jnp.concatenate([keys_narrow, values_narrow, keys_broad, values_broad], axis=1),
        "sp",
        axis=0,
        tiled=True,
    )
    kn, vn = memory[:, :narrow], memory[:, narrow : 2 * narrow]
    kb, vb = memory[:, 2 * narrow : 2 * narrow + broad], memory[:, 2 * narrow + broad :]
    cell_narrow = group_cell(query_narrow, kn, vn, outgate_narrow, gates_narrow, DH_A)
    cell_broad = group_cell(query_broad, kb, vb, outgate_broad, gates_broad, DH_B)

    own_count = residual.shape[0] // lax.axis_size("tp")
    proj = lax.psum_scatter(
        (
            jnp.dot(cell_narrow, outproj_narrow, preferred_element_type=jnp.float32)
            + jnp.dot(cell_broad, outproj_broad, preferred_element_type=jnp.float32)
        ).astype(jnp.bfloat16),
        "tp",
        scatter_dimension=0,
        tiled=True,
    ).astype(jnp.float32)
    offset = lax.axis_index("tp") * own_count
    stream = lax.dynamic_slice_in_dim(residual, offset, own_count, 0).astype(jnp.float32) + proj
    scaled = stream * lax.rsqrt(jnp.mean(stream * stream, axis=1, keepdims=True) + EPSILON)
    normed = (scaled * norm_gain.astype(jnp.float32)).astype(jnp.bfloat16)
    normed = lax.all_gather(normed, ("sp", "tp"), axis=0, tiled=True)
    nt = (((1,), (1,)), ((), ()))
    gate = lax.dot_general(normed, weights[0], nt, preferred_element_type=jnp.float32)
    upward = lax.dot_general(normed, weights[1], nt, preferred_element_type=jnp.float32)
    hidden = (jax.nn.silu(gate) * upward).astype(jnp.bfloat16)
    partial_value = jnp.dot(hidden, weights[2], preferred_element_type=jnp.float32)
    ffn = lax.psum_scatter(
        partial_value.astype(jnp.bfloat16), ("sp", "tp"), scatter_dimension=0, tiled=True
    ).astype(jnp.float32)
    return (stream + 0.5 * ffn).astype(jnp.bfloat16)


def fused_kernel(geometry, *refs):
    spread, members, wide, narrow_heads, broad_heads = geometry
    (res, qn, kn, vn, on, gn, qb, kb, vb, ob, gb, opn, opb, gain, gw, uw, dw, out) = refs[:18]
    (kv_all, info, gates, wt, w_all, pp, rs, x_all, part, r1, s2, r3) = refs[18:30]
    (kv_send, kv_recv, in_send, in_recv, w_send, w_recv, f_send, f_recv, g_send, g_recv) = refs[30:40]
    (p_send, p_recv, x_send, x_recv, e_send, e_recv, z_send, z_recv) = refs[40:48]
    rows = res.shape[0]
    own = rows // members
    depth = spread // 2
    chan, hid = gw.shape
    piece = hid // spread
    ca, cb = kn.shape[1], kb.shape[1]
    i, j = lax.axis_index("sp"), lax.axis_index("tp")
    z, x = i // 2, i % 2
    y, c = j // 2, j % 2
    ox = 1 - x
    f32, bf16 = jnp.float32, jnp.bfloat16
    sibling, x_peer = (i, j + 1 - 2 * c), (2 * z + ox, j)
    across = (1 - y) * 2 + c
    y_peer = (i, across)

    def ranked(n):
        pick = 0
        for a in range(depth):
            others = sorted(
                (b for b in range(depth) if b != a),
                key=lambda b: (abs(a - b), (a < depth // 2) == (b < depth // 2)),
            )
            pick = pick + jnp.where(z == a, others[n], 0)
        return pick

    def send(src, dst, s_sem, r_sem, to):
        copy = pltpu.make_async_remote_copy(
            src_ref=src, dst_ref=dst, send_sem=s_sem, recv_sem=r_sem, device_id=to, device_id_type=MESH
        )
        copy.start()
        return copy

    def arrived(ref, sem):
        pltpu.make_async_remote_copy(
            src_ref=ref, dst_ref=ref, send_sem=sem, recv_sem=sem, device_id=(i, j), device_id_type=MESH
        ).wait_recv()

    def sent(ref, sem, cond=None):
        def wait():
            pltpu.make_async_remote_copy(
                src_ref=ref, dst_ref=ref, send_sem=sem, recv_sem=sem, device_id=(i, j), device_id_type=MESH
            ).wait_send()

        if cond is None:
            wait()
        else:
            pl.when(cond)(wait)

    barrier = pltpu.get_barrier_semaphore()
    for k in range(1, spread):
        pl.semaphore_signal(barrier, inc=1, device_id=((i + k) % spread, j), device_id_type=MESH)
    for k in range(1, members):
        pl.semaphore_signal(barrier, inc=1, device_id=(i, (j + k) % members), device_id_type=MESH)

    kv_all[i, :, 0:ca] = kn[...]
    kv_all[i, :, ca : 2 * ca] = vn[...]
    kv_all[i, :, 2 * ca : 2 * ca + cb] = kb[...]
    kv_all[i, :, 2 * ca + cb : 2 * ca + 2 * cb] = vb[...]
    gates[...] = jnp.zeros_like(gates)
    for role in range(4):
        at = 8 * (role % 2)
        gates[role // 2, at : at + narrow_heads, :] = gn[role]
        gates[role // 2, at + narrow_heads : at + narrow_heads + broad_heads, :] = gb[role]
    in_gate, pre = gates[0], gates[1]
    forget = jnp.minimum(pre, 0.0) - jnp.log1p(jnp.exp(-jnp.abs(pre)))
    r_at = lax.broadcasted_iota(jnp.int32, (rows, rows), 0)
    c_at = lax.broadcasted_iota(jnp.int32, (rows, rows), 1)
    run = lambda m: jnp.dot(
        forget, m.astype(f32), preferred_element_type=f32, precision=lax.Precision.HIGHEST
    )
    forward_row = lax.broadcasted_iota(jnp.int32, in_gate.shape, 0) < 8
    cumulative = jnp.where(forward_row, run(r_at <= c_at), run(r_at >= c_at))
    total = jnp.where(
        forward_row,
        jnp.broadcast_to(cumulative[:, rows - 1 : rows], in_gate.shape),
        jnp.broadcast_to(cumulative[:, 0:1], in_gate.shape),
    )
    own_column = in_gate - cumulative
    info[i, 0] = total + own_column
    info[i, 1] = total
    pl.semaphore_wait(barrier, spread + members - 2)

    def pass_kv(slot, way, to):
        send(kv_all.at[slot], kv_all.at[slot], kv_send.at[way, slot], kv_recv.at[slot], to)
        send(info.at[slot], info.at[slot], in_send.at[way, slot], in_recv.at[slot], to)

    def kv_arrived(slot):
        arrived(kv_all.at[slot], kv_recv.at[slot])
        arrived(info.at[slot], in_recv.at[slot])

    @pl.when(z + 1 < depth)
    def _():
        pass_kv(i, 0, (i + 2, j))

    @pl.when(z >= 1)
    def _():
        pass_kv(i, 1, (i - 2, j))

    pass_kv(i, 2, (2 * z + ox, j))

    for m, ref in enumerate((gw, uw, dw)):
        for k in range(hid // 128):
            wt[m, k * 128 : (k + 1) * 128, :] = ref[:, k * 128 : (k + 1) * 128].T
    mine = pl.ds(pl.multiple_of(i * piece, 16), piece)

    def w_slot(jj, p):
        return w_all.at[:, jj, :, pl.ds(pl.multiple_of(p * chan, 128), chan)]

    def send_weights(p):
        theirs = pl.ds(pl.multiple_of(p * piece, 16), piece)
        send(wt.at[:, theirs, :], w_slot(j, i), w_send.at[p], w_recv.at[i], (p, j))

    def share_weights(p):
        slot = w_slot(j, p)
        arrived(slot, w_recv.at[p])
        send(slot, slot, f_send.at[0, p], f_recv.at[0, p], sibling)
        send(slot, slot, g_send.at[p], g_recv.at[p], y_peer)

    def share_across(p):
        slot = w_slot(across, p)
        arrived(slot, g_recv.at[p])
        send(slot, slot, f_send.at[1, p], f_recv.at[1, p], sibling)

    columns = pl.ds(pl.multiple_of(i * chan, 128), chan)
    block = wt.at[:, mine, :]
    send(block, w_slot(j, i), g_send.at[i], g_recv.at[i], y_peer)
    send(block, w_slot(j, i), f_send.at[0, i], f_recv.at[0, i], sibling)
    w_all[:, j, :, columns] = wt[:, mine, :]
    for s in range(1, depth):

        @pl.when(z - s >= 0)
        def _():
            slot = i - 2 * s
            kv_arrived(slot)

            @pl.when(z + 1 < depth)
            def _():
                pass_kv(slot, 0, (i + 2, j))

            pass_kv(slot, 2, (2 * z + ox, j))

        @pl.when(z + s < depth)
        def _():
            slot = i + 2 * s
            kv_arrived(slot)

            @pl.when(z >= 1)
            def _():
                pass_kv(slot, 1, (i - 2, j))

            pass_kv(slot, 2, (2 * z + ox, j))

    straight = [2 * ranked(n) + x for n in range(depth - 1)]
    crossed = [2 * z + ox] + [2 * ranked(n) + ox for n in range(depth - 1)]
    middle = jnp.logical_or(z == depth // 2 - 1, z == depth // 2)

    @pl.when(middle)
    def _():
        send_weights(straight[0])

    def kv_sent(slot, way, cond=None):
        sent(kv_all.at[slot], kv_send.at[way, slot], cond)
        sent(info.at[slot], in_send.at[way, slot], cond)

    for zz in range(depth):
        kv_sent(2 * zz + x, 0, jnp.logical_and(zz <= z, z + 1 < depth))
        kv_sent(2 * zz + x, 1, jnp.logical_and(zz >= z, z >= 1))

    @pl.when(jnp.logical_not(middle))
    def _():
        send_weights(straight[0])

    send_weights(straight[1])
    for zz in range(depth):
        kv_arrived(2 * zz + ox)
    send_weights(crossed[0])
    for p in straight[2:]:
        send_weights(p)

    offset = jnp.zeros_like(total)
    pieces = [None] * spread
    forward_sum = jnp.zeros_like(total)
    ahead = [None] * spread
    for k in reversed(range(spread)):
        ahead[k] = forward_sum
        forward_sum = forward_sum + jnp.where(k < i, info[k, 1], 0.0)
    backward_sum = jnp.zeros_like(total)
    for k in range(spread):
        reach = jnp.where(forward_row, ahead[k], backward_sum) + info[k, 0]
        seen = jnp.logical_or(
            jnp.logical_and(forward_row, k < i), jnp.logical_and(jnp.logical_not(forward_row), k > i)
        )
        pieces[k] = jnp.where(k == i, own_column, jnp.where(seen, reach, FAR))
        backward_sum = backward_sum + jnp.where(k > i, info[k, 1], 0.0)
    column = jnp.concatenate(pieces, axis=1)
    t_at = lax.broadcasted_iota(jnp.int32, (rows, spread * rows), 0) + i * rows
    s_at = lax.broadcasted_iota(jnp.int32, (rows, spread * rows), 1)
    masks = (s_at <= t_at, s_at >= t_at)
    nt = (((1,), (1,)), ((), ()))
    proj = jnp.zeros((rows, res.shape[1]), f32)
    heads = [(qn, on, opn, 0, ca, h, ca // narrow_heads, h) for h in range(narrow_heads)]
    heads += [
        (qb, ob, opb, 2 * ca, cb, h, cb // broad_heads, narrow_heads + h) for h in range(broad_heads)
    ]
    for query, outgate, outproj, base, group, h, width, row in heads:
        lanes = slice(h * width, (h + 1) * width)
        keys = kv_all[:, :, base + h * width : base + (h + 1) * width].reshape(spread * rows, width)
        vals = kv_all[:, :, base + group + h * width : base + group + (h + 1) * width].reshape(
            spread * rows, width
        )
        scores = lax.dot_general(query[:, lanes], keys, nt, preferred_element_type=f32) * width ** (-0.5)
        summed = jnp.zeros((rows, width), f32)
        for direction in range(2):
            at = 8 * direction + row
            weight = jnp.where(
                masks[direction],
                jnp.broadcast_to(column[at : at + 1, :], scores.shape),
                FAR,
            )
            top = jnp.max(weight, axis=1, keepdims=True)
            p = jnp.exp(weight - top) * scores
            den = jnp.sum(p, axis=1, keepdims=True)
            num = jnp.dot(p.astype(bf16), vals, preferred_element_type=f32)
            summed = summed + num / jnp.maximum(jnp.abs(den), 1.0)
        normed = summed * lax.rsqrt(jnp.mean(summed * summed, axis=1, keepdims=True) + EPSILON)
        opened = 1.0 / (1.0 + jnp.exp(-outgate[:, lanes].astype(f32)))
        cell = (normed * opened).astype(bf16)
        proj = proj + jnp.dot(cell, outproj[lanes, :], preferred_element_type=f32)
    pp[...] = proj.astype(bf16).reshape(pp.shape)

    for k in range(1, members):
        q = (j + k) % members
        send(pp.at[q], rs.at[j], p_send.at[q], p_recv.at[j], (i, q))
    share_weights(straight[0])
    for p in crossed[1:4]:
        send_weights(p)
    stream = res[pl.ds(pl.multiple_of(j * own, own), own), :].astype(f32) + pp[j].astype(f32)
    for k in range(1, members):
        q = (j + k) % members
        arrived(rs.at[q], p_recv.at[q])
        stream = stream + rs[q].astype(f32)
    scaled = stream * lax.rsqrt(jnp.mean(stream * stream, axis=1, keepdims=True) + EPSILON)
    x_all[x, z] = (scaled * gain[...].astype(f32).reshape(1, wide)).astype(bf16)

    def pass_x(zz, sem, to):
        slot = x_all.at[x, zz]
        send(slot, slot, sem, x_recv.at[x, zz], to)

    def x_arrived(xx, zz):
        arrived(x_all.at[xx, zz], x_recv.at[xx, zz])

    for n in range(depth - 1):
        pass_x(z, x_send.at[0, n], (2 * ranked(n) + x, j))
    pass_x(z, x_send.at[1, z], x_peer)

    def forward_x(n):
        zz = ranked(n)
        x_arrived(x, zz)
        pass_x(zz, x_send.at[1, zz], x_peer)

    share_weights(straight[1])
    share_across(i)
    share_weights(straight[2])
    share_across(straight[0])
    share_weights(crossed[0])
    share_across(straight[1])
    share_weights(crossed[1])
    share_across(straight[2])
    share_weights(crossed[2])
    share_across(crossed[0])
    share_weights(crossed[3])
    forward_x(0)
    forward_x(1)
    forward_x(2)
    share_across(crossed[1])
    share_across(crossed[2])
    share_across(crossed[3])
    for zz in range(depth):
        x_arrived(ox, zz)
    other, other_across = 2 * y + 1 - c, 2 * (1 - y) + 1 - c
    for p in [i] + straight + crossed:
        arrived(w_slot(other, p), f_recv.at[0, p])
        arrived(w_slot(other_across, p), f_recv.at[1, p])

    units = members * piece

    def chunk(xx):
        a = x_all[xx].reshape(depth * own, -1)
        gate = lax.dot_general(a, w_all[0].reshape(units, -1), nt, preferred_element_type=f32)
        up = lax.dot_general(a, w_all[1].reshape(units, -1), nt, preferred_element_type=f32)
        hidden = (gate / (1.0 + jnp.exp(-gate)) * up).astype(bf16)
        got = jnp.dot(hidden, w_all[2].reshape(units, -1), preferred_element_type=f32)
        part[xx] = got.astype(bf16).reshape(depth, own, -1)

    ends = [(z + depth // 2) % depth] + [(z + k) % depth for k in range(1, depth) if 2 * k != depth]
    chunk(ox)
    for zz in ends + [z]:
        send(part.at[ox, zz], r1.at[zz], e_send.at[zz], e_recv.at[zz], x_peer)
    chunk(x)
    for zz in ends:
        arrived(r1.at[zz], e_recv.at[zz])
        s2[zz] = (part[x, zz].astype(f32) + r1[zz].astype(f32)).astype(bf16)
        send(s2.at[zz], r3.at[z], z_send.at[zz], z_recv.at[z], (2 * zz + x, j))
    arrived(r1.at[z], e_recv.at[z])
    ffn = part[x, z].astype(f32) + r1[z].astype(f32)
    for zz in ends:
        arrived(r3.at[zz], z_recv.at[zz])
        ffn = ffn + r3[zz].astype(f32)
    out[...] = (stream + 0.5 * ffn).astype(out.dtype)

    for zz in range(depth):
        kv_sent(2 * zz + x, 2)
        slot = x_all.at[x, zz]
        sent(slot, x_send.at[1, zz])
        sent(r1.at[0], e_send.at[zz])
    for n in range(depth - 1):
        sent(x_all.at[0, 0], x_send.at[0, n])
    for p in straight + crossed:
        sent(block, w_send.at[p])
    for p in range(spread):
        sent(block, f_send.at[0, p])
        sent(block, f_send.at[1, p])
        sent(block, g_send.at[p])
    for k in range(1, members):
        sent(rs.at[0], p_send.at[(j + k) % members])
    for zz in ends:
        sent(s2.at[0], z_send.at[zz])


def fused_shards(*args):
    (res, qn, kn, vn, on, gn, qb, kb, vb, ob, gb, opn, opb, gain, gw, uw, dw) = args
    spread, members = lax.axis_size("sp"), lax.axis_size("tp")
    rows, wide = res.shape
    own, depth = rows // members, spread // 2
    chan, hid = gw.shape
    piece = hid // spread
    kvw = 2 * (kn.shape[1] + kb.shape[1])
    bf16, f32 = jnp.bfloat16, jnp.float32
    v = pltpu.VMEM
    dma = pltpu.SemaphoreType.DMA
    scratch = [
        v((spread, rows, kvw), bf16),
        v((spread, 2, 16, rows), f32),
        v((2, 16, rows), f32),
        v((3, hid, chan), bf16),
        v((3, members, piece, wide), bf16),
        v((members, own, wide), bf16),
        v((members, own, wide), bf16),
        v((2, depth, own, wide), bf16),
        v((2, depth, own, wide), bf16),
        v((depth, own, wide), bf16),
        v((depth, own, wide), bf16),
        v((depth, own, wide), bf16),
        dma((3, spread)),
        dma((spread,)),
        dma((3, spread)),
        dma((spread,)),
        dma((spread,)),
        dma((spread,)),
        dma((2, spread)),
        dma((2, spread)),
        dma((spread,)),
        dma((spread,)),
        dma((members,)),
        dma((members,)),
        dma((2, depth)),
        dma((2, depth)),
        dma((depth,)),
        dma((depth,)),
        dma((depth,)),
        dma((depth,)),
    ]
    geometry = (spread, members, wide, gn.shape[1], gb.shape[1])
    return pl.pallas_call(
        functools.partial(fused_kernel, geometry),
        out_shape=jax.ShapeDtypeStruct((own, wide), bf16),
        in_specs=[pl.BlockSpec(memory_space=pltpu.VMEM)] * 17,
        out_specs=pl.BlockSpec(memory_space=pltpu.VMEM),
        scratch_shapes=scratch,
        compiler_params=pltpu.CompilerParams(
            collective_id=0, has_side_effects=True, vmem_limit_bytes=60 * 1024 * 1024
        ),
        name="fused",
    )(res, qn, kn, vn, on, gn, qb, kb, vb, ob, gb, opn, opb, gain, gw, uw, dw)


def pick(*args):
    res, kn, gn, gb, gw = args[0], args[2], args[5], args[10], args[14]
    spread, members = lax.axis_size("sp"), lax.axis_size("tp")
    rows = res.shape[0]
    chan, hid = gw.shape
    fits = (
        spread % 2 == 0
        and spread >= 4
        and members == 4
        and rows == 128
        and spread * rows <= 2048
        and chan % 128 == 0
        and hid % (16 * spread) == 0
        and hid % 128 == 0
        and gn.shape[1] + gb.shape[1] <= 8
    )
    return fused_shards(*args) if fits else shards(*args)


def solution(mesh):
    in_specs = (
        P("sp", None),
        P("sp", "tp"),
        P("sp", "tp"),
        P("sp", "tp"),
        P("sp", "tp"),
        P(None, "tp", "sp"),
        P("sp", "tp"),
        P("sp", "tp"),
        P("sp", "tp"),
        P("sp", "tp"),
        P(None, "tp", "sp"),
        P("tp", None),
        P("tp", None),
        P(),
        P("sp", "tp"),
        P("sp", "tp"),
        P("sp", "tp"),
    )
    out_specs = P(("sp", "tp"), None)
    return jax.shard_map(pick, mesh=mesh, in_specs=in_specs, out_specs=out_specs, check_vma=False)
```

```python
import functools

import jax
import jax.numpy as jnp
from jax import lax
from jax.experimental import pallas as pl
from jax.experimental.pallas import tpu as pltpu
from jax.sharding import PartitionSpec as P

DH_A = 128
DH_B = 256

EPSILON = 1e-06
FAR = -1e30
MESH = pl.DeviceIdType.MESH


def direction_columns(in_gate, log_forget, reverse):
    place, length = lax.axis_index("sp"), lax.axis_size("sp")
    cumulative = lax.cumsum(log_forget, axis=1, reverse=reverse)
    total = cumulative[:, 0] if reverse else cumulative[:, -1]
    toward_end = total[:, None] - cumulative + in_gate
    packed = jnp.concatenate([toward_end, total[:, None]], axis=1)
    every = lax.all_gather(packed, "sp")
    ends, totals = every[:, :, :-1], every[:, :, -1]
    index = jnp.arange(length)
    if reverse:
        between = (index[None, :] > place) & (index[None, :] < index[:, None])
        valid = index > place
    else:
        between = (index[None, :] < place) & (index[None, :] > index[:, None])
        valid = index < place
    offset = jnp.sum(jnp.where(between[:, :, None], totals[None], 0.0), axis=1)
    columns = jnp.where(valid[:, None, None], offset[:, :, None] + ends, FAR)
    own = (in_gate - cumulative)[None]
    columns = jnp.where((index == place)[:, None, None], own, columns)
    return jnp.moveaxis(columns, 0, 1).reshape(in_gate.shape[0], -1)


def group_cell(query, keys, values, outgate, gates, width):
    rows, every = query.shape[0], keys.shape[0]
    place = lax.axis_index("sp")
    heads = query.shape[1] // width
    q = query.reshape(rows, heads, width)
    k = keys.reshape(every, heads, width)
    v = values.reshape(every, heads, width)
    scores = jnp.einsum("thd,shd->hts", q, k, preferred_element_type=jnp.float32) * width ** (-0.5)
    t_at = (place * rows + jnp.arange(rows))[:, None]
    s_at = jnp.arange(every)[None, :]
    summed = 0.0
    for direction in range(2):
        columns = direction_columns(
            gates[direction], jax.nn.log_sigmoid(gates[2 + direction]), direction == 1
        )
        mask = s_at >= t_at if direction else s_at <= t_at
        log_weight = jnp.where(mask[None], columns[:, None, :], FAR)
        top = jnp.max(log_weight, axis=2, keepdims=True)
        weighted = jnp.exp(log_weight - top) * scores
        den = jnp.sum(weighted, axis=2)
        num = jnp.einsum(
            "hts,shd->thd", weighted.astype(jnp.bfloat16), v, preferred_element_type=jnp.float32
        )
        summed = summed + num / jnp.maximum(jnp.abs(jnp.transpose(den)), 1.0)[:, :, None]
    normed = summed * lax.rsqrt(jnp.mean(summed * summed, axis=2, keepdims=True) + EPSILON)
    return (normed.reshape(rows, -1) * jax.nn.sigmoid(outgate.astype(jnp.float32))).astype(
        jnp.bfloat16
    )


def shards(
    residual,
    query_narrow,
    keys_narrow,
    values_narrow,
    outgate_narrow,
    gates_narrow,
    query_broad,
    keys_broad,
    values_broad,
    outgate_broad,
    gates_broad,
    outproj_narrow,
    outproj_broad,
    norm_gain,
    gate_weight,
    up_weight,
    down_weight,
):
    spread = lax.axis_size("sp")
    channels, hidden_own = gate_weight.shape
    stacked = jnp.stack([gate_weight.T, up_weight.T, down_weight.T])
    pieces = stacked.reshape(3, spread, hidden_own // spread, channels)
    pieces = lax.all_to_all(pieces, "sp", split_axis=1, concat_axis=1)
    weights = jnp.swapaxes(pieces, 1, 2).reshape(3, hidden_own // spread, -1)

    narrow, broad = keys_narrow.shape[1], keys_broad.shape[1]
    memory = lax.all_gather(
        jnp.concatenate([keys_narrow, values_narrow, keys_broad, values_broad], axis=1),
        "sp",
        axis=0,
        tiled=True,
    )
    kn, vn = memory[:, :narrow], memory[:, narrow : 2 * narrow]
    kb, vb = memory[:, 2 * narrow : 2 * narrow + broad], memory[:, 2 * narrow + broad :]
    cell_narrow = group_cell(query_narrow, kn, vn, outgate_narrow, gates_narrow, DH_A)
    cell_broad = group_cell(query_broad, kb, vb, outgate_broad, gates_broad, DH_B)

    own_count = residual.shape[0] // lax.axis_size("tp")
    proj = lax.psum_scatter(
        (
            jnp.dot(cell_narrow, outproj_narrow, preferred_element_type=jnp.float32)
            + jnp.dot(cell_broad, outproj_broad, preferred_element_type=jnp.float32)
        ).astype(jnp.bfloat16),
        "tp",
        scatter_dimension=0,
        tiled=True,
    ).astype(jnp.float32)
    offset = lax.axis_index("tp") * own_count
    stream = lax.dynamic_slice_in_dim(residual, offset, own_count, 0).astype(jnp.float32) + proj
    scaled = stream * lax.rsqrt(jnp.mean(stream * stream, axis=1, keepdims=True) + EPSILON)
    normed = (scaled * norm_gain.astype(jnp.float32)).astype(jnp.bfloat16)
    normed = lax.all_gather(normed, ("sp", "tp"), axis=0, tiled=True)
    nt = (((1,), (1,)), ((), ()))
    gate = lax.dot_general(normed, weights[0], nt, preferred_element_type=jnp.float32)
    upward = lax.dot_general(normed, weights[1], nt, preferred_element_type=jnp.float32)
    hidden = (jax.nn.silu(gate) * upward).astype(jnp.bfloat16)
    partial_value = jnp.dot(hidden, weights[2], preferred_element_type=jnp.float32)
    ffn = lax.psum_scatter(
        partial_value.astype(jnp.bfloat16), ("sp", "tp"), scatter_dimension=0, tiled=True
    ).astype(jnp.float32)
    return (stream + 0.5 * ffn).astype(jnp.bfloat16)


def fused_kernel(geometry, *refs):
    spread, members, wide, narrow_heads, broad_heads = geometry
    (res, qn, kn, vn, on, gn, qb, kb, vb, ob, gb, opn, opb, gain, gw, uw, dw, out) = refs[:18]
    (kv_all, info, gates, wt, w_all, pp, rs, x_all, part, r1, s2, r3) = refs[18:30]
    (st_out, sn_out, st_in, sn_in) = refs[30:34]
    (kv_send, kv_recv, in_send, in_recv, w_send, w_recv, f_send, f_recv, g_send, g_recv) = refs[34:44]
    (p_send, p_recv, x_send, x_recv, e_send, e_recv, z_send, z_recv) = refs[44:52]
    (st_send, st_recv, sn_recv) = refs[52:55]
    rows = res.shape[0]
    own = rows // members
    depth = spread // 2
    chan, hid = gw.shape
    piece = hid // spread
    ca, cb = kn.shape[1], kb.shape[1]
    i, j = lax.axis_index("sp"), lax.axis_index("tp")
    z, x = i // 2, i % 2
    y, c = j // 2, j % 2
    ox = 1 - x
    size = spread // 2
    half, local = i // size, i % size
    f32, bf16 = jnp.float32, jnp.bfloat16
    sibling, x_peer = (i, j + 1 - 2 * c), (2 * z + ox, j)
    across = (1 - y) * 2 + c
    y_peer = (i, across)

    def ranked(n):
        pick = 0
        for a in range(depth):
            others = sorted(
                (b for b in range(depth) if b != a),
                key=lambda b: (abs(a - b), (a < depth // 2) == (b < depth // 2)),
            )
            pick = pick + jnp.where(z == a, others[n], 0)
        return pick

    def send(src, dst, s_sem, r_sem, to):
        copy = pltpu.make_async_remote_copy(
            src_ref=src, dst_ref=dst, send_sem=s_sem, recv_sem=r_sem, device_id=to, device_id_type=MESH
        )
        copy.start()
        return copy

    def arrived(ref, sem):
        pltpu.make_async_remote_copy(
            src_ref=ref, dst_ref=ref, send_sem=sem, recv_sem=sem, device_id=(i, j), device_id_type=MESH
        ).wait_recv()

    def sent(ref, sem, cond=None):
        def wait():
            pltpu.make_async_remote_copy(
                src_ref=ref, dst_ref=ref, send_sem=sem, recv_sem=sem, device_id=(i, j), device_id_type=MESH
            ).wait_send()

        if cond is None:
            wait()
        else:
            pl.when(cond)(wait)

    barrier = pltpu.get_barrier_semaphore()
    for k in range(1, spread):
        pl.semaphore_signal(barrier, inc=1, device_id=((i + k) % spread, j), device_id_type=MESH)
    for k in range(1, members):
        pl.semaphore_signal(barrier, inc=1, device_id=(i, (j + k) % members), device_id_type=MESH)

    kv_all[local, :, 0:ca] = kn[...]
    kv_all[local, :, ca : 2 * ca] = vn[...]
    kv_all[local, :, 2 * ca : 2 * ca + cb] = kb[...]
    kv_all[local, :, 2 * ca + cb : 2 * ca + 2 * cb] = vb[...]
    gates[...] = jnp.zeros_like(gates)
    for role in range(4):
        at = 8 * (role % 2)
        gates[role // 2, at : at + narrow_heads, :] = gn[role]
        gates[role // 2, at + narrow_heads : at + narrow_heads + broad_heads, :] = gb[role]
    in_gate, pre = gates[0], gates[1]
    forget = jnp.minimum(pre, 0.0) - jnp.log1p(jnp.exp(-jnp.abs(pre)))
    r_at = lax.broadcasted_iota(jnp.int32, (rows, rows), 0)
    c_at = lax.broadcasted_iota(jnp.int32, (rows, rows), 1)
    run = lambda m: jnp.dot(
        forget, m.astype(f32), preferred_element_type=f32, precision=lax.Precision.HIGHEST
    )
    forward_row = lax.broadcasted_iota(jnp.int32, in_gate.shape, 0) < 8
    cumulative = jnp.where(forward_row, run(r_at <= c_at), run(r_at >= c_at))
    total = jnp.where(
        forward_row,
        jnp.broadcast_to(cumulative[:, rows - 1 : rows], in_gate.shape),
        jnp.broadcast_to(cumulative[:, 0:1], in_gate.shape),
    )
    own_column = in_gate - cumulative
    info[local, 0] = total + own_column
    info[local, 1] = total
    pl.semaphore_wait(barrier, spread + members - 2)

    mates = [(local + k) % size for k in range(1, size)]
    for k, mate in enumerate(mates):
        to = (half * size + mate, j)
        send(kv_all.at[local], kv_all.at[local], kv_send.at[k], kv_recv.at[local], to)
        send(info.at[local], info.at[local], in_send.at[k], in_recv.at[local], to)

    for m, ref in enumerate((gw, uw, dw)):
        for k in range(hid // 128):
            wt[m, k * 128 : (k + 1) * 128, :] = ref[:, k * 128 : (k + 1) * 128].T
    mine = pl.ds(pl.multiple_of(i * piece, 16), piece)

    def w_slot(jj, p):
        return w_all.at[:, jj, :, pl.ds(pl.multiple_of(p * chan, 128), chan)]

    def send_weights(p):
        theirs = pl.ds(pl.multiple_of(p * piece, 16), piece)
        send(wt.at[:, theirs, :], w_slot(j, i), w_send.at[p], w_recv.at[i], (p, j))

    def share_weights(p):
        slot = w_slot(j, p)
        arrived(slot, w_recv.at[p])
        send(slot, slot, f_send.at[0, p], f_recv.at[0, p], sibling)
        send(slot, slot, g_send.at[p], g_recv.at[p], y_peer)

    def share_across(p):
        slot = w_slot(across, p)
        arrived(slot, g_recv.at[p])
        send(slot, slot, f_send.at[1, p], f_recv.at[1, p], sibling)

    columns = pl.ds(pl.multiple_of(i * chan, 128), chan)
    block = wt.at[:, mine, :]
    send(block, w_slot(j, i), g_send.at[i], g_recv.at[i], y_peer)
    send(block, w_slot(j, i), f_send.at[0, i], f_recv.at[0, i], sibling)
    w_all[:, j, :, columns] = wt[:, mine, :]
    straight = [2 * ranked(n) + x for n in range(depth - 1)]
    crossed = [2 * z + ox] + [2 * ranked(n) + ox for n in range(depth - 1)]
    middle = jnp.logical_or(z == depth // 2 - 1, z == depth // 2)

    @pl.when(middle)
    def _():
        for p in (straight[0], crossed[1], straight[2], straight[1]):
            send_weights(p)

    @pl.when(jnp.logical_not(middle))
    def _():
        send_weights(straight[1])

    send_weights(crossed[0])
    in_turn = [
        jnp.where(middle, a, b)
        for a, b in zip(
            [straight[0], crossed[1], crossed[0], straight[2], crossed[3], straight[1], crossed[2]],
            [straight[0], crossed[0], straight[1], crossed[1], crossed[2], straight[2], crossed[3]],
        )
    ]

    for mate in mates:
        arrived(kv_all.at[mate], kv_recv.at[mate])
        arrived(info.at[mate], in_recv.at[mate])

    before, after = [], [None] * size
    passed = jnp.zeros_like(total)
    for k in range(size):
        before.append(passed)
        passed = passed + info[k, 1]
    passed = jnp.zeros_like(total)
    for k in reversed(range(size)):
        after[k] = passed
        passed = passed + info[k, 1]
    to_end = jnp.concatenate(
        [info[k, 0] + jnp.where(forward_row, after[k], before[k]) for k in range(size)], axis=1
    )
    to_end = jnp.where(half == 0, to_end[0:8], to_end[8:16])
    end_max = jnp.max(to_end, axis=1, keepdims=True)
    share = jnp.transpose(
        jnp.concatenate([jnp.exp(to_end - end_max), jnp.zeros((rows - 8, size * rows), f32)], axis=0)
    )
    share_a = jnp.where(x == 0, share[:, 0:1], share[:, 1:2])
    share_b = share[:, narrow_heads : narrow_heads + 1]
    wa, wb = ca // narrow_heads, cb // 2

    def kv_lanes(start, width):
        return kv_all[:, :, pl.ds(pl.multiple_of(start, 128), width)].reshape(size * rows, width)

    tn = (((0,), (0,)), ((), ()))
    keys_a, keys_b = kv_lanes(x * wa, wa), kv_lanes(2 * ca, cb)
    values_a = (share_a * kv_lanes(ca + x * wa, wa).astype(f32)).astype(bf16)
    values_b = (share_b * kv_lanes(2 * ca + cb + x * wb, wb).astype(f32)).astype(bf16)
    st_out[0:wa, :] = lax.dot_general(keys_a, values_a, tn, preferred_element_type=f32).astype(bf16)
    st_out[wa : wa + cb, :] = lax.dot_general(keys_b, values_b, tn, preferred_element_type=f32).astype(bf16)
    norm_a = jnp.sum(share_a * keys_a.astype(f32), axis=0, keepdims=True)
    norm_b = jnp.sum(share_b * keys_b.astype(f32), axis=0, keepdims=True)
    sn_out[:, 0:wa] = jnp.broadcast_to(norm_a, (8, wa))
    sn_out[:, wa : wa + cb] = jnp.broadcast_to(norm_b, (8, cb))
    sn_out[:, wa + cb :] = jnp.broadcast_to(end_max, (8, rows))
    mirror = ((i + size) % spread, j)
    send(sn_out, sn_in.at[x], st_send.at[1], sn_recv.at[x], mirror)
    send(st_out, st_in.at[x], st_send.at[0], st_recv.at[x], mirror)

    @pl.when(middle)
    def _():
        for p in (crossed[3], crossed[2]):
            send_weights(p)

    @pl.when(jnp.logical_not(middle))
    def _():
        for p in (straight[2], crossed[2], straight[0], crossed[3], crossed[1]):
            send_weights(p)

    for p in in_turn[:3]:
        share_weights(p)
    arrived(sn_in.at[x], sn_recv.at[x])
    arrived(st_in.at[x], st_recv.at[x])
    send(sn_in.at[x], sn_in.at[x], st_send.at[3], sn_recv.at[x], x_peer)
    send(st_in.at[x], st_in.at[x], st_send.at[2], st_recv.at[x], x_peer)
    arrived(sn_in.at[ox], sn_recv.at[ox])
    arrived(st_in.at[ox], st_recv.at[ox])

    pieces = [None] * size
    forward_sum = jnp.zeros_like(total)
    ahead = [None] * size
    for k in reversed(range(size)):
        ahead[k] = forward_sum
        forward_sum = forward_sum + jnp.where(k < local, info[k, 1], 0.0)
    backward_sum = jnp.zeros_like(total)
    for k in range(size):
        reach = jnp.where(forward_row, ahead[k], backward_sum) + info[k, 0]
        seen = jnp.logical_or(
            jnp.logical_and(forward_row, k < local),
            jnp.logical_and(jnp.logical_not(forward_row), k > local),
        )
        pieces[k] = jnp.where(k == local, own_column, jnp.where(seen, reach, FAR))
        backward_sum = backward_sum + jnp.where(k > local, info[k, 1], 0.0)
    column = jnp.concatenate(pieces, axis=1)
    past = sn_in[x, :, wa + cb :] + jnp.where(half == 1, forward_sum[0:8], backward_sum[8:16])
    t_at = lax.broadcasted_iota(jnp.int32, (rows, size * rows), 0) + local * rows
    s_at = lax.broadcasted_iota(jnp.int32, (rows, size * rows), 1)
    masks = (s_at <= t_at, s_at >= t_at)
    nt = (((1,), (1,)), ((), ()))
    proj = jnp.zeros((rows, res.shape[1]), f32)
    heads = [(qn, on, opn, 0, ca, h, ca // narrow_heads, h) for h in range(narrow_heads)]
    heads += [
        (qb, ob, opb, 2 * ca, cb, h, cb // broad_heads, narrow_heads + h) for h in range(broad_heads)
    ]
    for query, outgate, outproj, base, group, h, width, row in heads:
        lanes = slice(h * width, (h + 1) * width)
        keys = kv_all[:, :, base + h * width : base + (h + 1) * width].reshape(size * rows, width)
        vals = kv_all[:, :, base + group + h * width : base + group + (h + 1) * width].reshape(
            size * rows, width
        )
        queries = query[:, lanes]
        scores = lax.dot_general(queries, keys, nt, preferred_element_type=f32) * width ** (-0.5)
        if row < narrow_heads:
            memory, normer = st_in[row, 0:wa, :], sn_in[row, 0:1, 0:wa]
        else:
            memory = jnp.concatenate([st_in[0, wa:, :], st_in[1, wa:, :]], axis=1)
            normer = sn_in[0, 0:1, wa : wa + cb]
        recalled = jnp.dot(queries, memory, preferred_element_type=f32) * width ** (-0.5)
        recall_den = jnp.sum(queries.astype(f32) * normer, axis=1, keepdims=True) * width ** (-0.5)
        summed = jnp.zeros((rows, width), f32)
        for direction in range(2):
            at = 8 * direction + row
            weight = jnp.where(
                masks[direction],
                jnp.broadcast_to(column[at : at + 1, :], scores.shape),
                FAR,
            )
            carried = jnp.where(half == 1 - direction, past[row : row + 1, 0:1], FAR)
            top = jnp.maximum(jnp.max(weight, axis=1, keepdims=True), carried)
            kept = jnp.exp(carried - top)
            p = jnp.exp(weight - top) * scores
            den = jnp.sum(p, axis=1, keepdims=True) + kept * recall_den
            num = jnp.dot(p.astype(bf16), vals, preferred_element_type=f32) + kept * recalled
            summed = summed + num / jnp.maximum(jnp.abs(den), 1.0)
        normed = summed * lax.rsqrt(jnp.mean(summed * summed, axis=1, keepdims=True) + EPSILON)
        opened = 1.0 / (1.0 + jnp.exp(-outgate[:, lanes].astype(f32)))
        cell = (normed * opened).astype(bf16)
        proj = proj + jnp.dot(cell, outproj[lanes, :], preferred_element_type=f32)
    pp[...] = proj.astype(bf16).reshape(pp.shape)

    for k in range(1, members):
        q = (j + k) % members
        send(pp.at[q], rs.at[j], p_send.at[q], p_recv.at[j], (i, q))
    stream = res[pl.ds(pl.multiple_of(j * own, own), own), :].astype(f32) + pp[j].astype(f32)
    for k in range(1, members):
        q = (j + k) % members
        arrived(rs.at[q], p_recv.at[q])
        stream = stream + rs[q].astype(f32)
    scaled = stream * lax.rsqrt(jnp.mean(stream * stream, axis=1, keepdims=True) + EPSILON)
    x_all[x, z] = (scaled * gain[...].astype(f32).reshape(1, wide)).astype(bf16)

    def pass_x(zz, sem, to):
        slot = x_all.at[x, zz]
        send(slot, slot, sem, x_recv.at[x, zz], to)

    def x_arrived(xx, zz):
        arrived(x_all.at[xx, zz], x_recv.at[xx, zz])

    for n in range(depth - 1):
        pass_x(z, x_send.at[0, n], (2 * ranked(n) + x, j))
    pass_x(z, x_send.at[1, z], x_peer)

    def forward_x(n):
        zz = ranked(n)
        x_arrived(x, zz)
        pass_x(zz, x_send.at[1, zz], x_peer)

    share_weights(in_turn[3])
    share_across(i)
    share_across(in_turn[0])
    share_weights(in_turn[4])
    share_across(in_turn[1])
    share_across(in_turn[2])
    share_weights(in_turn[5])
    share_weights(in_turn[6])
    share_across(in_turn[3])
    forward_x(0)
    forward_x(1)
    forward_x(2)
    share_across(in_turn[4])
    share_across(in_turn[5])
    share_across(in_turn[6])
    for zz in range(depth):
        x_arrived(ox, zz)
    other, other_across = 2 * y + 1 - c, 2 * (1 - y) + 1 - c
    for p in [i] + in_turn:
        arrived(w_slot(other, p), f_recv.at[0, p])
        arrived(w_slot(other_across, p), f_recv.at[1, p])

    units = members * piece

    def chunk(xx):
        a = x_all[xx].reshape(depth * own, -1)
        gate = lax.dot_general(a, w_all[0].reshape(units, -1), nt, preferred_element_type=f32)
        up = lax.dot_general(a, w_all[1].reshape(units, -1), nt, preferred_element_type=f32)
        hidden = (gate / (1.0 + jnp.exp(-gate)) * up).astype(bf16)
        got = jnp.dot(hidden, w_all[2].reshape(units, -1), preferred_element_type=f32)
        part[xx] = got.astype(bf16).reshape(depth, own, -1)

    ends = [(z + depth // 2) % depth] + [(z + k) % depth for k in range(1, depth) if 2 * k != depth]
    chunk(ox)
    for zz in ends + [z]:
        send(part.at[ox, zz], r1.at[zz], e_send.at[zz], e_recv.at[zz], x_peer)
    chunk(x)
    for zz in ends:
        arrived(r1.at[zz], e_recv.at[zz])
        s2[zz] = (part[x, zz].astype(f32) + r1[zz].astype(f32)).astype(bf16)
        send(s2.at[zz], r3.at[z], z_send.at[zz], z_recv.at[z], (2 * zz + x, j))
    arrived(r1.at[z], e_recv.at[z])
    ffn = part[x, z].astype(f32) + r1[z].astype(f32)
    for zz in ends:
        arrived(r3.at[zz], z_recv.at[zz])
        ffn = ffn + r3[zz].astype(f32)
    out[...] = (stream + 0.5 * ffn).astype(out.dtype)

    for k in range(size - 1):
        sent(kv_all.at[0], kv_send.at[k])
        sent(info.at[0], in_send.at[k])
    sent(st_out, st_send.at[0])
    sent(sn_out, st_send.at[1])
    sent(st_out, st_send.at[2])
    sent(sn_out, st_send.at[3])
    for zz in range(depth):
        slot = x_all.at[x, zz]
        sent(slot, x_send.at[1, zz])
        sent(r1.at[0], e_send.at[zz])
    for n in range(depth - 1):
        sent(x_all.at[0, 0], x_send.at[0, n])
    for p in straight + crossed:
        sent(block, w_send.at[p])
    for p in range(spread):
        sent(block, f_send.at[0, p])
        sent(block, f_send.at[1, p])
        sent(block, g_send.at[p])
    for k in range(1, members):
        sent(rs.at[0], p_send.at[(j + k) % members])
    for zz in ends:
        sent(s2.at[0], z_send.at[zz])


def fused_shards(*args):
    (res, qn, kn, vn, on, gn, qb, kb, vb, ob, gb, opn, opb, gain, gw, uw, dw) = args
    spread, members = lax.axis_size("sp"), lax.axis_size("tp")
    rows, wide = res.shape
    own, depth = rows // members, spread // 2
    chan, hid = gw.shape
    piece = hid // spread
    kvw = 2 * (kn.shape[1] + kb.shape[1])
    bf16, f32 = jnp.bfloat16, jnp.float32
    state_rows = DH_A + DH_B
    v = pltpu.VMEM
    dma = pltpu.SemaphoreType.DMA
    scratch = [
        v((spread // 2, rows, kvw), bf16),
        v((spread // 2, 2, 16, rows), f32),
        v((2, 16, rows), f32),
        v((3, hid, chan), bf16),
        v((3, members, piece, wide), bf16),
        v((members, own, wide), bf16),
        v((members, own, wide), bf16),
        v((2, depth, own, wide), bf16),
        v((2, depth, own, wide), bf16),
        v((depth, own, wide), bf16),
        v((depth, own, wide), bf16),
        v((depth, own, wide), bf16),
        v((state_rows, 128), bf16),
        v((8, state_rows + rows), f32),
        v((2, state_rows, 128), bf16),
        v((2, 8, state_rows + rows), f32),
        dma((spread // 2,)),
        dma((spread // 2,)),
        dma((spread // 2,)),
        dma((spread // 2,)),
        dma((spread,)),
        dma((spread,)),
        dma((2, spread)),
        dma((2, spread)),
        dma((spread,)),
        dma((spread,)),
        dma((members,)),
        dma((members,)),
        dma((2, depth)),
        dma((2, depth)),
        dma((depth,)),
        dma((depth,)),
        dma((depth,)),
        dma((depth,)),
        dma((4,)),
        dma((2,)),
        dma((2,)),
    ]
    geometry = (spread, members, wide, gn.shape[1], gb.shape[1])
    return pl.pallas_call(
        functools.partial(fused_kernel, geometry),
        out_shape=jax.ShapeDtypeStruct((own, wide), bf16),
        in_specs=[pl.BlockSpec(memory_space=pltpu.VMEM)] * 17,
        out_specs=pl.BlockSpec(memory_space=pltpu.VMEM),
        scratch_shapes=scratch,
        compiler_params=pltpu.CompilerParams(
            collective_id=0, has_side_effects=True, vmem_limit_bytes=60 * 1024 * 1024
        ),
        name="fused",
    )(res, qn, kn, vn, on, gn, qb, kb, vb, ob, gb, opn, opb, gain, gw, uw, dw)


def pick(*args):
    res, kn, gn, gb, gw = args[0], args[2], args[5], args[10], args[14]
    spread, members = lax.axis_size("sp"), lax.axis_size("tp")
    rows = res.shape[0]
    chan, hid = gw.shape
    fits = (
        spread == 8
        and members == 4
        and rows == 128
        and spread * rows <= 2048
        and chan % 128 == 0
        and hid % (16 * spread) == 0
        and hid % 128 == 0
        and (gn.shape[1], gb.shape[1]) == (2, 1)
        and kn.shape[1] == 2 * DH_A
        and DH_A == 128
        and DH_B == 256
    )
    return fused_shards(*args) if fits else shards(*args)


def solution(mesh):
    in_specs = (
        P("sp", None),
        P("sp", "tp"),
        P("sp", "tp"),
        P("sp", "tp"),
        P("sp", "tp"),
        P(None, "tp", "sp"),
        P("sp", "tp"),
        P("sp", "tp"),
        P("sp", "tp"),
        P("sp", "tp"),
        P(None, "tp", "sp"),
        P("tp", None),
        P("tp", None),
        P(),
        P("sp", "tp"),
        P("sp", "tp"),
        P("sp", "tp"),
    )
    out_specs = P(("sp", "tp"), None)
    return jax.shard_map(pick, mesh=mesh, in_specs=in_specs, out_specs=out_specs, check_vma=False)
```

```python
import functools

import jax
import jax.numpy as jnp
from jax import lax
from jax.experimental import pallas as pl
from jax.experimental.pallas import tpu as pltpu
from jax.sharding import PartitionSpec as P

DH_A = 128
DH_B = 256

EPSILON = 1e-06
FAR = -1e30
MESH = pl.DeviceIdType.MESH


def direction_columns(in_gate, log_forget, reverse):
    place, length = lax.axis_index("sp"), lax.axis_size("sp")
    cumulative = lax.cumsum(log_forget, axis=1, reverse=reverse)
    total = cumulative[:, 0] if reverse else cumulative[:, -1]
    toward_end = total[:, None] - cumulative + in_gate
    packed = jnp.concatenate([toward_end, total[:, None]], axis=1)
    every = lax.all_gather(packed, "sp")
    ends, totals = every[:, :, :-1], every[:, :, -1]
    index = jnp.arange(length)
    if reverse:
        between = (index[None, :] > place) & (index[None, :] < index[:, None])
        valid = index > place
    else:
        between = (index[None, :] < place) & (index[None, :] > index[:, None])
        valid = index < place
    offset = jnp.sum(jnp.where(between[:, :, None], totals[None], 0.0), axis=1)
    columns = jnp.where(valid[:, None, None], offset[:, :, None] + ends, FAR)
    own = (in_gate - cumulative)[None]
    columns = jnp.where((index == place)[:, None, None], own, columns)
    return jnp.moveaxis(columns, 0, 1).reshape(in_gate.shape[0], -1)


def group_cell(query, keys, values, outgate, gates, width):
    rows, every = query.shape[0], keys.shape[0]
    place = lax.axis_index("sp")
    heads = query.shape[1] // width
    q = query.reshape(rows, heads, width)
    k = keys.reshape(every, heads, width)
    v = values.reshape(every, heads, width)
    scores = jnp.einsum("thd,shd->hts", q, k, preferred_element_type=jnp.float32) * width ** (-0.5)
    t_at = (place * rows + jnp.arange(rows))[:, None]
    s_at = jnp.arange(every)[None, :]
    summed = 0.0
    for direction in range(2):
        columns = direction_columns(
            gates[direction], jax.nn.log_sigmoid(gates[2 + direction]), direction == 1
        )
        mask = s_at >= t_at if direction else s_at <= t_at
        log_weight = jnp.where(mask[None], columns[:, None, :], FAR)
        top = jnp.max(log_weight, axis=2, keepdims=True)
        weighted = jnp.exp(log_weight - top) * scores
        den = jnp.sum(weighted, axis=2)
        num = jnp.einsum(
            "hts,shd->thd", weighted.astype(jnp.bfloat16), v, preferred_element_type=jnp.float32
        )
        summed = summed + num / jnp.maximum(jnp.abs(jnp.transpose(den)), 1.0)[:, :, None]
    normed = summed * lax.rsqrt(jnp.mean(summed * summed, axis=2, keepdims=True) + EPSILON)
    return (normed.reshape(rows, -1) * jax.nn.sigmoid(outgate.astype(jnp.float32))).astype(
        jnp.bfloat16
    )


def shards(
    residual,
    query_narrow,
    keys_narrow,
    values_narrow,
    outgate_narrow,
    gates_narrow,
    query_broad,
    keys_broad,
    values_broad,
    outgate_broad,
    gates_broad,
    outproj_narrow,
    outproj_broad,
    norm_gain,
    gate_weight,
    up_weight,
    down_weight,
):
    spread = lax.axis_size("sp")
    channels, hidden_own = gate_weight.shape
    stacked = jnp.stack([gate_weight.T, up_weight.T, down_weight.T])
    pieces = stacked.reshape(3, spread, hidden_own // spread, channels)
    pieces = lax.all_to_all(pieces, "sp", split_axis=1, concat_axis=1)
    weights = jnp.swapaxes(pieces, 1, 2).reshape(3, hidden_own // spread, -1)

    narrow, broad = keys_narrow.shape[1], keys_broad.shape[1]
    memory = lax.all_gather(
        jnp.concatenate([keys_narrow, values_narrow, keys_broad, values_broad], axis=1),
        "sp",
        axis=0,
        tiled=True,
    )
    kn, vn = memory[:, :narrow], memory[:, narrow : 2 * narrow]
    kb, vb = memory[:, 2 * narrow : 2 * narrow + broad], memory[:, 2 * narrow + broad :]
    cell_narrow = group_cell(query_narrow, kn, vn, outgate_narrow, gates_narrow, DH_A)
    cell_broad = group_cell(query_broad, kb, vb, outgate_broad, gates_broad, DH_B)

    own_count = residual.shape[0] // lax.axis_size("tp")
    proj = lax.psum_scatter(
        (
            jnp.dot(cell_narrow, outproj_narrow, preferred_element_type=jnp.float32)
            + jnp.dot(cell_broad, outproj_broad, preferred_element_type=jnp.float32)
        ).astype(jnp.bfloat16),
        "tp",
        scatter_dimension=0,
        tiled=True,
    ).astype(jnp.float32)
    offset = lax.axis_index("tp") * own_count
    stream = lax.dynamic_slice_in_dim(residual, offset, own_count, 0).astype(jnp.float32) + proj
    scaled = stream * lax.rsqrt(jnp.mean(stream * stream, axis=1, keepdims=True) + EPSILON)
    normed = (scaled * norm_gain.astype(jnp.float32)).astype(jnp.bfloat16)
    normed = lax.all_gather(normed, ("sp", "tp"), axis=0, tiled=True)
    nt = (((1,), (1,)), ((), ()))
    gate = lax.dot_general(normed, weights[0], nt, preferred_element_type=jnp.float32)
    upward = lax.dot_general(normed, weights[1], nt, preferred_element_type=jnp.float32)
    hidden = (jax.nn.silu(gate) * upward).astype(jnp.bfloat16)
    partial_value = jnp.dot(hidden, weights[2], preferred_element_type=jnp.float32)
    ffn = lax.psum_scatter(
        partial_value.astype(jnp.bfloat16), ("sp", "tp"), scatter_dimension=0, tiled=True
    ).astype(jnp.float32)
    return (stream + 0.5 * ffn).astype(jnp.bfloat16)


def fused_kernel(geometry, *refs):
    spread, members, wide, narrow_heads, broad_heads = geometry
    (res, qn, kn, vn, on, gn, qb, kb, vb, ob, gb, opn, opb, gain, gw, uw, dw, out) = refs[:18]
    (kv_all, info, gates, wt, w_all, pp, rs, x_all, part, r1, s2, r3) = refs[18:30]
    (st_out, sn_out, st_in, sn_in) = refs[30:34]
    (kv_send, kv_recv, in_send, in_recv, w_send, w_recv, f_send, f_recv, g_send, g_recv) = refs[34:44]
    (p_send, p_recv, x_send, x_recv, e_send, e_recv, z_send, z_recv) = refs[44:52]
    (st_send, st_recv, sn_recv) = refs[52:55]
    rows = res.shape[0]
    own = rows // members
    depth = spread // 2
    chan, hid = gw.shape
    piece = hid // spread
    ca, cb = kn.shape[1], kb.shape[1]
    i, j = lax.axis_index("sp"), lax.axis_index("tp")
    z, x = i // 2, i % 2
    y, c = j // 2, j % 2
    ox = 1 - x
    size = spread // 2
    half, local = i // size, i % size
    f32, bf16 = jnp.float32, jnp.bfloat16
    sibling, x_peer = (i, j + 1 - 2 * c), (2 * z + ox, j)
    across = (1 - y) * 2 + c
    y_peer = (i, across)

    def ranked(n):
        pick = 0
        for a in range(depth):
            others = sorted(
                (b for b in range(depth) if b != a),
                key=lambda b: (abs(a - b), (a < depth // 2) == (b < depth // 2)),
            )
            pick = pick + jnp.where(z == a, others[n], 0)
        return pick

    def send(src, dst, s_sem, r_sem, to):
        copy = pltpu.make_async_remote_copy(
            src_ref=src, dst_ref=dst, send_sem=s_sem, recv_sem=r_sem, device_id=to, device_id_type=MESH
        )
        copy.start()
        return copy

    def arrived(ref, sem):
        pltpu.make_async_remote_copy(
            src_ref=ref, dst_ref=ref, send_sem=sem, recv_sem=sem, device_id=(i, j), device_id_type=MESH
        ).wait_recv()

    def sent(ref, sem, cond=None):
        def wait():
            pltpu.make_async_remote_copy(
                src_ref=ref, dst_ref=ref, send_sem=sem, recv_sem=sem, device_id=(i, j), device_id_type=MESH
            ).wait_send()

        if cond is None:
            wait()
        else:
            pl.when(cond)(wait)

    barrier = pltpu.get_barrier_semaphore()
    for k in range(1, spread):
        pl.semaphore_signal(barrier, inc=1, device_id=((i + k) % spread, j), device_id_type=MESH)
    for k in range(1, members):
        pl.semaphore_signal(barrier, inc=1, device_id=(i, (j + k) % members), device_id_type=MESH)

    kv_all[local, :, 0:ca] = kn[...]
    kv_all[local, :, ca : 2 * ca] = vn[...]
    kv_all[local, :, 2 * ca : 2 * ca + cb] = kb[...]
    kv_all[local, :, 2 * ca + cb : 2 * ca + 2 * cb] = vb[...]
    gates[...] = jnp.zeros_like(gates)
    for role in range(4):
        at = 8 * (role % 2)
        gates[role // 2, at : at + narrow_heads, :] = gn[role]
        gates[role // 2, at + narrow_heads : at + narrow_heads + broad_heads, :] = gb[role]
    in_gate, pre = gates[0], gates[1]
    forget = jnp.minimum(pre, 0.0) - jnp.log1p(jnp.exp(-jnp.abs(pre)))
    r_at = lax.broadcasted_iota(jnp.int32, (rows, rows), 0)
    c_at = lax.broadcasted_iota(jnp.int32, (rows, rows), 1)
    run = lambda m: jnp.dot(
        forget, m.astype(f32), preferred_element_type=f32, precision=lax.Precision.HIGHEST
    )
    forward_row = lax.broadcasted_iota(jnp.int32, in_gate.shape, 0) < 8
    cumulative = jnp.where(forward_row, run(r_at <= c_at), run(r_at >= c_at))
    total = jnp.where(
        forward_row,
        jnp.broadcast_to(cumulative[:, rows - 1 : rows], in_gate.shape),
        jnp.broadcast_to(cumulative[:, 0:1], in_gate.shape),
    )
    own_column = in_gate - cumulative
    info[local, 0] = total + own_column
    info[local, 1] = total
    pl.semaphore_wait(barrier, spread + members - 2)

    mates = [(local + k) % size for k in range(1, size)]
    for k, mate in enumerate(mates):
        to = (half * size + mate, j)
        send(kv_all.at[local], kv_all.at[local], kv_send.at[k], kv_recv.at[local], to)
        send(info.at[local], info.at[local], in_send.at[k], in_recv.at[local], to)

    for m, ref in enumerate((gw, uw, dw)):
        for k in range(hid // 128):
            wt[m, k * 128 : (k + 1) * 128, :] = ref[:, k * 128 : (k + 1) * 128].T
    mine = pl.ds(pl.multiple_of(i * piece, 16), piece)

    def w_slot(jj, p):
        return w_all.at[:, jj, :, pl.ds(pl.multiple_of(p * chan, 128), chan)]

    def send_weights(p):
        theirs = pl.ds(pl.multiple_of(p * piece, 16), piece)
        send(wt.at[:, theirs, :], w_slot(j, i), w_send.at[p], w_recv.at[i], (p, j))

    def share_weights(p):
        slot = w_slot(j, p)
        arrived(slot, w_recv.at[p])
        send(slot, slot, f_send.at[0, p], f_recv.at[0, p], sibling)
        send(slot, slot, g_send.at[p], g_recv.at[p], y_peer)

    def share_across(p):
        slot = w_slot(across, p)
        arrived(slot, g_recv.at[p])
        send(slot, slot, f_send.at[1, p], f_recv.at[1, p], sibling)

    columns = pl.ds(pl.multiple_of(i * chan, 128), chan)
    block = wt.at[:, mine, :]
    send(block, w_slot(j, i), g_send.at[i], g_recv.at[i], y_peer)
    send(block, w_slot(j, i), f_send.at[0, i], f_recv.at[0, i], sibling)
    w_all[:, j, :, columns] = wt[:, mine, :]
    straight = [2 * ranked(n) + x for n in range(depth - 1)]
    crossed = [2 * z + ox] + [2 * ranked(n) + ox for n in range(depth - 1)]
    middle = jnp.logical_or(z == depth // 2 - 1, z == depth // 2)

    @pl.when(middle)
    def _():
        for p in (straight[2], straight[0], straight[1]):
            send_weights(p)

    @pl.when(jnp.logical_not(middle))
    def _():
        send_weights(straight[1])

    send_weights(crossed[0])

    @pl.when(middle)
    def _():
        send_weights(crossed[2])

    in_turn = [
        jnp.where(middle, a, b)
        for a, b in zip(
            [straight[0], straight[2], crossed[0], straight[1], crossed[1], crossed[3], crossed[2]],
            [straight[1], crossed[0], straight[0], crossed[1], straight[2], crossed[3], crossed[2]],
        )
    ]

    for mate in mates:
        arrived(kv_all.at[mate], kv_recv.at[mate])
        arrived(info.at[mate], in_recv.at[mate])

    before, after = [], [None] * size
    passed = jnp.zeros_like(total)
    for k in range(size):
        before.append(passed)
        passed = passed + info[k, 1]
    passed = jnp.zeros_like(total)
    for k in reversed(range(size)):
        after[k] = passed
        passed = passed + info[k, 1]
    to_end = jnp.concatenate(
        [info[k, 0] + jnp.where(forward_row, after[k], before[k]) for k in range(size)], axis=1
    )
    to_end = jnp.where(half == 0, to_end[0:8], to_end[8:16])
    end_max = jnp.max(to_end, axis=1, keepdims=True)
    share = jnp.transpose(
        jnp.concatenate([jnp.exp(to_end - end_max), jnp.zeros((rows - 8, size * rows), f32)], axis=0)
    )
    share_a = jnp.where(x == 0, share[:, 0:1], share[:, 1:2])
    share_b = share[:, narrow_heads : narrow_heads + 1]
    wa, wb = ca // narrow_heads, cb // 2

    def kv_lanes(start, width):
        return kv_all[:, :, pl.ds(pl.multiple_of(start, 128), width)].reshape(size * rows, width)

    tn = (((0,), (0,)), ((), ()))
    keys_a, keys_b = kv_lanes(x * wa, wa), kv_lanes(2 * ca, cb)
    values_a = (share_a * kv_lanes(ca + x * wa, wa).astype(f32)).astype(bf16)
    values_b = (share_b * kv_lanes(2 * ca + cb + x * wb, wb).astype(f32)).astype(bf16)
    st_out[0:wa, :] = lax.dot_general(keys_a, values_a, tn, preferred_element_type=f32).astype(bf16)
    st_out[wa : wa + cb, :] = lax.dot_general(keys_b, values_b, tn, preferred_element_type=f32).astype(bf16)
    norm_a = jnp.sum(share_a * keys_a.astype(f32), axis=0, keepdims=True)
    norm_b = jnp.sum(share_b * keys_b.astype(f32), axis=0, keepdims=True)
    sn_out[:, 0:wa] = jnp.broadcast_to(norm_a, (8, wa))
    sn_out[:, wa : wa + cb] = jnp.broadcast_to(norm_b, (8, cb))
    sn_out[:, wa + cb :] = jnp.broadcast_to(end_max, (8, rows))
    mirror = ((i + size) % spread, j)
    send(sn_out, sn_in.at[x], st_send.at[1], sn_recv.at[x], mirror)
    send(st_out, st_in.at[x], st_send.at[0], st_recv.at[x], mirror)

    @pl.when(middle)
    def _():
        for p in (crossed[1], crossed[3]):
            send_weights(p)

    @pl.when(jnp.logical_not(middle))
    def _():
        send_weights(straight[0])

    share_weights(in_turn[0])
    arrived(sn_in.at[x], sn_recv.at[x])
    arrived(st_in.at[x], st_recv.at[x])
    send(sn_in.at[x], sn_in.at[x], st_send.at[3], sn_recv.at[x], x_peer)
    send(st_in.at[x], st_in.at[x], st_send.at[2], st_recv.at[x], x_peer)

    @pl.when(jnp.logical_not(middle))
    def _():
        for p in (straight[2], crossed[2], crossed[3], crossed[1]):
            send_weights(p)

    share_weights(in_turn[1])
    arrived(sn_in.at[ox], sn_recv.at[ox])
    arrived(st_in.at[ox], st_recv.at[ox])

    pieces = [None] * size
    forward_sum = jnp.zeros_like(total)
    ahead = [None] * size
    for k in reversed(range(size)):
        ahead[k] = forward_sum
        forward_sum = forward_sum + jnp.where(k < local, info[k, 1], 0.0)
    backward_sum = jnp.zeros_like(total)
    for k in range(size):
        reach = jnp.where(forward_row, ahead[k], backward_sum) + info[k, 0]
        seen = jnp.logical_or(
            jnp.logical_and(forward_row, k < local),
            jnp.logical_and(jnp.logical_not(forward_row), k > local),
        )
        pieces[k] = jnp.where(k == local, own_column, jnp.where(seen, reach, FAR))
        backward_sum = backward_sum + jnp.where(k > local, info[k, 1], 0.0)
    column = jnp.concatenate(pieces, axis=1)
    past = sn_in[x, :, wa + cb :] + jnp.where(half == 1, forward_sum[0:8], backward_sum[8:16])
    t_at = lax.broadcasted_iota(jnp.int32, (rows, size * rows), 0) + local * rows
    s_at = lax.broadcasted_iota(jnp.int32, (rows, size * rows), 1)
    masks = (s_at <= t_at, s_at >= t_at)
    nt = (((1,), (1,)), ((), ()))
    proj = jnp.zeros((rows, res.shape[1]), f32)
    heads = [(qn, on, opn, 0, ca, h, ca // narrow_heads, h) for h in range(narrow_heads)]
    heads += [
        (qb, ob, opb, 2 * ca, cb, h, cb // broad_heads, narrow_heads + h) for h in range(broad_heads)
    ]
    for query, outgate, outproj, base, group, h, width, row in heads:
        lanes = slice(h * width, (h + 1) * width)
        keys = kv_all[:, :, base + h * width : base + (h + 1) * width].reshape(size * rows, width)
        vals = kv_all[:, :, base + group + h * width : base + group + (h + 1) * width].reshape(
            size * rows, width
        )
        queries = query[:, lanes]
        scores = lax.dot_general(queries, keys, nt, preferred_element_type=f32) * width ** (-0.5)
        if row < narrow_heads:
            memory, normer = st_in[row, 0:wa, :], sn_in[row, 0:1, 0:wa]
        else:
            memory = jnp.concatenate([st_in[0, wa:, :], st_in[1, wa:, :]], axis=1)
            normer = sn_in[0, 0:1, wa : wa + cb]
        recalled = jnp.dot(queries, memory, preferred_element_type=f32) * width ** (-0.5)
        recall_den = jnp.sum(queries.astype(f32) * normer, axis=1, keepdims=True) * width ** (-0.5)
        summed = jnp.zeros((rows, width), f32)
        for direction in range(2):
            at = 8 * direction + row
            weight = jnp.where(
                masks[direction],
                jnp.broadcast_to(column[at : at + 1, :], scores.shape),
                FAR,
            )
            carried = jnp.where(half == 1 - direction, past[row : row + 1, 0:1], FAR)
            top = jnp.maximum(jnp.max(weight, axis=1, keepdims=True), carried)
            kept = jnp.exp(carried - top)
            p = jnp.exp(weight - top) * scores
            den = jnp.sum(p, axis=1, keepdims=True) + kept * recall_den
            num = jnp.dot(p.astype(bf16), vals, preferred_element_type=f32) + kept * recalled
            summed = summed + num / jnp.maximum(jnp.abs(den), 1.0)
        normed = summed * lax.rsqrt(jnp.mean(summed * summed, axis=1, keepdims=True) + EPSILON)
        opened = 1.0 / (1.0 + jnp.exp(-outgate[:, lanes].astype(f32)))
        cell = (normed * opened).astype(bf16)
        proj = proj + jnp.dot(cell, outproj[lanes, :], preferred_element_type=f32)
    pp[...] = proj.astype(bf16).reshape(pp.shape)

    for k in range(1, members):
        q = (j + k) % members
        send(pp.at[q], rs.at[j], p_send.at[q], p_recv.at[j], (i, q))
    share_weights(in_turn[2])
    stream = res[pl.ds(pl.multiple_of(j * own, own), own), :].astype(f32) + pp[j].astype(f32)
    for k in range(1, members):
        q = (j + k) % members
        arrived(rs.at[q], p_recv.at[q])
        stream = stream + rs[q].astype(f32)
    scaled = stream * lax.rsqrt(jnp.mean(stream * stream, axis=1, keepdims=True) + EPSILON)
    x_all[x, z] = (scaled * gain[...].astype(f32).reshape(1, wide)).astype(bf16)

    def pass_x(zz, sem, to):
        slot = x_all.at[x, zz]
        send(slot, slot, sem, x_recv.at[x, zz], to)

    def x_arrived(xx, zz):
        arrived(x_all.at[xx, zz], x_recv.at[xx, zz])

    for n in range(depth - 1):
        pass_x(z, x_send.at[0, n], (2 * ranked(n) + x, j))
    pass_x(z, x_send.at[1, z], x_peer)

    def forward_x(n):
        zz = ranked(n)
        x_arrived(x, zz)
        pass_x(zz, x_send.at[1, zz], x_peer)

    share_weights(in_turn[3])
    share_across(i)
    share_across(in_turn[0])
    share_weights(in_turn[4])
    share_across(in_turn[1])
    share_weights(in_turn[5])
    share_across(in_turn[2])
    share_weights(in_turn[6])
    share_across(in_turn[3])
    forward_x(0)
    forward_x(1)
    forward_x(2)
    share_across(in_turn[4])
    share_across(in_turn[5])
    share_across(in_turn[6])
    for zz in range(depth):
        x_arrived(ox, zz)
    other, other_across = 2 * y + 1 - c, 2 * (1 - y) + 1 - c
    for p in [i] + in_turn:
        arrived(w_slot(other, p), f_recv.at[0, p])
        arrived(w_slot(other_across, p), f_recv.at[1, p])

    units = members * piece

    def chunk(xx):
        a = x_all[xx].reshape(depth * own, -1)
        gate = lax.dot_general(a, w_all[0].reshape(units, -1), nt, preferred_element_type=f32)
        up = lax.dot_general(a, w_all[1].reshape(units, -1), nt, preferred_element_type=f32)
        hidden = (gate / (1.0 + jnp.exp(-gate)) * up).astype(bf16)
        got = jnp.dot(hidden, w_all[2].reshape(units, -1), preferred_element_type=f32)
        part[xx] = got.astype(bf16).reshape(depth, own, -1)

    ends = [(z + depth // 2) % depth] + [(z + k) % depth for k in range(1, depth) if 2 * k != depth]
    chunk(ox)
    for zz in ends + [z]:
        send(part.at[ox, zz], r1.at[zz], e_send.at[zz], e_recv.at[zz], x_peer)
    chunk(x)
    for zz in ends:
        arrived(r1.at[zz], e_recv.at[zz])
        s2[zz] = (part[x, zz].astype(f32) + r1[zz].astype(f32)).astype(bf16)
        send(s2.at[zz], r3.at[z], z_send.at[zz], z_recv.at[z], (2 * zz + x, j))
    arrived(r1.at[z], e_recv.at[z])
    ffn = part[x, z].astype(f32) + r1[z].astype(f32)
    for zz in ends:
        arrived(r3.at[zz], z_recv.at[zz])
        ffn = ffn + r3[zz].astype(f32)
    out[...] = (stream + 0.5 * ffn).astype(out.dtype)

    for k in range(size - 1):
        sent(kv_all.at[0], kv_send.at[k])
        sent(info.at[0], in_send.at[k])
    sent(st_out, st_send.at[0])
    sent(sn_out, st_send.at[1])
    sent(st_out, st_send.at[2])
    sent(sn_out, st_send.at[3])
    for zz in range(depth):
        slot = x_all.at[x, zz]
        sent(slot, x_send.at[1, zz])
        sent(r1.at[0], e_send.at[zz])
    for n in range(depth - 1):
        sent(x_all.at[0, 0], x_send.at[0, n])
    for p in straight + crossed:
        sent(block, w_send.at[p])
    for p in range(spread):
        sent(block, f_send.at[0, p])
        sent(block, f_send.at[1, p])
        sent(block, g_send.at[p])
    for k in range(1, members):
        sent(rs.at[0], p_send.at[(j + k) % members])
    for zz in ends:
        sent(s2.at[0], z_send.at[zz])


def fused_shards(*args):
    (res, qn, kn, vn, on, gn, qb, kb, vb, ob, gb, opn, opb, gain, gw, uw, dw) = args
    spread, members = lax.axis_size("sp"), lax.axis_size("tp")
    rows, wide = res.shape
    own, depth = rows // members, spread // 2
    chan, hid = gw.shape
    piece = hid // spread
    kvw = 2 * (kn.shape[1] + kb.shape[1])
    bf16, f32 = jnp.bfloat16, jnp.float32
    state_rows = DH_A + DH_B
    v = pltpu.VMEM
    dma = pltpu.SemaphoreType.DMA
    scratch = [
        v((spread // 2, rows, kvw), bf16),
        v((spread // 2, 2, 16, rows), f32),
        v((2, 16, rows), f32),
        v((3, hid, chan), bf16),
        v((3, members, piece, wide), bf16),
        v((members, own, wide), bf16),
        v((members, own, wide), bf16),
        v((2, depth, own, wide), bf16),
        v((2, depth, own, wide), bf16),
        v((depth, own, wide), bf16),
        v((depth, own, wide), bf16),
        v((depth, own, wide), bf16),
        v((state_rows, 128), bf16),
        v((8, state_rows + rows), f32),
        v((2, state_rows, 128), bf16),
        v((2, 8, state_rows + rows), f32),
        dma((spread // 2,)),
        dma((spread // 2,)),
        dma((spread // 2,)),
        dma((spread // 2,)),
        dma((spread,)),
        dma((spread,)),
        dma((2, spread)),
        dma((2, spread)),
        dma((spread,)),
        dma((spread,)),
        dma((members,)),
        dma((members,)),
        dma((2, depth)),
        dma((2, depth)),
        dma((depth,)),
        dma((depth,)),
        dma((depth,)),
        dma((depth,)),
        dma((4,)),
        dma((2,)),
        dma((2,)),
    ]
    geometry = (spread, members, wide, gn.shape[1], gb.shape[1])
    return pl.pallas_call(
        functools.partial(fused_kernel, geometry),
        out_shape=jax.ShapeDtypeStruct((own, wide), bf16),
        in_specs=[pl.BlockSpec(memory_space=pltpu.VMEM)] * 17,
        out_specs=pl.BlockSpec(memory_space=pltpu.VMEM),
        scratch_shapes=scratch,
        compiler_params=pltpu.CompilerParams(
            collective_id=0, has_side_effects=True, vmem_limit_bytes=60 * 1024 * 1024
        ),
        name="fused",
    )(res, qn, kn, vn, on, gn, qb, kb, vb, ob, gb, opn, opb, gain, gw, uw, dw)


def pick(*args):
    res, kn, gn, gb, gw = args[0], args[2], args[5], args[10], args[14]
    spread, members = lax.axis_size("sp"), lax.axis_size("tp")
    rows = res.shape[0]
    chan, hid = gw.shape
    fits = (
        spread == 8
        and members == 4
        and rows == 128
        and spread * rows <= 2048
        and chan % 128 == 0
        and hid % (16 * spread) == 0
        and hid % 128 == 0
        and (gn.shape[1], gb.shape[1]) == (2, 1)
        and kn.shape[1] == 2 * DH_A
        and DH_A == 128
        and DH_B == 256
    )
    return fused_shards(*args) if fits else shards(*args)


def solution(mesh):
    in_specs = (
        P("sp", None),
        P("sp", "tp"),
        P("sp", "tp"),
        P("sp", "tp"),
        P("sp", "tp"),
        P(None, "tp", "sp"),
        P("sp", "tp"),
        P("sp", "tp"),
        P("sp", "tp"),
        P("sp", "tp"),
        P(None, "tp", "sp"),
        P("tp", None),
        P("tp", None),
        P(),
        P("sp", "tp"),
        P("sp", "tp"),
        P("sp", "tp"),
    )
    out_specs = P(("sp", "tp"), None)
    return jax.shard_map(pick, mesh=mesh, in_specs=in_specs, out_specs=out_specs, check_vma=False)
```

```python
import functools

import jax
import jax.numpy as jnp
from jax import lax
from jax.experimental import pallas as pl
from jax.experimental.pallas import tpu as pltpu
from jax.sharding import PartitionSpec as P

DH_A = 128
DH_B = 256

EPSILON = 1e-06
FAR = -1e30
MESH = pl.DeviceIdType.MESH


def direction_columns(in_gate, log_forget, reverse):
    place, length = lax.axis_index("sp"), lax.axis_size("sp")
    cumulative = lax.cumsum(log_forget, axis=1, reverse=reverse)
    total = cumulative[:, 0] if reverse else cumulative[:, -1]
    toward_end = total[:, None] - cumulative + in_gate
    packed = jnp.concatenate([toward_end, total[:, None]], axis=1)
    every = lax.all_gather(packed, "sp")
    ends, totals = every[:, :, :-1], every[:, :, -1]
    index = jnp.arange(length)
    if reverse:
        between = (index[None, :] > place) & (index[None, :] < index[:, None])
        valid = index > place
    else:
        between = (index[None, :] < place) & (index[None, :] > index[:, None])
        valid = index < place
    offset = jnp.sum(jnp.where(between[:, :, None], totals[None], 0.0), axis=1)
    columns = jnp.where(valid[:, None, None], offset[:, :, None] + ends, FAR)
    own = (in_gate - cumulative)[None]
    columns = jnp.where((index == place)[:, None, None], own, columns)
    return jnp.moveaxis(columns, 0, 1).reshape(in_gate.shape[0], -1)


def group_cell(query, keys, values, outgate, gates, width):
    rows, every = query.shape[0], keys.shape[0]
    place = lax.axis_index("sp")
    heads = query.shape[1] // width
    q = query.reshape(rows, heads, width)
    k = keys.reshape(every, heads, width)
    v = values.reshape(every, heads, width)
    scores = jnp.einsum("thd,shd->hts", q, k, preferred_element_type=jnp.float32) * width ** (-0.5)
    t_at = (place * rows + jnp.arange(rows))[:, None]
    s_at = jnp.arange(every)[None, :]
    summed = 0.0
    for direction in range(2):
        columns = direction_columns(
            gates[direction], jax.nn.log_sigmoid(gates[2 + direction]), direction == 1
        )
        mask = s_at >= t_at if direction else s_at <= t_at
        log_weight = jnp.where(mask[None], columns[:, None, :], FAR)
        top = jnp.max(log_weight, axis=2, keepdims=True)
        weighted = jnp.exp(log_weight - top) * scores
        den = jnp.sum(weighted, axis=2)
        num = jnp.einsum(
            "hts,shd->thd", weighted.astype(jnp.bfloat16), v, preferred_element_type=jnp.float32
        )
        summed = summed + num / jnp.maximum(jnp.abs(jnp.transpose(den)), 1.0)[:, :, None]
    normed = summed * lax.rsqrt(jnp.mean(summed * summed, axis=2, keepdims=True) + EPSILON)
    return (normed.reshape(rows, -1) * jax.nn.sigmoid(outgate.astype(jnp.float32))).astype(
        jnp.bfloat16
    )


def shards(
    residual,
    query_narrow,
    keys_narrow,
    values_narrow,
    outgate_narrow,
    gates_narrow,
    query_broad,
    keys_broad,
    values_broad,
    outgate_broad,
    gates_broad,
    outproj_narrow,
    outproj_broad,
    norm_gain,
    gate_weight,
    up_weight,
    down_weight,
):
    spread = lax.axis_size("sp")
    channels, hidden_own = gate_weight.shape
    stacked = jnp.stack([gate_weight.T, up_weight.T, down_weight.T])
    pieces = stacked.reshape(3, spread, hidden_own // spread, channels)
    pieces = lax.all_to_all(pieces, "sp", split_axis=1, concat_axis=1)
    weights = jnp.swapaxes(pieces, 1, 2).reshape(3, hidden_own // spread, -1)

    narrow, broad = keys_narrow.shape[1], keys_broad.shape[1]
    memory = lax.all_gather(
        jnp.concatenate([keys_narrow, values_narrow, keys_broad, values_broad], axis=1),
        "sp",
        axis=0,
        tiled=True,
    )
    kn, vn = memory[:, :narrow], memory[:, narrow : 2 * narrow]
    kb, vb = memory[:, 2 * narrow : 2 * narrow + broad], memory[:, 2 * narrow + broad :]
    cell_narrow = group_cell(query_narrow, kn, vn, outgate_narrow, gates_narrow, DH_A)
    cell_broad = group_cell(query_broad, kb, vb, outgate_broad, gates_broad, DH_B)

    own_count = residual.shape[0] // lax.axis_size("tp")
    proj = lax.psum_scatter(
        (
            jnp.dot(cell_narrow, outproj_narrow, preferred_element_type=jnp.float32)
            + jnp.dot(cell_broad, outproj_broad, preferred_element_type=jnp.float32)
        ).astype(jnp.bfloat16),
        "tp",
        scatter_dimension=0,
        tiled=True,
    ).astype(jnp.float32)
    offset = lax.axis_index("tp") * own_count
    stream = lax.dynamic_slice_in_dim(residual, offset, own_count, 0).astype(jnp.float32) + proj
    scaled = stream * lax.rsqrt(jnp.mean(stream * stream, axis=1, keepdims=True) + EPSILON)
    normed = (scaled * norm_gain.astype(jnp.float32)).astype(jnp.bfloat16)
    normed = lax.all_gather(normed, ("sp", "tp"), axis=0, tiled=True)
    nt = (((1,), (1,)), ((), ()))
    gate = lax.dot_general(normed, weights[0], nt, preferred_element_type=jnp.float32)
    upward = lax.dot_general(normed, weights[1], nt, preferred_element_type=jnp.float32)
    hidden = (jax.nn.silu(gate) * upward).astype(jnp.bfloat16)
    partial_value = jnp.dot(hidden, weights[2], preferred_element_type=jnp.float32)
    ffn = lax.psum_scatter(
        partial_value.astype(jnp.bfloat16), ("sp", "tp"), scatter_dimension=0, tiled=True
    ).astype(jnp.float32)
    return (stream + 0.5 * ffn).astype(jnp.bfloat16)


def fused_kernel(geometry, *refs):
    spread, members, wide, narrow_heads, broad_heads = geometry
    held, out = refs[:17], refs[17]
    (kv_all, info, gates, wt, w_all, pp, rs, x_all, part, r1, s2, r3) = refs[18:30]
    (st_out, sn_out, st_in, sn_in) = refs[30:34]
    (kv_send, kv_recv, in_send, in_recv, w_send, w_recv, f_send, f_recv, g_send, g_recv) = refs[34:44]
    (p_send, p_recv, x_send, x_recv, e_send, e_recv, z_send, z_recv) = refs[44:52]
    (st_send, st_recv, sn_recv, load_sem) = refs[52:56]
    (res, qn, on, gn, qb, ob, gb, opn, opb, gain, gw, uw, dw) = refs[56:69]
    rows = res.shape[0]
    own = rows // members
    depth = spread // 2
    chan, hid = gw.shape
    piece = hid // spread
    ca, cb = held[2].shape[1], held[7].shape[1]
    i, j = lax.axis_index("sp"), lax.axis_index("tp")
    z, x = i // 2, i % 2
    y, c = j // 2, j % 2
    ox = 1 - x
    size = spread // 2
    half, local = i // size, i % size
    f32, bf16 = jnp.float32, jnp.bfloat16
    sibling, x_peer = (i, j + 1 - 2 * c), (2 * z + ox, j)
    across = (1 - y) * 2 + c
    y_peer = (i, across)

    def ranked(n):
        pick = 0
        for a in range(depth):
            others = sorted(
                (b for b in range(depth) if b != a),
                key=lambda b: (abs(a - b), (a < depth // 2) == (b < depth // 2)),
            )
            pick = pick + jnp.where(z == a, others[n], 0)
        return pick

    def send(src, dst, s_sem, r_sem, to):
        copy = pltpu.make_async_remote_copy(
            src_ref=src, dst_ref=dst, send_sem=s_sem, recv_sem=r_sem, device_id=to, device_id_type=MESH
        )
        copy.start()
        return copy

    def arrived(ref, sem):
        pltpu.make_async_remote_copy(
            src_ref=ref, dst_ref=ref, send_sem=sem, recv_sem=sem, device_id=(i, j), device_id_type=MESH
        ).wait_recv()

    def sent(ref, sem, cond=None):
        def wait():
            pltpu.make_async_remote_copy(
                src_ref=ref, dst_ref=ref, send_sem=sem, recv_sem=sem, device_id=(i, j), device_id_type=MESH
            ).wait_send()

        if cond is None:
            wait()
        else:
            pl.when(cond)(wait)

    barrier = pltpu.get_barrier_semaphore()
    for k in range(1, spread):
        pl.semaphore_signal(barrier, inc=1, device_id=((i + k) % spread, j), device_id_type=MESH)
    for k in range(1, members):
        pl.semaphore_signal(barrier, inc=1, device_id=(i, (j + k) % members), device_id_type=MESH)

    mine_kv = kv_all.at[local]
    targets = {
        5: gn,
        10: gb,
        2: mine_kv.at[:, 0:ca],
        3: mine_kv.at[:, ca : 2 * ca],
        7: mine_kv.at[:, 2 * ca : 2 * ca + cb],
        8: mine_kv.at[:, 2 * ca + cb : 2 * ca + 2 * cb],
        14: gw,
        15: uw,
        16: dw,
        1: qn,
        6: qb,
        4: on,
        9: ob,
        11: opn,
        12: opb,
        0: res,
        13: gain,
    }
    loads = {n: pltpu.make_async_copy(held[n], ref, load_sem.at[n]) for n, ref in targets.items()}
    for load in loads.values():
        load.start()

    def loaded(*numbers):
        for n in numbers:
            loads[n].wait()

    loaded(5, 10)
    gates[...] = jnp.zeros_like(gates)
    for role in range(4):
        at = 8 * (role % 2)
        gates[role // 2, at : at + narrow_heads, :] = gn[role]
        gates[role // 2, at + narrow_heads : at + narrow_heads + broad_heads, :] = gb[role]
    in_gate, pre = gates[0], gates[1]
    forget = jnp.minimum(pre, 0.0) - jnp.log1p(jnp.exp(-jnp.abs(pre)))
    r_at = lax.broadcasted_iota(jnp.int32, (rows, rows), 0)
    c_at = lax.broadcasted_iota(jnp.int32, (rows, rows), 1)
    run = lambda m: jnp.dot(
        forget, m.astype(f32), preferred_element_type=f32, precision=lax.Precision.HIGHEST
    )
    forward_row = lax.broadcasted_iota(jnp.int32, in_gate.shape, 0) < 8
    cumulative = jnp.where(forward_row, run(r_at <= c_at), run(r_at >= c_at))
    total = jnp.where(
        forward_row,
        jnp.broadcast_to(cumulative[:, rows - 1 : rows], in_gate.shape),
        jnp.broadcast_to(cumulative[:, 0:1], in_gate.shape),
    )
    own_column = in_gate - cumulative
    info[local, 0] = total + own_column
    info[local, 1] = total
    pl.semaphore_wait(barrier, spread + members - 2)

    loaded(2, 3, 7, 8)
    mates = [(local + k) % size for k in range(1, size)]
    for k, mate in enumerate(mates):
        to = (half * size + mate, j)
        send(kv_all.at[local], kv_all.at[local], kv_send.at[k], kv_recv.at[local], to)
        send(info.at[local], info.at[local], in_send.at[k], in_recv.at[local], to)

    loaded(14, 15, 16)
    for m, ref in enumerate((gw, uw, dw)):
        for k in range(hid // 128):
            wt[m, k * 128 : (k + 1) * 128, :] = ref[:, k * 128 : (k + 1) * 128].T
    mine = pl.ds(pl.multiple_of(i * piece, 16), piece)

    def w_slot(jj, p):
        return w_all.at[:, jj, :, pl.ds(pl.multiple_of(p * chan, 128), chan)]

    def send_weights(p):
        theirs = pl.ds(pl.multiple_of(p * piece, 16), piece)
        send(wt.at[:, theirs, :], w_slot(j, i), w_send.at[p], w_recv.at[i], (p, j))

    def share_weights(p):
        slot = w_slot(j, p)
        arrived(slot, w_recv.at[p])
        send(slot, slot, f_send.at[0, p], f_recv.at[0, p], sibling)
        send(slot, slot, g_send.at[p], g_recv.at[p], y_peer)

    def share_across(p):
        slot = w_slot(across, p)
        arrived(slot, g_recv.at[p])
        send(slot, slot, f_send.at[1, p], f_recv.at[1, p], sibling)

    columns = pl.ds(pl.multiple_of(i * chan, 128), chan)
    block = wt.at[:, mine, :]
    send(block, w_slot(j, i), g_send.at[i], g_recv.at[i], y_peer)
    send(block, w_slot(j, i), f_send.at[0, i], f_recv.at[0, i], sibling)
    w_all[:, j, :, columns] = wt[:, mine, :]
    straight = [2 * ranked(n) + x for n in range(depth - 1)]
    crossed = [2 * z + ox] + [2 * ranked(n) + ox for n in range(depth - 1)]
    middle = jnp.logical_or(z == depth // 2 - 1, z == depth // 2)

    @pl.when(middle)
    def _():
        for p in (straight[2], straight[0], straight[1]):
            send_weights(p)

    @pl.when(jnp.logical_not(middle))
    def _():
        send_weights(straight[1])

    send_weights(crossed[0])

    @pl.when(middle)
    def _():
        send_weights(crossed[2])

    in_turn = [
        jnp.where(middle, a, b)
        for a, b in zip(
            [straight[0], straight[2], crossed[0], straight[1], crossed[1], crossed[3], crossed[2]],
            [straight[1], crossed[0], straight[0], crossed[1], straight[2], crossed[3], crossed[2]],
        )
    ]

    for mate in mates:
        arrived(kv_all.at[mate], kv_recv.at[mate])
        arrived(info.at[mate], in_recv.at[mate])

    before, after = [], [None] * size
    passed = jnp.zeros_like(total)
    for k in range(size):
        before.append(passed)
        passed = passed + info[k, 1]
    passed = jnp.zeros_like(total)
    for k in reversed(range(size)):
        after[k] = passed
        passed = passed + info[k, 1]
    to_end = jnp.concatenate(
        [info[k, 0] + jnp.where(forward_row, after[k], before[k]) for k in range(size)], axis=1
    )
    to_end = jnp.where(half == 0, to_end[0:8], to_end[8:16])
    end_max = jnp.max(to_end, axis=1, keepdims=True)
    share = jnp.transpose(
        jnp.concatenate([jnp.exp(to_end - end_max), jnp.zeros((rows - 8, size * rows), f32)], axis=0)
    )
    share_a = jnp.where(x == 0, share[:, 0:1], share[:, 1:2])
    share_b = share[:, narrow_heads : narrow_heads + 1]
    wa, wb = ca // narrow_heads, cb // 2

    def kv_lanes(start, width):
        return kv_all[:, :, pl.ds(pl.multiple_of(start, 128), width)].reshape(size * rows, width)

    tn = (((0,), (0,)), ((), ()))
    keys_a, keys_b = kv_lanes(x * wa, wa), kv_lanes(2 * ca, cb)
    values_a = (share_a * kv_lanes(ca + x * wa, wa).astype(f32)).astype(bf16)
    values_b = (share_b * kv_lanes(2 * ca + cb + x * wb, wb).astype(f32)).astype(bf16)
    st_out[0:wa, :] = lax.dot_general(keys_a, values_a, tn, preferred_element_type=f32).astype(bf16)
    st_out[wa : wa + cb, :] = lax.dot_general(keys_b, values_b, tn, preferred_element_type=f32).astype(bf16)
    norm_a = jnp.sum(share_a * keys_a.astype(f32), axis=0, keepdims=True)
    norm_b = jnp.sum(share_b * keys_b.astype(f32), axis=0, keepdims=True)
    sn_out[:, 0:wa] = jnp.broadcast_to(norm_a, (8, wa))
    sn_out[:, wa : wa + cb] = jnp.broadcast_to(norm_b, (8, cb))
    sn_out[:, wa + cb :] = jnp.broadcast_to(end_max, (8, rows))
    mirror = ((i + size) % spread, j)
    send(sn_out, sn_in.at[x], st_send.at[1], sn_recv.at[x], mirror)
    send(st_out, st_in.at[x], st_send.at[0], st_recv.at[x], mirror)

    @pl.when(middle)
    def _():
        for p in (crossed[1], crossed[3]):
            send_weights(p)

    @pl.when(jnp.logical_not(middle))
    def _():
        send_weights(straight[0])

    share_weights(in_turn[0])
    arrived(sn_in.at[x], sn_recv.at[x])
    arrived(st_in.at[x], st_recv.at[x])
    send(sn_in.at[x], sn_in.at[x], st_send.at[3], sn_recv.at[x], x_peer)
    send(st_in.at[x], st_in.at[x], st_send.at[2], st_recv.at[x], x_peer)

    @pl.when(jnp.logical_not(middle))
    def _():
        for p in (straight[2], crossed[2], crossed[3], crossed[1]):
            send_weights(p)

    share_weights(in_turn[1])
    arrived(sn_in.at[ox], sn_recv.at[ox])
    arrived(st_in.at[ox], st_recv.at[ox])

    loaded(1, 6, 4, 9, 11, 12, 0, 13)
    pieces = [None] * size
    forward_sum = jnp.zeros_like(total)
    ahead = [None] * size
    for k in reversed(range(size)):
        ahead[k] = forward_sum
        forward_sum = forward_sum + jnp.where(k < local, info[k, 1], 0.0)
    backward_sum = jnp.zeros_like(total)
    for k in range(size):
        reach = jnp.where(forward_row, ahead[k], backward_sum) + info[k, 0]
        seen = jnp.logical_or(
            jnp.logical_and(forward_row, k < local),
            jnp.logical_and(jnp.logical_not(forward_row), k > local),
        )
        pieces[k] = jnp.where(k == local, own_column, jnp.where(seen, reach, FAR))
        backward_sum = backward_sum + jnp.where(k > local, info[k, 1], 0.0)
    column = jnp.concatenate(pieces, axis=1)
    past = sn_in[x, :, wa + cb :] + jnp.where(half == 1, forward_sum[0:8], backward_sum[8:16])
    t_at = lax.broadcasted_iota(jnp.int32, (rows, size * rows), 0) + local * rows
    s_at = lax.broadcasted_iota(jnp.int32, (rows, size * rows), 1)
    masks = (s_at <= t_at, s_at >= t_at)
    nt = (((1,), (1,)), ((), ()))
    proj = jnp.zeros((rows, res.shape[1]), f32)
    heads = [(qn, on, opn, 0, ca, h, ca // narrow_heads, h) for h in range(narrow_heads)]
    heads += [
        (qb, ob, opb, 2 * ca, cb, h, cb // broad_heads, narrow_heads + h) for h in range(broad_heads)
    ]
    for query, outgate, outproj, base, group, h, width, row in heads:
        lanes = slice(h * width, (h + 1) * width)
        keys = kv_all[:, :, base + h * width : base + (h + 1) * width].reshape(size * rows, width)
        vals = kv_all[:, :, base + group + h * width : base + group + (h + 1) * width].reshape(
            size * rows, width
        )
        queries = query[:, lanes]
        scores = lax.dot_general(queries, keys, nt, preferred_element_type=f32) * width ** (-0.5)
        if row < narrow_heads:
            memory, normer = st_in[row, 0:wa, :], sn_in[row, 0:1, 0:wa]
        else:
            memory = jnp.concatenate([st_in[0, wa:, :], st_in[1, wa:, :]], axis=1)
            normer = sn_in[0, 0:1, wa : wa + cb]
        recalled = jnp.dot(queries, memory, preferred_element_type=f32) * width ** (-0.5)
        recall_den = jnp.sum(queries.astype(f32) * normer, axis=1, keepdims=True) * width ** (-0.5)
        summed = jnp.zeros((rows, width), f32)
        for direction in range(2):
            at = 8 * direction + row
            weight = jnp.where(
                masks[direction],
                jnp.broadcast_to(column[at : at + 1, :], scores.shape),
                FAR,
            )
            carried = jnp.where(half == 1 - direction, past[row : row + 1, 0:1], FAR)
            top = jnp.maximum(jnp.max(weight, axis=1, keepdims=True), carried)
            kept = jnp.exp(carried - top)
            p = jnp.exp(weight - top) * scores
            den = jnp.sum(p, axis=1, keepdims=True) + kept * recall_den
            num = jnp.dot(p.astype(bf16), vals, preferred_element_type=f32) + kept * recalled
            summed = summed + num / jnp.maximum(jnp.abs(den), 1.0)
        normed = summed * lax.rsqrt(jnp.mean(summed * summed, axis=1, keepdims=True) + EPSILON)
        opened = 1.0 / (1.0 + jnp.exp(-outgate[:, lanes].astype(f32)))
        cell = (normed * opened).astype(bf16)
        proj = proj + jnp.dot(cell, outproj[lanes, :], preferred_element_type=f32)
    pp[...] = proj.astype(bf16).reshape(pp.shape)

    for k in range(1, members):
        q = (j + k) % members
        send(pp.at[q], rs.at[j], p_send.at[q], p_recv.at[j], (i, q))
    share_weights(in_turn[2])
    stream = res[pl.ds(pl.multiple_of(j * own, own), own), :].astype(f32) + pp[j].astype(f32)
    for k in range(1, members):
        q = (j + k) % members
        arrived(rs.at[q], p_recv.at[q])
        stream = stream + rs[q].astype(f32)
    scaled = stream * lax.rsqrt(jnp.mean(stream * stream, axis=1, keepdims=True) + EPSILON)
    x_all[x, z] = (scaled * gain[...].astype(f32).reshape(1, wide)).astype(bf16)

    def pass_x(zz, sem, to):
        slot = x_all.at[x, zz]
        send(slot, slot, sem, x_recv.at[x, zz], to)

    def x_arrived(xx, zz):
        arrived(x_all.at[xx, zz], x_recv.at[xx, zz])

    for n in range(2):
        pass_x(z, x_send.at[0, n], (2 * ranked(n) + x, j))
    pass_x(z, x_send.at[1, z], x_peer)

    def forward_x(n):
        zz = ranked(n)
        x_arrived(x, zz)
        if n != 1:

            @pl.when(middle)
            def _():
                pass_x(zz, x_send.at[0, 2 + n // 2], (2 * ranked(1) + x, j))

        pass_x(zz, x_send.at[1, zz], x_peer)

    share_weights(in_turn[3])
    share_across(i)
    share_across(in_turn[0])
    share_weights(in_turn[4])
    share_across(in_turn[1])
    share_weights(in_turn[5])
    share_across(in_turn[2])
    share_weights(in_turn[6])
    share_across(in_turn[3])
    forward_x(2)
    forward_x(1)
    forward_x(0)
    share_across(in_turn[4])
    share_across(in_turn[5])
    share_across(in_turn[6])
    for zz in range(depth):
        x_arrived(ox, zz)
    other, other_across = 2 * y + 1 - c, 2 * (1 - y) + 1 - c
    for p in [i] + in_turn:
        arrived(w_slot(other, p), f_recv.at[0, p])
        arrived(w_slot(other_across, p), f_recv.at[1, p])

    units = members * piece

    def chunk(xx):
        a = x_all[xx].reshape(depth * own, -1)
        gate = lax.dot_general(a, w_all[0].reshape(units, -1), nt, preferred_element_type=f32)
        up = lax.dot_general(a, w_all[1].reshape(units, -1), nt, preferred_element_type=f32)
        hidden = (gate / (1.0 + jnp.exp(-gate)) * up).astype(bf16)
        got = jnp.dot(hidden, w_all[2].reshape(units, -1), preferred_element_type=f32)
        part[xx] = got.astype(bf16).reshape(depth, own, -1)

    ends = [(z + depth // 2) % depth] + [(z + k) % depth for k in range(1, depth) if 2 * k != depth]
    chunk(ox)
    for zz in ends + [z]:
        send(part.at[ox, zz], r1.at[zz], e_send.at[zz], e_recv.at[zz], x_peer)
    chunk(x)
    for zz in ends:
        arrived(r1.at[zz], e_recv.at[zz])
        s2[zz] = (part[x, zz].astype(f32) + r1[zz].astype(f32)).astype(bf16)
        send(s2.at[zz], r3.at[z], z_send.at[zz], z_recv.at[z], (2 * zz + x, j))
    arrived(r1.at[z], e_recv.at[z])
    ffn = part[x, z].astype(f32) + r1[z].astype(f32)
    for zz in ends:
        arrived(r3.at[zz], z_recv.at[zz])
        ffn = ffn + r3[zz].astype(f32)
    out[...] = (stream + 0.5 * ffn).astype(out.dtype)

    for k in range(size - 1):
        sent(kv_all.at[0], kv_send.at[k])
        sent(info.at[0], in_send.at[k])
    sent(st_out, st_send.at[0])
    sent(sn_out, st_send.at[1])
    sent(st_out, st_send.at[2])
    sent(sn_out, st_send.at[3])
    for zz in range(depth):
        slot = x_all.at[x, zz]
        sent(slot, x_send.at[1, zz])
        sent(r1.at[0], e_send.at[zz])
    for n in range(4):
        sent(x_all.at[0, 0], x_send.at[0, n], None if n < 2 else middle)
    for p in straight + crossed:
        sent(block, w_send.at[p])
    for p in range(spread):
        sent(block, f_send.at[0, p])
        sent(block, f_send.at[1, p])
        sent(block, g_send.at[p])
    for k in range(1, members):
        sent(rs.at[0], p_send.at[(j + k) % members])
    for zz in ends:
        sent(s2.at[0], z_send.at[zz])


def fused_shards(*args):
    (res, qn, kn, vn, on, gn, qb, kb, vb, ob, gb, opn, opb, gain, gw, uw, dw) = args
    spread, members = lax.axis_size("sp"), lax.axis_size("tp")
    rows, wide = res.shape
    own, depth = rows // members, spread // 2
    chan, hid = gw.shape
    piece = hid // spread
    kvw = 2 * (kn.shape[1] + kb.shape[1])
    bf16, f32 = jnp.bfloat16, jnp.float32
    state_rows = DH_A + DH_B
    v = pltpu.VMEM
    dma = pltpu.SemaphoreType.DMA
    scratch = [
        v((spread // 2, rows, kvw), bf16),
        v((spread // 2, 2, 16, rows), f32),
        v((2, 16, rows), f32),
        v((3, hid, chan), bf16),
        v((3, members, piece, wide), bf16),
        v((members, own, wide), bf16),
        v((members, own, wide), bf16),
        v((2, depth, own, wide), bf16),
        v((2, depth, own, wide), bf16),
        v((depth, own, wide), bf16),
        v((depth, own, wide), bf16),
        v((depth, own, wide), bf16),
        v((state_rows, 128), bf16),
        v((8, state_rows + rows), f32),
        v((2, state_rows, 128), bf16),
        v((2, 8, state_rows + rows), f32),
        dma((spread // 2,)),
        dma((spread // 2,)),
        dma((spread // 2,)),
        dma((spread // 2,)),
        dma((spread,)),
        dma((spread,)),
        dma((2, spread)),
        dma((2, spread)),
        dma((spread,)),
        dma((spread,)),
        dma((members,)),
        dma((members,)),
        dma((2, depth)),
        dma((2, depth)),
        dma((depth,)),
        dma((depth,)),
        dma((depth,)),
        dma((depth,)),
        dma((4,)),
        dma((2,)),
        dma((2,)),
        dma((17,)),
    ]
    scratch += [v(a.shape, a.dtype) for a in (res, qn, on, gn, qb, ob, gb, opn, opb, gain, gw, uw, dw)]
    geometry = (spread, members, wide, gn.shape[1], gb.shape[1])
    return pl.pallas_call(
        functools.partial(fused_kernel, geometry),
        out_shape=jax.ShapeDtypeStruct((own, wide), bf16),
        in_specs=[pl.BlockSpec(memory_space=pltpu.HBM)] * 17,
        out_specs=pl.BlockSpec(memory_space=pltpu.VMEM),
        scratch_shapes=scratch,
        compiler_params=pltpu.CompilerParams(
            collective_id=0, has_side_effects=True, vmem_limit_bytes=40 * 1024 * 1024
        ),
        name="fused",
    )(*[pltpu.with_memory_space_constraint(a, pltpu.HBM) for a in args])


def pick(*args):
    res, kn, gn, gb, gw = args[0], args[2], args[5], args[10], args[14]
    spread, members = lax.axis_size("sp"), lax.axis_size("tp")
    rows = res.shape[0]
    chan, hid = gw.shape
    fits = (
        spread == 8
        and members == 4
        and rows == 128
        and spread * rows <= 2048
        and chan % 128 == 0
        and hid % (16 * spread) == 0
        and hid % 128 == 0
        and (gn.shape[1], gb.shape[1]) == (2, 1)
        and kn.shape[1] == 2 * DH_A
        and DH_A == 128
        and DH_B == 256
    )
    return fused_shards(*args) if fits else shards(*args)


def solution(mesh):
    in_specs = (
        P("sp", None),
        P("sp", "tp"),
        P("sp", "tp"),
        P("sp", "tp"),
        P("sp", "tp"),
        P(None, "tp", "sp"),
        P("sp", "tp"),
        P("sp", "tp"),
        P("sp", "tp"),
        P("sp", "tp"),
        P(None, "tp", "sp"),
        P("tp", None),
        P("tp", None),
        P(),
        P("sp", "tp"),
        P("sp", "tp"),
        P("sp", "tp"),
    )
    out_specs = P(("sp", "tp"), None)
    return jax.shard_map(pick, mesh=mesh, in_specs=in_specs, out_specs=out_specs, check_vma=False)
```

```python
import functools

import jax
import jax.numpy as jnp
from jax import lax
from jax.experimental import pallas as pl
from jax.experimental.pallas import tpu as pltpu
from jax.sharding import PartitionSpec as P

DH_A = 128
DH_B = 256

EPSILON = 1e-06
FAR = -1e30
MESH = pl.DeviceIdType.MESH


def direction_columns(in_gate, log_forget, reverse):
    place, length = lax.axis_index("sp"), lax.axis_size("sp")
    cumulative = lax.cumsum(log_forget, axis=1, reverse=reverse)
    total = cumulative[:, 0] if reverse else cumulative[:, -1]
    toward_end = total[:, None] - cumulative + in_gate
    packed = jnp.concatenate([toward_end, total[:, None]], axis=1)
    every = lax.all_gather(packed, "sp")
    ends, totals = every[:, :, :-1], every[:, :, -1]
    index = jnp.arange(length)
    if reverse:
        between = (index[None, :] > place) & (index[None, :] < index[:, None])
        valid = index > place
    else:
        between = (index[None, :] < place) & (index[None, :] > index[:, None])
        valid = index < place
    offset = jnp.sum(jnp.where(between[:, :, None], totals[None], 0.0), axis=1)
    columns = jnp.where(valid[:, None, None], offset[:, :, None] + ends, FAR)
    own = (in_gate - cumulative)[None]
    columns = jnp.where((index == place)[:, None, None], own, columns)
    return jnp.moveaxis(columns, 0, 1).reshape(in_gate.shape[0], -1)


def group_cell(query, keys, values, outgate, gates, width):
    rows, every = query.shape[0], keys.shape[0]
    place = lax.axis_index("sp")
    heads = query.shape[1] // width
    q = query.reshape(rows, heads, width)
    k = keys.reshape(every, heads, width)
    v = values.reshape(every, heads, width)
    scores = jnp.einsum("thd,shd->hts", q, k, preferred_element_type=jnp.float32) * width ** (-0.5)
    t_at = (place * rows + jnp.arange(rows))[:, None]
    s_at = jnp.arange(every)[None, :]
    summed = 0.0
    for direction in range(2):
        columns = direction_columns(
            gates[direction], jax.nn.log_sigmoid(gates[2 + direction]), direction == 1
        )
        mask = s_at >= t_at if direction else s_at <= t_at
        log_weight = jnp.where(mask[None], columns[:, None, :], FAR)
        top = jnp.max(log_weight, axis=2, keepdims=True)
        weighted = jnp.exp(log_weight - top) * scores
        den = jnp.sum(weighted, axis=2)
        num = jnp.einsum(
            "hts,shd->thd", weighted.astype(jnp.bfloat16), v, preferred_element_type=jnp.float32
        )
        summed = summed + num / jnp.maximum(jnp.abs(jnp.transpose(den)), 1.0)[:, :, None]
    normed = summed * lax.rsqrt(jnp.mean(summed * summed, axis=2, keepdims=True) + EPSILON)
    return (normed.reshape(rows, -1) * jax.nn.sigmoid(outgate.astype(jnp.float32))).astype(
        jnp.bfloat16
    )


def shards(
    residual,
    query_narrow,
    keys_narrow,
    values_narrow,
    outgate_narrow,
    gates_narrow,
    query_broad,
    keys_broad,
    values_broad,
    outgate_broad,
    gates_broad,
    outproj_narrow,
    outproj_broad,
    norm_gain,
    gate_weight,
    up_weight,
    down_weight,
):
    spread = lax.axis_size("sp")
    channels, hidden_own = gate_weight.shape
    stacked = jnp.stack([gate_weight.T, up_weight.T, down_weight.T])
    pieces = stacked.reshape(3, spread, hidden_own // spread, channels)
    pieces = lax.all_to_all(pieces, "sp", split_axis=1, concat_axis=1)
    weights = jnp.swapaxes(pieces, 1, 2).reshape(3, hidden_own // spread, -1)

    narrow, broad = keys_narrow.shape[1], keys_broad.shape[1]
    memory = lax.all_gather(
        jnp.concatenate([keys_narrow, values_narrow, keys_broad, values_broad], axis=1),
        "sp",
        axis=0,
        tiled=True,
    )
    kn, vn = memory[:, :narrow], memory[:, narrow : 2 * narrow]
    kb, vb = memory[:, 2 * narrow : 2 * narrow + broad], memory[:, 2 * narrow + broad :]
    cell_narrow = group_cell(query_narrow, kn, vn, outgate_narrow, gates_narrow, DH_A)
    cell_broad = group_cell(query_broad, kb, vb, outgate_broad, gates_broad, DH_B)

    own_count = residual.shape[0] // lax.axis_size("tp")
    proj = lax.psum_scatter(
        (
            jnp.dot(cell_narrow, outproj_narrow, preferred_element_type=jnp.float32)
            + jnp.dot(cell_broad, outproj_broad, preferred_element_type=jnp.float32)
        ).astype(jnp.bfloat16),
        "tp",
        scatter_dimension=0,
        tiled=True,
    ).astype(jnp.float32)
    offset = lax.axis_index("tp") * own_count
    stream = lax.dynamic_slice_in_dim(residual, offset, own_count, 0).astype(jnp.float32) + proj
    scaled = stream * lax.rsqrt(jnp.mean(stream * stream, axis=1, keepdims=True) + EPSILON)
    normed = (scaled * norm_gain.astype(jnp.float32)).astype(jnp.bfloat16)
    normed = lax.all_gather(normed, ("sp", "tp"), axis=0, tiled=True)
    nt = (((1,), (1,)), ((), ()))
    gate = lax.dot_general(normed, weights[0], nt, preferred_element_type=jnp.float32)
    upward = lax.dot_general(normed, weights[1], nt, preferred_element_type=jnp.float32)
    hidden = (jax.nn.silu(gate) * upward).astype(jnp.bfloat16)
    partial_value = jnp.dot(hidden, weights[2], preferred_element_type=jnp.float32)
    ffn = lax.psum_scatter(
        partial_value.astype(jnp.bfloat16), ("sp", "tp"), scatter_dimension=0, tiled=True
    ).astype(jnp.float32)
    return (stream + 0.5 * ffn).astype(jnp.bfloat16)


def fused_kernel(geometry, *refs):
    spread, members, wide, narrow_heads, broad_heads = geometry
    held, out = refs[:17], refs[17]
    (kv_all, info, gates, wt, w_all, pp, rs, x_all, part, r1, s2, r3) = refs[18:30]
    (st_out, sn_out, st_in, sn_in) = refs[30:34]
    (kv_send, kv_recv, in_send, in_recv, w_send, w_recv, f_send, f_recv, g_send, g_recv) = refs[34:44]
    (p_send, p_recv, x_send, x_recv, e_send, e_recv, z_send, z_recv) = refs[44:52]
    (st_send, st_recv, sn_recv, load_sem) = refs[52:56]
    (res, qn, on, gn, qb, ob, gb, opn, opb, gain, gw, uw, dw) = refs[56:69]
    rows = res.shape[0]
    own = rows // members
    depth = spread // 2
    chan, hid = gw.shape
    piece = hid // spread
    ca, cb = held[2].shape[1], held[7].shape[1]
    i, j = lax.axis_index("sp"), lax.axis_index("tp")
    z, x = i // 2, i % 2
    y, c = j // 2, j % 2
    ox = 1 - x
    size = spread // 2
    half, local = i // size, i % size
    f32, bf16 = jnp.float32, jnp.bfloat16
    sibling, x_peer = (i, j + 1 - 2 * c), (2 * z + ox, j)
    across = (1 - y) * 2 + c
    y_peer = (i, across)

    def ranked(n):
        pick = 0
        for a in range(depth):
            others = sorted(
                (b for b in range(depth) if b != a),
                key=lambda b: (abs(a - b), (a < depth // 2) == (b < depth // 2)),
            )
            pick = pick + jnp.where(z == a, others[n], 0)
        return pick

    def send(src, dst, s_sem, r_sem, to):
        copy = pltpu.make_async_remote_copy(
            src_ref=src, dst_ref=dst, send_sem=s_sem, recv_sem=r_sem, device_id=to, device_id_type=MESH
        )
        copy.start()
        return copy

    def arrived(ref, sem):
        pltpu.make_async_remote_copy(
            src_ref=ref, dst_ref=ref, send_sem=sem, recv_sem=sem, device_id=(i, j), device_id_type=MESH
        ).wait_recv()

    def sent(ref, sem, cond=None):
        def wait():
            pltpu.make_async_remote_copy(
                src_ref=ref, dst_ref=ref, send_sem=sem, recv_sem=sem, device_id=(i, j), device_id_type=MESH
            ).wait_send()

        if cond is None:
            wait()
        else:
            pl.when(cond)(wait)

    barrier = pltpu.get_barrier_semaphore()
    for k in range(1, spread):
        pl.semaphore_signal(barrier, inc=1, device_id=((i + k) % spread, j), device_id_type=MESH)
    for k in range(1, members):
        pl.semaphore_signal(barrier, inc=1, device_id=(i, (j + k) % members), device_id_type=MESH)

    mine_kv = kv_all.at[local]
    targets = {
        5: gn,
        10: gb,
        2: mine_kv.at[:, 0:ca],
        3: mine_kv.at[:, ca : 2 * ca],
        7: mine_kv.at[:, 2 * ca : 2 * ca + cb],
        8: mine_kv.at[:, 2 * ca + cb : 2 * ca + 2 * cb],
        14: gw,
        15: uw,
        16: dw,
        1: qn,
        6: qb,
        4: on,
        9: ob,
        11: opn,
        12: opb,
        0: res,
        13: gain,
    }
    loads = {n: pltpu.make_async_copy(held[n], ref, load_sem.at[n]) for n, ref in targets.items()}
    for load in loads.values():
        load.start()

    def loaded(*numbers):
        for n in numbers:
            loads[n].wait()

    loaded(5, 10)
    gates[...] = jnp.zeros_like(gates)
    for role in range(4):
        at = 8 * (role % 2)
        gates[role // 2, at : at + narrow_heads, :] = gn[role]
        gates[role // 2, at + narrow_heads : at + narrow_heads + broad_heads, :] = gb[role]
    in_gate, pre = gates[0], gates[1]
    forget = jnp.minimum(pre, 0.0) - jnp.log1p(jnp.exp(-jnp.abs(pre)))
    r_at = lax.broadcasted_iota(jnp.int32, (rows, rows), 0)
    c_at = lax.broadcasted_iota(jnp.int32, (rows, rows), 1)
    run = lambda m: jnp.dot(
        forget, m.astype(f32), preferred_element_type=f32, precision=lax.Precision.HIGHEST
    )
    forward_row = lax.broadcasted_iota(jnp.int32, in_gate.shape, 0) < 8
    cumulative = jnp.where(forward_row, run(r_at <= c_at), run(r_at >= c_at))
    total = jnp.where(
        forward_row,
        jnp.broadcast_to(cumulative[:, rows - 1 : rows], in_gate.shape),
        jnp.broadcast_to(cumulative[:, 0:1], in_gate.shape),
    )
    own_column = in_gate - cumulative
    info[local, 0] = total + own_column
    info[local, 1] = total
    pl.semaphore_wait(barrier, spread + members - 2)

    loaded(2, 3, 7, 8)
    mates = [(local + k) % size for k in range(1, size)]
    for k, mate in enumerate(mates):
        to = (half * size + mate, j)
        send(kv_all.at[local], kv_all.at[local], kv_send.at[k], kv_recv.at[local], to)
        send(info.at[local], info.at[local], in_send.at[k], in_recv.at[local], to)

    loaded(14, 15, 16)
    for m, ref in enumerate((gw, uw, dw)):
        for k in range(hid // 128):
            wt[m, k * 128 : (k + 1) * 128, :] = ref[:, k * 128 : (k + 1) * 128].T
    mine = pl.ds(pl.multiple_of(i * piece, 16), piece)

    whole, first, last = (0, 0, 3), (0, 0, 2), (1, 2, 3)

    def w_slot(jj, p, cut):
        return w_all.at[cut[1] : cut[2], jj, :, pl.ds(pl.multiple_of(p * chan, 128), chan)]

    def send_weights(p, part=whole):
        theirs = pl.ds(pl.multiple_of(p * piece, 16), piece)
        n = part[0]
        source = wt.at[part[1] : part[2], theirs, :]
        send(source, w_slot(j, i, part), w_send.at[n, p], w_recv.at[n, i], (p, j))

    def share_weights(p, part=whole):
        slot, n = w_slot(j, p, part), part[0]
        arrived(slot, w_recv.at[n, p])
        send(slot, slot, f_send.at[2 * n, p], f_recv.at[2 * n, p], sibling)
        send(slot, slot, g_send.at[n, p], g_recv.at[n, p], y_peer)

    def share_across(p, part=whole):
        slot, n = w_slot(across, p, part), part[0]
        arrived(slot, g_recv.at[n, p])
        send(slot, slot, f_send.at[2 * n + 1, p], f_recv.at[2 * n + 1, p], sibling)

    columns = pl.ds(pl.multiple_of(i * chan, 128), chan)
    block = wt.at[:, mine, :]
    send(block, w_slot(j, i, whole), g_send.at[0, i], g_recv.at[0, i], y_peer)
    send(block, w_slot(j, i, whole), f_send.at[0, i], f_recv.at[0, i], sibling)
    w_all[:, j, :, columns] = wt[:, mine, :]
    straight = [2 * ranked(n) + x for n in range(depth - 1)]
    crossed = [2 * z + ox] + [2 * ranked(n) + ox for n in range(depth - 1)]
    middle = jnp.logical_or(z == depth // 2 - 1, z == depth // 2)

    @pl.when(middle)
    def _():
        for p in (straight[2], straight[0], straight[1]):
            send_weights(p)

    @pl.when(jnp.logical_not(middle))
    def _():
        send_weights(straight[1])

    send_weights(crossed[0])

    @pl.when(middle)
    def _():
        send_weights(crossed[2], first)

    in_turn = [
        jnp.where(middle, a, b)
        for a, b in zip(
            [straight[0], straight[2], crossed[0], straight[1], crossed[1], crossed[3], crossed[2]],
            [straight[1], crossed[0], straight[0], straight[2], crossed[1], crossed[3], crossed[2]],
        )
    ]

    for mate in mates:
        arrived(kv_all.at[mate], kv_recv.at[mate])
        arrived(info.at[mate], in_recv.at[mate])

    before, after = [], [None] * size
    passed = jnp.zeros_like(total)
    for k in range(size):
        before.append(passed)
        passed = passed + info[k, 1]
    passed = jnp.zeros_like(total)
    for k in reversed(range(size)):
        after[k] = passed
        passed = passed + info[k, 1]
    to_end = jnp.concatenate(
        [info[k, 0] + jnp.where(forward_row, after[k], before[k]) for k in range(size)], axis=1
    )
    to_end = jnp.where(half == 0, to_end[0:8], to_end[8:16])
    end_max = jnp.max(to_end, axis=1, keepdims=True)
    share = jnp.transpose(
        jnp.concatenate([jnp.exp(to_end - end_max), jnp.zeros((rows - 8, size * rows), f32)], axis=0)
    )
    share_a = jnp.where(x == 0, share[:, 0:1], share[:, 1:2])
    share_b = share[:, narrow_heads : narrow_heads + 1]
    wa, wb = ca // narrow_heads, cb // 2

    def kv_lanes(start, width):
        return kv_all[:, :, pl.ds(pl.multiple_of(start, 128), width)].reshape(size * rows, width)

    tn = (((0,), (0,)), ((), ()))
    keys_a, keys_b = kv_lanes(x * wa, wa), kv_lanes(2 * ca, cb)
    values_a = (share_a * kv_lanes(ca + x * wa, wa).astype(f32)).astype(bf16)
    values_b = (share_b * kv_lanes(2 * ca + cb + x * wb, wb).astype(f32)).astype(bf16)
    st_out[0:wa, :] = lax.dot_general(keys_a, values_a, tn, preferred_element_type=f32).astype(bf16)
    st_out[wa : wa + cb, :] = lax.dot_general(keys_b, values_b, tn, preferred_element_type=f32).astype(bf16)
    norm_a = jnp.sum(share_a * keys_a.astype(f32), axis=0, keepdims=True)
    norm_b = jnp.sum(share_b * keys_b.astype(f32), axis=0, keepdims=True)
    sn_out[:, 0:wa] = jnp.broadcast_to(norm_a, (8, wa))
    sn_out[:, wa : wa + cb] = jnp.broadcast_to(norm_b, (8, cb))
    sn_out[:, wa + cb :] = jnp.broadcast_to(end_max, (8, rows))
    mirror = ((i + size) % spread, j)
    send(sn_out, sn_in.at[x], st_send.at[1], sn_recv.at[x], mirror)
    send(st_out, st_in.at[x], st_send.at[0], st_recv.at[x], mirror)

    @pl.when(middle)
    def _():
        for p in (crossed[1], crossed[3]):
            send_weights(p, first)

    @pl.when(jnp.logical_not(middle))
    def _():
        send_weights(straight[0])

    share_weights(in_turn[0])
    arrived(sn_in.at[x], sn_recv.at[x])
    arrived(st_in.at[x], st_recv.at[x])
    send(sn_in.at[x], sn_in.at[x], st_send.at[3], sn_recv.at[x], x_peer)
    send(st_in.at[x], st_in.at[x], st_send.at[2], st_recv.at[x], x_peer)

    @pl.when(jnp.logical_not(middle))
    def _():
        send_weights(straight[2])
        for p in (crossed[2], crossed[3], crossed[1]):
            send_weights(p, first)

    share_weights(in_turn[1])
    arrived(sn_in.at[ox], sn_recv.at[ox])
    arrived(st_in.at[ox], st_recv.at[ox])

    loaded(1, 6, 4, 9, 11, 12, 0, 13)
    pieces = [None] * size
    forward_sum = jnp.zeros_like(total)
    ahead = [None] * size
    for k in reversed(range(size)):
        ahead[k] = forward_sum
        forward_sum = forward_sum + jnp.where(k < local, info[k, 1], 0.0)
    backward_sum = jnp.zeros_like(total)
    for k in range(size):
        reach = jnp.where(forward_row, ahead[k], backward_sum) + info[k, 0]
        seen = jnp.logical_or(
            jnp.logical_and(forward_row, k < local),
            jnp.logical_and(jnp.logical_not(forward_row), k > local),
        )
        pieces[k] = jnp.where(k == local, own_column, jnp.where(seen, reach, FAR))
        backward_sum = backward_sum + jnp.where(k > local, info[k, 1], 0.0)
    column = jnp.concatenate(pieces, axis=1)
    past = sn_in[x, :, wa + cb :] + jnp.where(half == 1, forward_sum[0:8], backward_sum[8:16])
    t_at = lax.broadcasted_iota(jnp.int32, (rows, size * rows), 0) + local * rows
    s_at = lax.broadcasted_iota(jnp.int32, (rows, size * rows), 1)
    masks = (s_at <= t_at, s_at >= t_at)
    nt = (((1,), (1,)), ((), ()))
    proj = jnp.zeros((rows, res.shape[1]), f32)
    heads = [(qn, on, opn, 0, ca, h, ca // narrow_heads, h) for h in range(narrow_heads)]
    heads += [
        (qb, ob, opb, 2 * ca, cb, h, cb // broad_heads, narrow_heads + h) for h in range(broad_heads)
    ]
    for query, outgate, outproj, base, group, h, width, row in heads:
        lanes = slice(h * width, (h + 1) * width)
        keys = kv_all[:, :, base + h * width : base + (h + 1) * width].reshape(size * rows, width)
        vals = kv_all[:, :, base + group + h * width : base + group + (h + 1) * width].reshape(
            size * rows, width
        )
        queries = query[:, lanes]
        scores = lax.dot_general(queries, keys, nt, preferred_element_type=f32) * width ** (-0.5)
        if row < narrow_heads:
            memory, normer = st_in[row, 0:wa, :], sn_in[row, 0:1, 0:wa]
        else:
            memory = jnp.concatenate([st_in[0, wa:, :], st_in[1, wa:, :]], axis=1)
            normer = sn_in[0, 0:1, wa : wa + cb]
        recalled = jnp.dot(queries, memory, preferred_element_type=f32) * width ** (-0.5)
        recall_den = jnp.sum(queries.astype(f32) * normer, axis=1, keepdims=True) * width ** (-0.5)
        summed = jnp.zeros((rows, width), f32)
        for direction in range(2):
            at = 8 * direction + row
            weight = jnp.where(
                masks[direction],
                jnp.broadcast_to(column[at : at + 1, :], scores.shape),
                FAR,
            )
            carried = jnp.where(half == 1 - direction, past[row : row + 1, 0:1], FAR)
            top = jnp.maximum(jnp.max(weight, axis=1, keepdims=True), carried)
            kept = jnp.exp(carried - top)
            p = jnp.exp(weight - top) * scores
            den = jnp.sum(p, axis=1, keepdims=True) + kept * recall_den
            num = jnp.dot(p.astype(bf16), vals, preferred_element_type=f32) + kept * recalled
            summed = summed + num / jnp.maximum(jnp.abs(den), 1.0)
        normed = summed * lax.rsqrt(jnp.mean(summed * summed, axis=1, keepdims=True) + EPSILON)
        opened = 1.0 / (1.0 + jnp.exp(-outgate[:, lanes].astype(f32)))
        cell = (normed * opened).astype(bf16)
        proj = proj + jnp.dot(cell, outproj[lanes, :], preferred_element_type=f32)
    pp[...] = proj.astype(bf16).reshape(pp.shape)

    for k in range(1, members):
        q = (j + k) % members
        send(pp.at[q], rs.at[j], p_send.at[q], p_recv.at[j], (i, q))
    share_weights(in_turn[2])
    stream = res[pl.ds(pl.multiple_of(j * own, own), own), :].astype(f32) + pp[j].astype(f32)
    for k in range(1, members):
        q = (j + k) % members
        arrived(rs.at[q], p_recv.at[q])
        stream = stream + rs[q].astype(f32)
    scaled = stream * lax.rsqrt(jnp.mean(stream * stream, axis=1, keepdims=True) + EPSILON)
    x_all[x, z] = (scaled * gain[...].astype(f32).reshape(1, wide)).astype(bf16)

    def pass_x(zz, sem, to):
        slot = x_all.at[x, zz]
        send(slot, slot, sem, x_recv.at[x, zz], to)

    def x_arrived(xx, zz):
        arrived(x_all.at[xx, zz], x_recv.at[xx, zz])

    for n in range(2):
        pass_x(z, x_send.at[0, n], (2 * ranked(n) + x, j))
    pass_x(z, x_send.at[1, z], x_peer)

    def forward_x(n):
        zz = ranked(n)
        x_arrived(x, zz)
        if n != 1:

            @pl.when(middle)
            def _():
                pass_x(zz, x_send.at[0, 2 + n // 2], (2 * ranked(1) + x, j))

        pass_x(zz, x_send.at[1, zz], x_peer)

    for p in (crossed[2], crossed[3], crossed[1]):
        send_weights(p, last)
    share_weights(in_turn[3])
    share_across(i)
    share_across(in_turn[0])
    share_weights(in_turn[4], first)
    share_across(in_turn[1])
    share_weights(in_turn[5], first)
    share_across(in_turn[2])
    share_weights(in_turn[6], first)
    share_across(in_turn[3])
    forward_x(2)
    forward_x(1)
    forward_x(0)
    for p in in_turn[4:]:
        share_weights(p, last)
    for p in in_turn[4:]:
        share_across(p, first)
    for zz in range(depth):
        x_arrived(ox, zz)
    for p in in_turn[4:]:
        share_across(p, last)
    other, other_across = 2 * y + 1 - c, 2 * (1 - y) + 1 - c
    for p, cut in [(i, whole)] + [(p, whole) for p in in_turn[:4]] + [(p, first) for p in in_turn[4:]]:
        arrived(w_slot(other, p, cut), f_recv.at[0, p])
        arrived(w_slot(other_across, p, cut), f_recv.at[1, p])

    units = members * piece

    def hidden_of(xx):
        a = x_all[xx].reshape(depth * own, -1)
        gate = lax.dot_general(a, w_all[0].reshape(units, -1), nt, preferred_element_type=f32)
        up = lax.dot_general(a, w_all[1].reshape(units, -1), nt, preferred_element_type=f32)
        return (gate / (1.0 + jnp.exp(-gate)) * up).astype(bf16)

    def project(xx, hidden):
        got = jnp.dot(hidden, w_all[2].reshape(units, -1), preferred_element_type=f32)
        part[xx] = got.astype(bf16).reshape(depth, own, -1)

    ends = [(z + depth // 2) % depth] + [(z + k) % depth for k in range(1, depth) if 2 * k != depth]
    hidden = hidden_of(ox)
    for p in in_turn[4:]:
        arrived(w_slot(other, p, last), f_recv.at[2, p])
        arrived(w_slot(other_across, p, last), f_recv.at[3, p])
    project(ox, hidden)
    for zz in ends + [z]:
        send(part.at[ox, zz], r1.at[zz], e_send.at[zz], e_recv.at[zz], x_peer)
    project(x, hidden_of(x))
    for zz in ends:
        arrived(r1.at[zz], e_recv.at[zz])
        s2[zz] = (part[x, zz].astype(f32) + r1[zz].astype(f32)).astype(bf16)
        send(s2.at[zz], r3.at[z], z_send.at[zz], z_recv.at[z], (2 * zz + x, j))
    arrived(r1.at[z], e_recv.at[z])
    ffn = part[x, z].astype(f32) + r1[z].astype(f32)
    for zz in ends:
        arrived(r3.at[zz], z_recv.at[zz])
        ffn = ffn + r3[zz].astype(f32)
    out[...] = (stream + 0.5 * ffn).astype(out.dtype)

    for k in range(size - 1):
        sent(kv_all.at[0], kv_send.at[k])
        sent(info.at[0], in_send.at[k])
    sent(st_out, st_send.at[0])
    sent(sn_out, st_send.at[1])
    sent(st_out, st_send.at[2])
    sent(sn_out, st_send.at[3])
    for zz in range(depth):
        slot = x_all.at[x, zz]
        sent(slot, x_send.at[1, zz])
        sent(r1.at[0], e_send.at[zz])
    for n in range(4):
        sent(x_all.at[0, 0], x_send.at[0, n], None if n < 2 else middle)
    late = wt.at[2:3, mine, :]
    early = wt.at[0:2, mine, :]
    for p in straight + crossed[:1]:
        sent(block, w_send.at[0, p])
    for p in crossed[1:]:
        sent(early, w_send.at[0, p])
        sent(late, w_send.at[1, p])
    for p in [i] + in_turn[:4]:
        for ref in (g_send.at[0, p], f_send.at[0, p], f_send.at[1, p]):
            sent(block, ref)
    for p in in_turn[4:]:
        for ref in (g_send.at[0, p], f_send.at[0, p], f_send.at[1, p]):
            sent(early, ref)
        for ref in (g_send.at[1, p], f_send.at[2, p], f_send.at[3, p]):
            sent(late, ref)
    for k in range(1, members):
        sent(rs.at[0], p_send.at[(j + k) % members])
    for zz in ends:
        sent(s2.at[0], z_send.at[zz])


def fused_shards(*args):
    (res, qn, kn, vn, on, gn, qb, kb, vb, ob, gb, opn, opb, gain, gw, uw, dw) = args
    spread, members = lax.axis_size("sp"), lax.axis_size("tp")
    rows, wide = res.shape
    own, depth = rows // members, spread // 2
    chan, hid = gw.shape
    piece = hid // spread
    kvw = 2 * (kn.shape[1] + kb.shape[1])
    bf16, f32 = jnp.bfloat16, jnp.float32
    state_rows = DH_A + DH_B
    v = pltpu.VMEM
    dma = pltpu.SemaphoreType.DMA
    scratch = [
        v((spread // 2, rows, kvw), bf16),
        v((spread // 2, 2, 16, rows), f32),
        v((2, 16, rows), f32),
        v((3, hid, chan), bf16),
        v((3, members, piece, wide), bf16),
        v((members, own, wide), bf16),
        v((members, own, wide), bf16),
        v((2, depth, own, wide), bf16),
        v((2, depth, own, wide), bf16),
        v((depth, own, wide), bf16),
        v((depth, own, wide), bf16),
        v((depth, own, wide), bf16),
        v((state_rows, 128), bf16),
        v((8, state_rows + rows), f32),
        v((2, state_rows, 128), bf16),
        v((2, 8, state_rows + rows), f32),
        dma((spread // 2,)),
        dma((spread // 2,)),
        dma((spread // 2,)),
        dma((spread // 2,)),
        dma((2, spread)),
        dma((2, spread)),
        dma((4, spread)),
        dma((4, spread)),
        dma((2, spread)),
        dma((2, spread)),
        dma((members,)),
        dma((members,)),
        dma((2, depth)),
        dma((2, depth)),
        dma((depth,)),
        dma((depth,)),
        dma((depth,)),
        dma((depth,)),
        dma((4,)),
        dma((2,)),
        dma((2,)),
        dma((17,)),
    ]
    scratch += [v(a.shape, a.dtype) for a in (res, qn, on, gn, qb, ob, gb, opn, opb, gain, gw, uw, dw)]
    geometry = (spread, members, wide, gn.shape[1], gb.shape[1])
    return pl.pallas_call(
        functools.partial(fused_kernel, geometry),
        out_shape=jax.ShapeDtypeStruct((own, wide), bf16),
        in_specs=[pl.BlockSpec(memory_space=pltpu.HBM)] * 17,
        out_specs=pl.BlockSpec(memory_space=pltpu.VMEM),
        scratch_shapes=scratch,
        compiler_params=pltpu.CompilerParams(
            collective_id=0, has_side_effects=True, vmem_limit_bytes=40 * 1024 * 1024
        ),
        name="fused",
    )(*[pltpu.with_memory_space_constraint(a, pltpu.HBM) for a in args])


def pick(*args):
    res, kn, gn, gb, gw = args[0], args[2], args[5], args[10], args[14]
    spread, members = lax.axis_size("sp"), lax.axis_size("tp")
    rows = res.shape[0]
    chan, hid = gw.shape
    fits = (
        spread == 8
        and members == 4
        and rows == 128
        and spread * rows <= 2048
        and chan % 128 == 0
        and hid % (16 * spread) == 0
        and hid % 128 == 0
        and (gn.shape[1], gb.shape[1]) == (2, 1)
        and kn.shape[1] == 2 * DH_A
        and DH_A == 128
        and DH_B == 256
    )
    return fused_shards(*args) if fits else shards(*args)


def solution(mesh):
    in_specs = (
        P("sp", None),
        P("sp", "tp"),
        P("sp", "tp"),
        P("sp", "tp"),
        P("sp", "tp"),
        P(None, "tp", "sp"),
        P("sp", "tp"),
        P("sp", "tp"),
        P("sp", "tp"),
        P("sp", "tp"),
        P(None, "tp", "sp"),
        P("tp", None),
        P("tp", None),
        P(),
        P("sp", "tp"),
        P("sp", "tp"),
        P("sp", "tp"),
    )
    out_specs = P(("sp", "tp"), None)
    return jax.shard_map(pick, mesh=mesh, in_specs=in_specs, out_specs=out_specs, check_vma=False)
```

```python
import functools

import jax
import jax.numpy as jnp
from jax import lax
from jax.experimental import pallas as pl
from jax.experimental.pallas import tpu as pltpu
from jax.sharding import PartitionSpec as P

DH_A = 128
DH_B = 256

EPSILON = 1e-06
FAR = -1e30
MESH = pl.DeviceIdType.MESH


def direction_columns(in_gate, log_forget, reverse):
    place, length = lax.axis_index("sp"), lax.axis_size("sp")
    cumulative = lax.cumsum(log_forget, axis=1, reverse=reverse)
    total = cumulative[:, 0] if reverse else cumulative[:, -1]
    toward_end = total[:, None] - cumulative + in_gate
    packed = jnp.concatenate([toward_end, total[:, None]], axis=1)
    every = lax.all_gather(packed, "sp")
    ends, totals = every[:, :, :-1], every[:, :, -1]
    index = jnp.arange(length)
    if reverse:
        between = (index[None, :] > place) & (index[None, :] < index[:, None])
        valid = index > place
    else:
        between = (index[None, :] < place) & (index[None, :] > index[:, None])
        valid = index < place
    offset = jnp.sum(jnp.where(between[:, :, None], totals[None], 0.0), axis=1)
    columns = jnp.where(valid[:, None, None], offset[:, :, None] + ends, FAR)
    own = (in_gate - cumulative)[None]
    columns = jnp.where((index == place)[:, None, None], own, columns)
    return jnp.moveaxis(columns, 0, 1).reshape(in_gate.shape[0], -1)


def group_cell(query, keys, values, outgate, gates, width):
    rows, every = query.shape[0], keys.shape[0]
    place = lax.axis_index("sp")
    heads = query.shape[1] // width
    q = query.reshape(rows, heads, width)
    k = keys.reshape(every, heads, width)
    v = values.reshape(every, heads, width)
    scores = jnp.einsum("thd,shd->hts", q, k, preferred_element_type=jnp.float32) * width ** (-0.5)
    t_at = (place * rows + jnp.arange(rows))[:, None]
    s_at = jnp.arange(every)[None, :]
    summed = 0.0
    for direction in range(2):
        columns = direction_columns(
            gates[direction], jax.nn.log_sigmoid(gates[2 + direction]), direction == 1
        )
        mask = s_at >= t_at if direction else s_at <= t_at
        log_weight = jnp.where(mask[None], columns[:, None, :], FAR)
        top = jnp.max(log_weight, axis=2, keepdims=True)
        weighted = jnp.exp(log_weight - top) * scores
        den = jnp.sum(weighted, axis=2)
        num = jnp.einsum(
            "hts,shd->thd", weighted.astype(jnp.bfloat16), v, preferred_element_type=jnp.float32
        )
        summed = summed + num / jnp.maximum(jnp.abs(jnp.transpose(den)), 1.0)[:, :, None]
    normed = summed * lax.rsqrt(jnp.mean(summed * summed, axis=2, keepdims=True) + EPSILON)
    return (normed.reshape(rows, -1) * jax.nn.sigmoid(outgate.astype(jnp.float32))).astype(
        jnp.bfloat16
    )


def shards(
    residual,
    query_narrow,
    keys_narrow,
    values_narrow,
    outgate_narrow,
    gates_narrow,
    query_broad,
    keys_broad,
    values_broad,
    outgate_broad,
    gates_broad,
    outproj_narrow,
    outproj_broad,
    norm_gain,
    gate_weight,
    up_weight,
    down_weight,
):
    spread = lax.axis_size("sp")
    channels, hidden_own = gate_weight.shape
    stacked = jnp.stack([gate_weight.T, up_weight.T, down_weight.T])
    pieces = stacked.reshape(3, spread, hidden_own // spread, channels)
    pieces = lax.all_to_all(pieces, "sp", split_axis=1, concat_axis=1)
    weights = jnp.swapaxes(pieces, 1, 2).reshape(3, hidden_own // spread, -1)

    narrow, broad = keys_narrow.shape[1], keys_broad.shape[1]
    memory = lax.all_gather(
        jnp.concatenate([keys_narrow, values_narrow, keys_broad, values_broad], axis=1),
        "sp",
        axis=0,
        tiled=True,
    )
    kn, vn = memory[:, :narrow], memory[:, narrow : 2 * narrow]
    kb, vb = memory[:, 2 * narrow : 2 * narrow + broad], memory[:, 2 * narrow + broad :]
    cell_narrow = group_cell(query_narrow, kn, vn, outgate_narrow, gates_narrow, DH_A)
    cell_broad = group_cell(query_broad, kb, vb, outgate_broad, gates_broad, DH_B)

    own_count = residual.shape[0] // lax.axis_size("tp")
    proj = lax.psum_scatter(
        (
            jnp.dot(cell_narrow, outproj_narrow, preferred_element_type=jnp.float32)
            + jnp.dot(cell_broad, outproj_broad, preferred_element_type=jnp.float32)
        ).astype(jnp.bfloat16),
        "tp",
        scatter_dimension=0,
        tiled=True,
    ).astype(jnp.float32)
    offset = lax.axis_index("tp") * own_count
    stream = lax.dynamic_slice_in_dim(residual, offset, own_count, 0).astype(jnp.float32) + proj
    scaled = stream * lax.rsqrt(jnp.mean(stream * stream, axis=1, keepdims=True) + EPSILON)
    normed = (scaled * norm_gain.astype(jnp.float32)).astype(jnp.bfloat16)
    normed = lax.all_gather(normed, ("sp", "tp"), axis=0, tiled=True)
    nt = (((1,), (1,)), ((), ()))
    gate = lax.dot_general(normed, weights[0], nt, preferred_element_type=jnp.float32)
    upward = lax.dot_general(normed, weights[1], nt, preferred_element_type=jnp.float32)
    hidden = (jax.nn.silu(gate) * upward).astype(jnp.bfloat16)
    partial_value = jnp.dot(hidden, weights[2], preferred_element_type=jnp.float32)
    ffn = lax.psum_scatter(
        partial_value.astype(jnp.bfloat16), ("sp", "tp"), scatter_dimension=0, tiled=True
    ).astype(jnp.float32)
    return (stream + 0.5 * ffn).astype(jnp.bfloat16)


def fused_kernel(geometry, *refs):
    spread, members, wide, narrow_heads, broad_heads = geometry
    held, out = refs[:17], refs[17]
    (kv_all, info, gates, wt, w_all, pp, rs, x_all, part, r1, s2, r3) = refs[18:30]
    (st_out, sn_out, st_in, sn_in) = refs[30:34]
    (kv_send, kv_recv, in_send, in_recv, w_send, w_recv, f_send, f_recv, g_send, g_recv) = refs[34:44]
    (p_send, p_recv, x_send, x_recv, e_send, e_recv, z_send, z_recv) = refs[44:52]
    (st_send, st_recv, sn_recv, load_sem) = refs[52:56]
    (res, qn, on, gn, qb, ob, gb, opn, opb, gain, gw, uw, dw) = refs[56:69]
    rows = res.shape[0]
    own = rows // members
    depth = spread // 2
    chan, hid = gw.shape
    piece = hid // spread
    ca, cb = held[2].shape[1], held[7].shape[1]
    i, j = lax.axis_index("sp"), lax.axis_index("tp")
    z, x = i // 2, i % 2
    y, c = j // 2, j % 2
    ox = 1 - x
    size = spread // 2
    half, local = i // size, i % size
    f32, bf16 = jnp.float32, jnp.bfloat16
    sibling, x_peer = (i, j + 1 - 2 * c), (2 * z + ox, j)
    across = (1 - y) * 2 + c
    y_peer = (i, across)

    def ranked(n):
        pick = 0
        for a in range(depth):
            others = sorted(
                (b for b in range(depth) if b != a),
                key=lambda b: (abs(a - b), (a < depth // 2) == (b < depth // 2)),
            )
            pick = pick + jnp.where(z == a, others[n], 0)
        return pick

    def send(src, dst, s_sem, r_sem, to):
        copy = pltpu.make_async_remote_copy(
            src_ref=src, dst_ref=dst, send_sem=s_sem, recv_sem=r_sem, device_id=to, device_id_type=MESH
        )
        copy.start()
        return copy

    def arrived(ref, sem):
        pltpu.make_async_remote_copy(
            src_ref=ref, dst_ref=ref, send_sem=sem, recv_sem=sem, device_id=(i, j), device_id_type=MESH
        ).wait_recv()

    def sent(ref, sem, cond=None):
        def wait():
            pltpu.make_async_remote_copy(
                src_ref=ref, dst_ref=ref, send_sem=sem, recv_sem=sem, device_id=(i, j), device_id_type=MESH
            ).wait_send()

        if cond is None:
            wait()
        else:
            pl.when(cond)(wait)

    barrier = pltpu.get_barrier_semaphore()
    for k in range(1, spread):
        pl.semaphore_signal(barrier, inc=1, device_id=((i + k) % spread, j), device_id_type=MESH)
    for k in range(1, members):
        pl.semaphore_signal(barrier, inc=1, device_id=(i, (j + k) % members), device_id_type=MESH)

    mine_kv = kv_all.at[local]
    targets = {
        5: gn,
        10: gb,
        2: mine_kv.at[:, 0:ca],
        3: mine_kv.at[:, ca : 2 * ca],
        7: mine_kv.at[:, 2 * ca : 2 * ca + cb],
        8: mine_kv.at[:, 2 * ca + cb : 2 * ca + 2 * cb],
        14: gw,
        15: uw,
        16: dw,
        1: qn,
        6: qb,
        4: on,
        9: ob,
        11: opn,
        12: opb,
        0: res,
        13: gain,
    }
    loads = {n: pltpu.make_async_copy(held[n], ref, load_sem.at[n]) for n, ref in targets.items()}
    for load in loads.values():
        load.start()

    def loaded(*numbers):
        for n in numbers:
            loads[n].wait()

    loaded(5, 10)
    gates[...] = jnp.zeros_like(gates)
    for role in range(4):
        at = 8 * (role % 2)
        gates[role // 2, at : at + narrow_heads, :] = gn[role]
        gates[role // 2, at + narrow_heads : at + narrow_heads + broad_heads, :] = gb[role]
    in_gate, pre = gates[0], gates[1]
    forget = jnp.minimum(pre, 0.0) - jnp.log1p(jnp.exp(-jnp.abs(pre)))
    r_at = lax.broadcasted_iota(jnp.int32, (rows, rows), 0)
    c_at = lax.broadcasted_iota(jnp.int32, (rows, rows), 1)
    run = lambda m: jnp.dot(
        forget, m.astype(f32), preferred_element_type=f32, precision=lax.Precision.HIGHEST
    )
    forward_row = lax.broadcasted_iota(jnp.int32, in_gate.shape, 0) < 8
    cumulative = jnp.where(forward_row, run(r_at <= c_at), run(r_at >= c_at))
    total = jnp.where(
        forward_row,
        jnp.broadcast_to(cumulative[:, rows - 1 : rows], in_gate.shape),
        jnp.broadcast_to(cumulative[:, 0:1], in_gate.shape),
    )
    own_column = in_gate - cumulative
    info[local, 0] = total + own_column
    info[local, 1] = total
    pl.semaphore_wait(barrier, spread + members - 2)

    loaded(2, 3, 7, 8)
    mates = [(local + k) % size for k in range(1, size)]
    for k, mate in enumerate(mates):
        to = (half * size + mate, j)
        send(kv_all.at[local], kv_all.at[local], kv_send.at[k], kv_recv.at[local], to)
        send(info.at[local], info.at[local], in_send.at[k], in_recv.at[local], to)

    loaded(14, 15, 16)
    for m, ref in enumerate((gw, uw, dw)):
        for k in range(hid // 128):
            wt[m, k * 128 : (k + 1) * 128, :] = ref[:, k * 128 : (k + 1) * 128].T
    mine = pl.ds(pl.multiple_of(i * piece, 16), piece)

    whole, first, last = (0, 0, 3), (0, 0, 2), (1, 2, 3)

    def w_slot(jj, p, cut):
        return w_all.at[cut[1] : cut[2], jj, :, pl.ds(pl.multiple_of(p * chan, 128), chan)]

    def send_weights(p, part=whole):
        theirs = pl.ds(pl.multiple_of(p * piece, 16), piece)
        n = part[0]
        source = wt.at[part[1] : part[2], theirs, :]
        send(source, w_slot(j, i, part), w_send.at[n, p], w_recv.at[n, i], (p, j))

    def share_weights(p, part=whole):
        slot, n = w_slot(j, p, part), part[0]
        arrived(slot, w_recv.at[n, p])
        send(slot, slot, f_send.at[2 * n, p], f_recv.at[2 * n, p], sibling)
        send(slot, slot, g_send.at[n, p], g_recv.at[n, p], y_peer)

    def share_across(p, part=whole):
        slot, n = w_slot(across, p, part), part[0]
        arrived(slot, g_recv.at[n, p])
        send(slot, slot, f_send.at[2 * n + 1, p], f_recv.at[2 * n + 1, p], sibling)

    columns = pl.ds(pl.multiple_of(i * chan, 128), chan)
    block = wt.at[:, mine, :]
    send(block, w_slot(j, i, whole), g_send.at[0, i], g_recv.at[0, i], y_peer)
    send(block, w_slot(j, i, whole), f_send.at[0, i], f_recv.at[0, i], sibling)
    w_all[:, j, :, columns] = wt[:, mine, :]
    straight = [2 * ranked(n) + x for n in range(depth - 1)]
    crossed = [2 * z + ox] + [2 * ranked(n) + ox for n in range(depth - 1)]
    middle = jnp.logical_or(z == depth // 2 - 1, z == depth // 2)

    @pl.when(middle)
    def _():
        for p in (straight[2], straight[0], straight[1]):
            send_weights(p)

    @pl.when(jnp.logical_not(middle))
    def _():
        send_weights(straight[1])

    send_weights(crossed[0])

    @pl.when(middle)
    def _():
        send_weights(crossed[2], first)

    in_turn = [
        jnp.where(middle, a, b)
        for a, b in zip(
            [straight[0], straight[2], crossed[0], straight[1], crossed[1], crossed[3], crossed[2]],
            [straight[1], crossed[0], straight[0], straight[2], crossed[1], crossed[3], crossed[2]],
        )
    ]

    share_weights(in_turn[0])
    for mate in mates:
        arrived(kv_all.at[mate], kv_recv.at[mate])
        arrived(info.at[mate], in_recv.at[mate])

    before, after = [], [None] * size
    passed = jnp.zeros_like(total)
    for k in range(size):
        before.append(passed)
        passed = passed + info[k, 1]
    passed = jnp.zeros_like(total)
    for k in reversed(range(size)):
        after[k] = passed
        passed = passed + info[k, 1]
    to_end = jnp.concatenate(
        [info[k, 0] + jnp.where(forward_row, after[k], before[k]) for k in range(size)], axis=1
    )
    to_end = jnp.where(half == 0, to_end[0:8], to_end[8:16])
    end_max = jnp.max(to_end, axis=1, keepdims=True)
    share = jnp.transpose(
        jnp.concatenate([jnp.exp(to_end - end_max), jnp.zeros((rows - 8, size * rows), f32)], axis=0)
    )
    share_a = jnp.where(x == 0, share[:, 0:1], share[:, 1:2])
    share_b = share[:, narrow_heads : narrow_heads + 1]
    wa, wb = ca // narrow_heads, cb // 2

    def kv_lanes(start, width):
        return kv_all[:, :, pl.ds(pl.multiple_of(start, 128), width)].reshape(size * rows, width)

    tn = (((0,), (0,)), ((), ()))
    keys_a, keys_b = kv_lanes(x * wa, wa), kv_lanes(2 * ca, cb)
    values_a = (share_a * kv_lanes(ca + x * wa, wa).astype(f32)).astype(bf16)
    values_b = (share_b * kv_lanes(2 * ca + cb + x * wb, wb).astype(f32)).astype(bf16)
    st_out[0:wa, :] = lax.dot_general(keys_a, values_a, tn, preferred_element_type=f32).astype(bf16)
    st_out[wa : wa + cb, :] = lax.dot_general(keys_b, values_b, tn, preferred_element_type=f32).astype(bf16)
    norm_a = jnp.sum(share_a * keys_a.astype(f32), axis=0, keepdims=True)
    norm_b = jnp.sum(share_b * keys_b.astype(f32), axis=0, keepdims=True)
    sn_out[0:1, :] = norm_a
    sn_out[1:2, :] = norm_b[:, 0:wa]
    sn_out[2:3, :] = norm_b[:, wa:]
    sn_out[3:8, :] = jnp.broadcast_to(end_max[0:5], (5, rows))
    mirror = ((i + size) % spread, j)
    send(sn_out, sn_in.at[x], st_send.at[1], sn_recv.at[x], mirror)
    send(st_out, st_in.at[x], st_send.at[0], st_recv.at[x], mirror)

    @pl.when(middle)
    def _():
        for p in (crossed[1], crossed[3]):
            send_weights(p, first)

    @pl.when(jnp.logical_not(middle))
    def _():
        send_weights(straight[0])

    share_weights(in_turn[1])
    arrived(sn_in.at[x], sn_recv.at[x])
    arrived(st_in.at[x], st_recv.at[x])
    send(sn_in.at[x], sn_in.at[x], st_send.at[3], sn_recv.at[x], x_peer)
    send(st_in.at[x], st_in.at[x], st_send.at[2], st_recv.at[x], x_peer)

    @pl.when(jnp.logical_not(middle))
    def _():
        send_weights(straight[2])
        for p in (crossed[2], crossed[3], crossed[1]):
            send_weights(p, first)

    arrived(sn_in.at[ox], sn_recv.at[ox])
    arrived(st_in.at[ox], st_recv.at[ox])

    loaded(1, 6, 4, 9, 11, 12, 0, 13)
    pieces = [None] * size
    forward_sum = jnp.zeros_like(total)
    ahead = [None] * size
    for k in reversed(range(size)):
        ahead[k] = forward_sum
        forward_sum = forward_sum + jnp.where(k < local, info[k, 1], 0.0)
    backward_sum = jnp.zeros_like(total)
    for k in range(size):
        reach = jnp.where(forward_row, ahead[k], backward_sum) + info[k, 0]
        seen = jnp.logical_or(
            jnp.logical_and(forward_row, k < local),
            jnp.logical_and(jnp.logical_not(forward_row), k > local),
        )
        pieces[k] = jnp.where(k == local, own_column, jnp.where(seen, reach, FAR))
        backward_sum = backward_sum + jnp.where(k > local, info[k, 1], 0.0)
    column = jnp.concatenate(pieces, axis=1)
    past = sn_in[x, 3:8, :] + jnp.where(half == 1, forward_sum[0:5], backward_sum[8:13])
    t_at = lax.broadcasted_iota(jnp.int32, (rows, size * rows), 0) + local * rows
    s_at = lax.broadcasted_iota(jnp.int32, (rows, size * rows), 1)
    masks = (s_at <= t_at, s_at >= t_at)
    nt = (((1,), (1,)), ((), ()))
    proj = jnp.zeros((rows, res.shape[1]), f32)
    heads = [(qn, on, opn, 0, ca, h, ca // narrow_heads, h) for h in range(narrow_heads)]
    heads += [
        (qb, ob, opb, 2 * ca, cb, h, cb // broad_heads, narrow_heads + h) for h in range(broad_heads)
    ]
    for query, outgate, outproj, base, group, h, width, row in heads:
        lanes = slice(h * width, (h + 1) * width)
        keys = kv_all[:, :, base + h * width : base + (h + 1) * width].reshape(size * rows, width)
        vals = kv_all[:, :, base + group + h * width : base + group + (h + 1) * width].reshape(
            size * rows, width
        )
        queries = query[:, lanes]
        scores = lax.dot_general(queries, keys, nt, preferred_element_type=f32) * width ** (-0.5)
        if row < narrow_heads:
            memory, normer = st_in[row, 0:wa, :], sn_in[row, 0:1, :]
        else:
            memory = jnp.concatenate([st_in[0, wa:, :], st_in[1, wa:, :]], axis=1)
            normer = jnp.concatenate([sn_in[0, 1:2, :], sn_in[0, 2:3, :]], axis=1)
        recalled = jnp.dot(queries, memory, preferred_element_type=f32) * width ** (-0.5)
        recall_den = jnp.sum(queries.astype(f32) * normer, axis=1, keepdims=True) * width ** (-0.5)
        summed = jnp.zeros((rows, width), f32)
        for direction in range(2):
            at = 8 * direction + row
            weight = jnp.where(
                masks[direction],
                jnp.broadcast_to(column[at : at + 1, :], scores.shape),
                FAR,
            )
            carried = jnp.where(half == 1 - direction, past[row : row + 1, 0:1], FAR)
            top = jnp.maximum(jnp.max(weight, axis=1, keepdims=True), carried)
            kept = jnp.exp(carried - top)
            p = jnp.exp(weight - top) * scores
            den = jnp.sum(p, axis=1, keepdims=True) + kept * recall_den
            num = jnp.dot(p.astype(bf16), vals, preferred_element_type=f32) + kept * recalled
            summed = summed + num / jnp.maximum(jnp.abs(den), 1.0)
        normed = summed * lax.rsqrt(jnp.mean(summed * summed, axis=1, keepdims=True) + EPSILON)
        opened = 1.0 / (1.0 + jnp.exp(-outgate[:, lanes].astype(f32)))
        cell = (normed * opened).astype(bf16)
        proj = proj + jnp.dot(cell, outproj[lanes, :], preferred_element_type=f32)
    pp[...] = proj.astype(bf16).reshape(pp.shape)

    for k in range(1, members):
        q = (j + k) % members
        send(pp.at[q], rs.at[j], p_send.at[q], p_recv.at[j], (i, q))
    share_weights(in_turn[2])
    stream = res[pl.ds(pl.multiple_of(j * own, own), own), :].astype(f32) + pp[j].astype(f32)
    for k in range(1, members):
        q = (j + k) % members
        arrived(rs.at[q], p_recv.at[q])
        stream = stream + rs[q].astype(f32)
    scaled = stream * lax.rsqrt(jnp.mean(stream * stream, axis=1, keepdims=True) + EPSILON)
    x_all[x, z] = (scaled * gain[...].astype(f32).reshape(1, wide)).astype(bf16)

    def pass_x(zz, sem, to):
        slot = x_all.at[x, zz]
        send(slot, slot, sem, x_recv.at[x, zz], to)

    def x_arrived(xx, zz):
        arrived(x_all.at[xx, zz], x_recv.at[xx, zz])

    for n in range(2):
        pass_x(z, x_send.at[0, n], (2 * ranked(n) + x, j))
    pass_x(z, x_send.at[1, z], x_peer)

    def forward_x(n):
        zz = ranked(n)
        x_arrived(x, zz)
        if n != 1:

            @pl.when(middle)
            def _():
                pass_x(zz, x_send.at[0, 2 + n // 2], (2 * ranked(1) + x, j))

        pass_x(zz, x_send.at[1, zz], x_peer)

    for p in (crossed[1], crossed[3], crossed[2]):
        send_weights(p, last)
    share_weights(in_turn[3])
    share_across(i)
    share_across(in_turn[0])
    share_weights(in_turn[4], first)
    share_across(in_turn[1])
    share_weights(in_turn[5], first)
    share_across(in_turn[2])
    share_weights(in_turn[6], first)
    share_across(in_turn[3])
    forward_x(2)
    forward_x(0)
    forward_x(1)
    for p in in_turn[4:]:
        share_weights(p, last)
    for p in in_turn[4:]:
        share_across(p, first)
    for zz in range(depth):
        x_arrived(ox, zz)
    for p in in_turn[4:]:
        share_across(p, last)
    other, other_across = 2 * y + 1 - c, 2 * (1 - y) + 1 - c
    for p, cut in [(i, whole)] + [(p, whole) for p in in_turn[:4]] + [(p, first) for p in in_turn[4:]]:
        arrived(w_slot(other, p, cut), f_recv.at[0, p])
        arrived(w_slot(other_across, p, cut), f_recv.at[1, p])

    units = members * piece

    def hidden_of(xx):
        a = x_all[xx].reshape(depth * own, -1)
        gate = lax.dot_general(a, w_all[0].reshape(units, -1), nt, preferred_element_type=f32)
        up = lax.dot_general(a, w_all[1].reshape(units, -1), nt, preferred_element_type=f32)
        return (gate / (1.0 + jnp.exp(-gate)) * up).astype(bf16)

    def project(xx, hidden):
        got = jnp.dot(hidden, w_all[2].reshape(units, -1), preferred_element_type=f32)
        part[xx] = got.astype(bf16).reshape(depth, own, -1)

    ends = [(z + depth // 2) % depth] + [(z + k) % depth for k in range(1, depth) if 2 * k != depth]
    hidden = hidden_of(ox)
    for p in in_turn[4:]:
        arrived(w_slot(other, p, last), f_recv.at[2, p])
        arrived(w_slot(other_across, p, last), f_recv.at[3, p])
    project(ox, hidden)
    for zz in ends + [z]:
        send(part.at[ox, zz], r1.at[zz], e_send.at[zz], e_recv.at[zz], x_peer)
    project(x, hidden_of(x))
    for zz in ends:
        arrived(r1.at[zz], e_recv.at[zz])
        s2[zz] = (part[x, zz].astype(f32) + r1[zz].astype(f32)).astype(bf16)
        send(s2.at[zz], r3.at[z], z_send.at[zz], z_recv.at[z], (2 * zz + x, j))
    arrived(r1.at[z], e_recv.at[z])
    ffn = part[x, z].astype(f32) + r1[z].astype(f32)
    for zz in ends:
        arrived(r3.at[zz], z_recv.at[zz])
        ffn = ffn + r3[zz].astype(f32)
    out[...] = (stream + 0.5 * ffn).astype(out.dtype)

    for k in range(size - 1):
        sent(kv_all.at[0], kv_send.at[k])
        sent(info.at[0], in_send.at[k])
    sent(st_out, st_send.at[0])
    sent(sn_out, st_send.at[1])
    sent(st_out, st_send.at[2])
    sent(sn_out, st_send.at[3])
    for zz in range(depth):
        slot = x_all.at[x, zz]
        sent(slot, x_send.at[1, zz])
        sent(r1.at[0], e_send.at[zz])
    for n in range(4):
        sent(x_all.at[0, 0], x_send.at[0, n], None if n < 2 else middle)
    late = wt.at[2:3, mine, :]
    early = wt.at[0:2, mine, :]
    for p in straight + crossed[:1]:
        sent(block, w_send.at[0, p])
    for p in crossed[1:]:
        sent(early, w_send.at[0, p])
        sent(late, w_send.at[1, p])
    for p in [i] + in_turn[:4]:
        for ref in (g_send.at[0, p], f_send.at[0, p], f_send.at[1, p]):
            sent(block, ref)
    for p in in_turn[4:]:
        for ref in (g_send.at[0, p], f_send.at[0, p], f_send.at[1, p]):
            sent(early, ref)
        for ref in (g_send.at[1, p], f_send.at[2, p], f_send.at[3, p]):
            sent(late, ref)
    for k in range(1, members):
        sent(rs.at[0], p_send.at[(j + k) % members])
    for zz in ends:
        sent(s2.at[0], z_send.at[zz])


def fused_shards(*args):
    (res, qn, kn, vn, on, gn, qb, kb, vb, ob, gb, opn, opb, gain, gw, uw, dw) = args
    spread, members = lax.axis_size("sp"), lax.axis_size("tp")
    rows, wide = res.shape
    own, depth = rows // members, spread // 2
    chan, hid = gw.shape
    piece = hid // spread
    kvw = 2 * (kn.shape[1] + kb.shape[1])
    bf16, f32 = jnp.bfloat16, jnp.float32
    state_rows = DH_A + DH_B
    v = pltpu.VMEM
    dma = pltpu.SemaphoreType.DMA
    scratch = [
        v((spread // 2, rows, kvw), bf16),
        v((spread // 2, 2, 16, rows), f32),
        v((2, 16, rows), f32),
        v((3, hid, chan), bf16),
        v((3, members, piece, wide), bf16),
        v((members, own, wide), bf16),
        v((members, own, wide), bf16),
        v((2, depth, own, wide), bf16),
        v((2, depth, own, wide), bf16),
        v((depth, own, wide), bf16),
        v((depth, own, wide), bf16),
        v((depth, own, wide), bf16),
        v((state_rows, 128), bf16),
        v((8, rows), f32),
        v((2, state_rows, 128), bf16),
        v((2, 8, rows), f32),
        dma((spread // 2,)),
        dma((spread // 2,)),
        dma((spread // 2,)),
        dma((spread // 2,)),
        dma((2, spread)),
        dma((2, spread)),
        dma((4, spread)),
        dma((4, spread)),
        dma((2, spread)),
        dma((2, spread)),
        dma((members,)),
        dma((members,)),
        dma((2, depth)),
        dma((2, depth)),
        dma((depth,)),
        dma((depth,)),
        dma((depth,)),
        dma((depth,)),
        dma((4,)),
        dma((2,)),
        dma((2,)),
        dma((17,)),
    ]
    scratch += [v(a.shape, a.dtype) for a in (res, qn, on, gn, qb, ob, gb, opn, opb, gain, gw, uw, dw)]
    geometry = (spread, members, wide, gn.shape[1], gb.shape[1])
    return pl.pallas_call(
        functools.partial(fused_kernel, geometry),
        out_shape=jax.ShapeDtypeStruct((own, wide), bf16),
        in_specs=[pl.BlockSpec(memory_space=pltpu.HBM)] * 17,
        out_specs=pl.BlockSpec(memory_space=pltpu.VMEM),
        scratch_shapes=scratch,
        compiler_params=pltpu.CompilerParams(
            collective_id=0, has_side_effects=True, vmem_limit_bytes=40 * 1024 * 1024
        ),
        name="fused",
    )(*[pltpu.with_memory_space_constraint(a, pltpu.HBM) for a in args])


def pick(*args):
    res, kn, gn, gb, gw = args[0], args[2], args[5], args[10], args[14]
    spread, members = lax.axis_size("sp"), lax.axis_size("tp")
    rows = res.shape[0]
    chan, hid = gw.shape
    fits = (
        spread == 8
        and members == 4
        and rows == 128
        and spread * rows <= 2048
        and chan % 128 == 0
        and hid % (16 * spread) == 0
        and hid % 128 == 0
        and (gn.shape[1], gb.shape[1]) == (2, 1)
        and kn.shape[1] == 2 * DH_A
        and DH_A == 128
        and DH_B == 256
    )
    return fused_shards(*args) if fits else shards(*args)


def solution(mesh):
    in_specs = (
        P("sp", None),
        P("sp", "tp"),
        P("sp", "tp"),
        P("sp", "tp"),
        P("sp", "tp"),
        P(None, "tp", "sp"),
        P("sp", "tp"),
        P("sp", "tp"),
        P("sp", "tp"),
        P("sp", "tp"),
        P(None, "tp", "sp"),
        P("tp", None),
        P("tp", None),
        P(),
        P("sp", "tp"),
        P("sp", "tp"),
        P("sp", "tp"),
    )
    out_specs = P(("sp", "tp"), None)
    return jax.shard_map(pick, mesh=mesh, in_specs=in_specs, out_specs=out_specs, check_vma=False)
```

```python
import functools

import jax
import jax.numpy as jnp
from jax import lax
from jax.experimental import pallas as pl
from jax.experimental.pallas import tpu as pltpu
from jax.sharding import PartitionSpec as P

DH_A = 128
DH_B = 256

EPSILON = 1e-06
FAR = -1e30
MESH = pl.DeviceIdType.MESH


def direction_columns(in_gate, log_forget, reverse):
    place, length = lax.axis_index("sp"), lax.axis_size("sp")
    cumulative = lax.cumsum(log_forget, axis=1, reverse=reverse)
    total = cumulative[:, 0] if reverse else cumulative[:, -1]
    toward_end = total[:, None] - cumulative + in_gate
    packed = jnp.concatenate([toward_end, total[:, None]], axis=1)
    every = lax.all_gather(packed, "sp")
    ends, totals = every[:, :, :-1], every[:, :, -1]
    index = jnp.arange(length)
    if reverse:
        between = (index[None, :] > place) & (index[None, :] < index[:, None])
        valid = index > place
    else:
        between = (index[None, :] < place) & (index[None, :] > index[:, None])
        valid = index < place
    offset = jnp.sum(jnp.where(between[:, :, None], totals[None], 0.0), axis=1)
    columns = jnp.where(valid[:, None, None], offset[:, :, None] + ends, FAR)
    own = (in_gate - cumulative)[None]
    columns = jnp.where((index == place)[:, None, None], own, columns)
    return jnp.moveaxis(columns, 0, 1).reshape(in_gate.shape[0], -1)


def group_cell(query, keys, values, outgate, gates, width):
    rows, every = query.shape[0], keys.shape[0]
    place = lax.axis_index("sp")
    heads = query.shape[1] // width
    q = query.reshape(rows, heads, width)
    k = keys.reshape(every, heads, width)
    v = values.reshape(every, heads, width)
    scores = jnp.einsum("thd,shd->hts", q, k, preferred_element_type=jnp.float32) * width ** (-0.5)
    t_at = (place * rows + jnp.arange(rows))[:, None]
    s_at = jnp.arange(every)[None, :]
    summed = 0.0
    for direction in range(2):
        columns = direction_columns(
            gates[direction], jax.nn.log_sigmoid(gates[2 + direction]), direction == 1
        )
        mask = s_at >= t_at if direction else s_at <= t_at
        log_weight = jnp.where(mask[None], columns[:, None, :], FAR)
        top = jnp.max(log_weight, axis=2, keepdims=True)
        weighted = jnp.exp(log_weight - top) * scores
        den = jnp.sum(weighted, axis=2)
        num = jnp.einsum(
            "hts,shd->thd", weighted.astype(jnp.bfloat16), v, preferred_element_type=jnp.float32
        )
        summed = summed + num / jnp.maximum(jnp.abs(jnp.transpose(den)), 1.0)[:, :, None]
    normed = summed * lax.rsqrt(jnp.mean(summed * summed, axis=2, keepdims=True) + EPSILON)
    return (normed.reshape(rows, -1) * jax.nn.sigmoid(outgate.astype(jnp.float32))).astype(
        jnp.bfloat16
    )


def shards(
    residual,
    query_narrow,
    keys_narrow,
    values_narrow,
    outgate_narrow,
    gates_narrow,
    query_broad,
    keys_broad,
    values_broad,
    outgate_broad,
    gates_broad,
    outproj_narrow,
    outproj_broad,
    norm_gain,
    gate_weight,
    up_weight,
    down_weight,
):
    spread = lax.axis_size("sp")
    channels, hidden_own = gate_weight.shape
    stacked = jnp.stack([gate_weight.T, up_weight.T, down_weight.T])
    pieces = stacked.reshape(3, spread, hidden_own // spread, channels)
    pieces = lax.all_to_all(pieces, "sp", split_axis=1, concat_axis=1)
    weights = jnp.swapaxes(pieces, 1, 2).reshape(3, hidden_own // spread, -1)

    narrow, broad = keys_narrow.shape[1], keys_broad.shape[1]
    memory = lax.all_gather(
        jnp.concatenate([keys_narrow, values_narrow, keys_broad, values_broad], axis=1),
        "sp",
        axis=0,
        tiled=True,
    )
    kn, vn = memory[:, :narrow], memory[:, narrow : 2 * narrow]
    kb, vb = memory[:, 2 * narrow : 2 * narrow + broad], memory[:, 2 * narrow + broad :]
    cell_narrow = group_cell(query_narrow, kn, vn, outgate_narrow, gates_narrow, DH_A)
    cell_broad = group_cell(query_broad, kb, vb, outgate_broad, gates_broad, DH_B)

    own_count = residual.shape[0] // lax.axis_size("tp")
    proj = lax.psum_scatter(
        (
            jnp.dot(cell_narrow, outproj_narrow, preferred_element_type=jnp.float32)
            + jnp.dot(cell_broad, outproj_broad, preferred_element_type=jnp.float32)
        ).astype(jnp.bfloat16),
        "tp",
        scatter_dimension=0,
        tiled=True,
    ).astype(jnp.float32)
    offset = lax.axis_index("tp") * own_count
    stream = lax.dynamic_slice_in_dim(residual, offset, own_count, 0).astype(jnp.float32) + proj
    scaled = stream * lax.rsqrt(jnp.mean(stream * stream, axis=1, keepdims=True) + EPSILON)
    normed = (scaled * norm_gain.astype(jnp.float32)).astype(jnp.bfloat16)
    normed = lax.all_gather(normed, ("sp", "tp"), axis=0, tiled=True)
    nt = (((1,), (1,)), ((), ()))
    gate = lax.dot_general(normed, weights[0], nt, preferred_element_type=jnp.float32)
    upward = lax.dot_general(normed, weights[1], nt, preferred_element_type=jnp.float32)
    hidden = (jax.nn.silu(gate) * upward).astype(jnp.bfloat16)
    partial_value = jnp.dot(hidden, weights[2], preferred_element_type=jnp.float32)
    ffn = lax.psum_scatter(
        partial_value.astype(jnp.bfloat16), ("sp", "tp"), scatter_dimension=0, tiled=True
    ).astype(jnp.float32)
    return (stream + 0.5 * ffn).astype(jnp.bfloat16)


def fused_kernel(geometry, *refs):
    spread, members, wide, narrow_heads, broad_heads = geometry
    held, out = refs[:17], refs[17]
    (kv_all, info, gates, wt, w_all, pp, rs, x_all, part, r1, s2, r3) = refs[18:30]
    (st_out, sn_out, st_in, sn_in) = refs[30:34]
    (kv_send, kv_recv, in_send, in_recv, w_send, w_recv, f_send, f_recv, g_send, g_recv) = refs[34:44]
    (p_send, p_recv, x_send, x_recv, e_send, e_recv, z_send, z_recv) = refs[44:52]
    (st_send, st_recv, sn_recv, load_sem) = refs[52:56]
    (res, qn, on, gn, qb, ob, gb, opn, opb, gain, gw, uw, dw) = refs[56:69]
    rows = res.shape[0]
    own = rows // members
    depth = spread // 2
    chan, hid = gw.shape
    piece = hid // spread
    ca, cb = held[2].shape[1], held[7].shape[1]
    i, j = lax.axis_index("sp"), lax.axis_index("tp")
    z, x = i // 2, i % 2
    y, c = j // 2, j % 2
    ox = 1 - x
    size = spread // 2
    half, local = i // size, i % size
    f32, bf16 = jnp.float32, jnp.bfloat16
    sibling, x_peer = (i, j + 1 - 2 * c), (2 * z + ox, j)
    across = (1 - y) * 2 + c
    y_peer = (i, across)

    def ranked(n):
        pick = 0
        for a in range(depth):
            others = sorted(
                (b for b in range(depth) if b != a),
                key=lambda b: (abs(a - b), (a < depth // 2) == (b < depth // 2)),
            )
            pick = pick + jnp.where(z == a, others[n], 0)
        return pick

    def send(src, dst, s_sem, r_sem, to):
        copy = pltpu.make_async_remote_copy(
            src_ref=src, dst_ref=dst, send_sem=s_sem, recv_sem=r_sem, device_id=to, device_id_type=MESH
        )
        copy.start()
        return copy

    def arrived(ref, sem):
        pltpu.make_async_remote_copy(
            src_ref=ref, dst_ref=ref, send_sem=sem, recv_sem=sem, device_id=(i, j), device_id_type=MESH
        ).wait_recv()

    def sent(ref, sem, cond=None):
        def wait():
            pltpu.make_async_remote_copy(
                src_ref=ref, dst_ref=ref, send_sem=sem, recv_sem=sem, device_id=(i, j), device_id_type=MESH
            ).wait_send()

        if cond is None:
            wait()
        else:
            pl.when(cond)(wait)

    barrier = pltpu.get_barrier_semaphore()
    for k in range(1, spread):
        pl.semaphore_signal(barrier, inc=1, device_id=((i + k) % spread, j), device_id_type=MESH)
    for k in range(1, members):
        pl.semaphore_signal(barrier, inc=1, device_id=(i, (j + k) % members), device_id_type=MESH)

    mine_kv = kv_all.at[local]
    targets = {
        5: gn,
        10: gb,
        2: mine_kv.at[:, 0:ca],
        3: mine_kv.at[:, ca : 2 * ca],
        7: mine_kv.at[:, 2 * ca : 2 * ca + cb],
        8: mine_kv.at[:, 2 * ca + cb : 2 * ca + 2 * cb],
        14: gw,
        15: uw,
        16: dw,
        1: qn,
        6: qb,
        4: on,
        9: ob,
        11: opn,
        12: opb,
        0: res,
        13: gain,
    }
    loads = {n: pltpu.make_async_copy(held[n], ref, load_sem.at[n]) for n, ref in targets.items()}
    for load in loads.values():
        load.start()

    def loaded(*numbers):
        for n in numbers:
            loads[n].wait()

    loaded(5, 10)
    gates[...] = jnp.zeros_like(gates)
    for role in range(4):
        at = 8 * (role % 2)
        gates[role // 2, at : at + narrow_heads, :] = gn[role]
        gates[role // 2, at + narrow_heads : at + narrow_heads + broad_heads, :] = gb[role]
    in_gate, pre = gates[0], gates[1]
    forget = jnp.minimum(pre, 0.0) - jnp.log1p(jnp.exp(-jnp.abs(pre)))
    r_at = lax.broadcasted_iota(jnp.int32, (rows, rows), 0)
    c_at = lax.broadcasted_iota(jnp.int32, (rows, rows), 1)
    run = lambda m: jnp.dot(
        forget, m.astype(f32), preferred_element_type=f32, precision=lax.Precision.HIGHEST
    )
    forward_row = lax.broadcasted_iota(jnp.int32, in_gate.shape, 0) < 8
    cumulative = jnp.where(forward_row, run(r_at <= c_at), run(r_at >= c_at))
    total = jnp.where(
        forward_row,
        jnp.broadcast_to(cumulative[:, rows - 1 : rows], in_gate.shape),
        jnp.broadcast_to(cumulative[:, 0:1], in_gate.shape),
    )
    own_column = in_gate - cumulative
    info[local, 0] = total + own_column
    info[local, 1] = total
    pl.semaphore_wait(barrier, spread + members - 2)

    loaded(2, 3, 7, 8)
    mates = [(local + k) % size for k in range(1, size)]
    for k, mate in enumerate(mates):
        to = (half * size + mate, j)
        send(kv_all.at[local], kv_all.at[local], kv_send.at[k], kv_recv.at[local], to)
        send(info.at[local], info.at[local], in_send.at[k], in_recv.at[local], to)

    loaded(14, 15, 16)
    for m, ref in enumerate((gw, uw, dw)):
        for k in range(hid // 128):
            wt[m, k * 128 : (k + 1) * 128, :] = ref[:, k * 128 : (k + 1) * 128].T
    mine = pl.ds(pl.multiple_of(i * piece, 16), piece)

    whole, first, last = (0, 0, 3), (0, 0, 2), (1, 2, 3)

    def w_slot(jj, p, cut):
        return w_all.at[cut[1] : cut[2], jj, :, pl.ds(pl.multiple_of(p * chan, 128), chan)]

    def send_weights(p, part=whole):
        theirs = pl.ds(pl.multiple_of(p * piece, 16), piece)
        n = part[0]
        source = wt.at[part[1] : part[2], theirs, :]
        send(source, w_slot(j, i, part), w_send.at[n, p], w_recv.at[n, i], (p, j))

    def share_weights(p, part=whole):
        slot, n = w_slot(j, p, part), part[0]
        arrived(slot, w_recv.at[n, p])
        send(slot, slot, f_send.at[2 * n, p], f_recv.at[2 * n, p], sibling)
        send(slot, slot, g_send.at[n, p], g_recv.at[n, p], y_peer)

    def share_across(p, part=whole):
        slot, n = w_slot(across, p, part), part[0]
        arrived(slot, g_recv.at[n, p])
        send(slot, slot, f_send.at[2 * n + 1, p], f_recv.at[2 * n + 1, p], sibling)

    columns = pl.ds(pl.multiple_of(i * chan, 128), chan)
    block = wt.at[:, mine, :]
    send(block, w_slot(j, i, whole), g_send.at[0, i], g_recv.at[0, i], y_peer)
    send(block, w_slot(j, i, whole), f_send.at[0, i], f_recv.at[0, i], sibling)
    w_all[:, j, :, columns] = wt[:, mine, :]
    straight = [2 * ranked(n) + x for n in range(depth - 1)]
    crossed = [2 * z + ox] + [2 * ranked(n) + ox for n in range(depth - 1)]
    middle = jnp.logical_or(z == depth // 2 - 1, z == depth // 2)

    @pl.when(middle)
    def _():
        for p in (straight[2], straight[0], straight[1]):
            send_weights(p)

    @pl.when(jnp.logical_not(middle))
    def _():
        send_weights(straight[1])

    send_weights(crossed[0])

    @pl.when(middle)
    def _():
        send_weights(crossed[2], first)

    in_turn = [
        jnp.where(middle, a, b)
        for a, b in zip(
            [straight[0], straight[2], crossed[0], straight[1], crossed[1], crossed[3], crossed[2]],
            [straight[1], crossed[0], straight[0], straight[2], crossed[1], crossed[3], crossed[2]],
        )
    ]

    share_weights(in_turn[0])
    for mate in mates:
        arrived(kv_all.at[mate], kv_recv.at[mate])
        arrived(info.at[mate], in_recv.at[mate])

    before, after = [], [None] * size
    passed = jnp.zeros_like(total)
    for k in range(size):
        before.append(passed)
        passed = passed + info[k, 1]
    passed = jnp.zeros_like(total)
    for k in reversed(range(size)):
        after[k] = passed
        passed = passed + info[k, 1]
    to_end = jnp.concatenate(
        [info[k, 0] + jnp.where(forward_row, after[k], before[k]) for k in range(size)], axis=1
    )
    to_end = jnp.where(half == 0, to_end[0:8], to_end[8:16])
    end_max = jnp.max(to_end, axis=1, keepdims=True)
    share = jnp.transpose(
        jnp.concatenate([jnp.exp(to_end - end_max), jnp.zeros((rows - 8, size * rows), f32)], axis=0)
    )
    share_a = jnp.where(x == 0, share[:, 0:1], share[:, 1:2])
    share_b = share[:, narrow_heads : narrow_heads + 1]
    wa, wb = ca // narrow_heads, cb // 2

    def kv_lanes(start, width):
        return kv_all[:, :, pl.ds(pl.multiple_of(start, 128), width)].reshape(size * rows, width)

    tn = (((0,), (0,)), ((), ()))
    keys_a, keys_b = kv_lanes(x * wa, wa), kv_lanes(2 * ca, cb)
    values_a = (share_a * kv_lanes(ca + x * wa, wa).astype(f32)).astype(bf16)
    values_b = (share_b * kv_lanes(2 * ca + cb + x * wb, wb).astype(f32)).astype(bf16)
    st_out[0:wa, :] = lax.dot_general(keys_a, values_a, tn, preferred_element_type=f32).astype(bf16)
    st_out[wa : wa + cb, :] = lax.dot_general(keys_b, values_b, tn, preferred_element_type=f32).astype(bf16)
    norm_a = jnp.sum(share_a * keys_a.astype(f32), axis=0, keepdims=True)
    norm_b = jnp.sum(share_b * keys_b.astype(f32), axis=0, keepdims=True)
    sn_out[0:1, :] = norm_a
    sn_out[1:2, :] = norm_b[:, 0:wa]
    sn_out[2:3, :] = norm_b[:, wa:]
    sn_out[3:8, :] = jnp.broadcast_to(end_max[0:5], (5, rows))
    mirror = ((i + size) % spread, j)
    send(sn_out, sn_in.at[x], st_send.at[1], sn_recv.at[x], mirror)
    send(st_out, st_in.at[x], st_send.at[0], st_recv.at[x], mirror)

    @pl.when(middle)
    def _():
        for p in (crossed[1], crossed[3]):
            send_weights(p, first)

    @pl.when(jnp.logical_not(middle))
    def _():
        send_weights(straight[0])

    share_weights(in_turn[1])
    arrived(sn_in.at[x], sn_recv.at[x])
    arrived(st_in.at[x], st_recv.at[x])
    send(sn_in.at[x], sn_in.at[x], st_send.at[3], sn_recv.at[x], x_peer)
    send(st_in.at[x], st_in.at[x], st_send.at[2], st_recv.at[x], x_peer)

    @pl.when(jnp.logical_not(middle))
    def _():
        send_weights(straight[2])
        for p in (crossed[2], crossed[3], crossed[1]):
            send_weights(p, first)

    arrived(sn_in.at[ox], sn_recv.at[ox])
    arrived(st_in.at[ox], st_recv.at[ox])

    loaded(1, 6, 4, 9, 11, 12, 0, 13)
    pieces = [None] * size
    forward_sum = jnp.zeros_like(total)
    ahead = [None] * size
    for k in reversed(range(size)):
        ahead[k] = forward_sum
        forward_sum = forward_sum + jnp.where(k < local, info[k, 1], 0.0)
    backward_sum = jnp.zeros_like(total)
    for k in range(size):
        reach = jnp.where(forward_row, ahead[k], backward_sum) + info[k, 0]
        seen = jnp.logical_or(
            jnp.logical_and(forward_row, k < local),
            jnp.logical_and(jnp.logical_not(forward_row), k > local),
        )
        pieces[k] = jnp.where(k == local, own_column, jnp.where(seen, reach, FAR))
        backward_sum = backward_sum + jnp.where(k > local, info[k, 1], 0.0)
    column = jnp.concatenate(pieces, axis=1)
    past = sn_in[x, 3:8, :] + jnp.where(half == 1, forward_sum[0:5], backward_sum[8:13])
    t_at = lax.broadcasted_iota(jnp.int32, (rows, size * rows), 0) + local * rows
    s_at = lax.broadcasted_iota(jnp.int32, (rows, size * rows), 1)
    masks = (s_at <= t_at, s_at >= t_at)
    nt = (((1,), (1,)), ((), ()))
    proj = jnp.zeros((rows, res.shape[1]), f32)
    heads = [(qn, on, opn, 0, ca, h, ca // narrow_heads, h) for h in range(narrow_heads)]
    heads += [
        (qb, ob, opb, 2 * ca, cb, h, cb // broad_heads, narrow_heads + h) for h in range(broad_heads)
    ]
    for query, outgate, outproj, base, group, h, width, row in heads:
        lanes = slice(h * width, (h + 1) * width)
        keys = kv_all[:, :, base + h * width : base + (h + 1) * width].reshape(size * rows, width)
        vals = kv_all[:, :, base + group + h * width : base + group + (h + 1) * width].reshape(
            size * rows, width
        )
        queries = query[:, lanes]
        scores = lax.dot_general(queries, keys, nt, preferred_element_type=f32) * width ** (-0.5)
        if row < narrow_heads:
            memory, normer = st_in[row, 0:wa, :], sn_in[row, 0:1, :]
        else:
            memory = jnp.concatenate([st_in[0, wa:, :], st_in[1, wa:, :]], axis=1)
            normer = jnp.concatenate([sn_in[0, 1:2, :], sn_in[0, 2:3, :]], axis=1)
        recalled = jnp.dot(queries, memory, preferred_element_type=f32) * width ** (-0.5)
        recall_den = jnp.sum(queries.astype(f32) * normer, axis=1, keepdims=True) * width ** (-0.5)
        summed = jnp.zeros((rows, width), f32)
        for direction in range(2):
            at = 8 * direction + row
            weight = jnp.where(
                masks[direction],
                jnp.broadcast_to(column[at : at + 1, :], scores.shape),
                FAR,
            )
            carried = jnp.where(half == 1 - direction, past[row : row + 1, 0:1], FAR)
            top = jnp.maximum(jnp.max(weight, axis=1, keepdims=True), carried)
            kept = jnp.exp(carried - top)
            p = jnp.exp(weight - top) * scores
            den = jnp.sum(p, axis=1, keepdims=True) + kept * recall_den
            num = jnp.dot(p.astype(bf16), vals, preferred_element_type=f32) + kept * recalled
            summed = summed + num / jnp.maximum(jnp.abs(den), 1.0)
        normed = summed * lax.rsqrt(jnp.mean(summed * summed, axis=1, keepdims=True) + EPSILON)
        opened = 1.0 / (1.0 + jnp.exp(-outgate[:, lanes].astype(f32)))
        cell = (normed * opened).astype(bf16)
        proj = proj + jnp.dot(cell, outproj[lanes, :], preferred_element_type=f32)
    pp[...] = proj.astype(bf16).reshape(pp.shape)

    for k in range(1, members):
        q = (j + k) % members
        send(pp.at[q], rs.at[j], p_send.at[q], p_recv.at[j], (i, q))
    share_weights(in_turn[2])
    stream = res[pl.ds(pl.multiple_of(j * own, own), own), :].astype(f32) + pp[j].astype(f32)
    for k in range(1, members):
        q = (j + k) % members
        arrived(rs.at[q], p_recv.at[q])
        stream = stream + rs[q].astype(f32)
    scaled = stream * lax.rsqrt(jnp.mean(stream * stream, axis=1, keepdims=True) + EPSILON)
    x_all[x, z] = (scaled * gain[...].astype(f32).reshape(1, wide)).astype(bf16)

    def pass_x(zz, sem, to):
        slot = x_all.at[x, zz]
        send(slot, slot, sem, x_recv.at[x, zz], to)

    def x_arrived(xx, zz):
        arrived(x_all.at[xx, zz], x_recv.at[xx, zz])

    for n in range(2):
        pass_x(z, x_send.at[0, n], (2 * ranked(n) + x, j))
    pass_x(z, x_send.at[1, z], x_peer)

    def forward_x(n):
        zz = ranked(n)
        x_arrived(x, zz)
        if n != 1:

            @pl.when(middle)
            def _():
                pass_x(zz, x_send.at[0, 2 + n // 2], (2 * ranked(1) + x, j))

        pass_x(zz, x_send.at[1, zz], x_peer)

    for p in (crossed[1], crossed[3], crossed[2]):
        send_weights(p, last)
    share_weights(in_turn[3])
    share_across(i)
    share_across(in_turn[0])
    share_weights(in_turn[4], first)
    share_across(in_turn[1])
    share_weights(in_turn[5], first)
    share_across(in_turn[2])
    share_weights(in_turn[6], first)
    share_across(in_turn[3])
    forward_x(2)
    forward_x(0)
    forward_x(1)
    for p in in_turn[4:]:
        share_weights(p, last)
    for p in in_turn[4:]:
        share_across(p, first)
    for zz in range(depth):
        x_arrived(ox, zz)
    for p in in_turn[4:]:
        share_across(p, last)
    other, other_across = 2 * y + 1 - c, 2 * (1 - y) + 1 - c
    for p, cut in [(i, whole)] + [(p, whole) for p in in_turn[:4]] + [(p, first) for p in in_turn[4:]]:
        arrived(w_slot(other, p, cut), f_recv.at[0, p])
        arrived(w_slot(other_across, p, cut), f_recv.at[1, p])

    units = members * piece

    def hidden_of(xx):
        a = x_all[xx].reshape(depth * own, -1)
        gate = lax.dot_general(a, w_all[0].reshape(units, -1), nt, preferred_element_type=f32)
        up = lax.dot_general(a, w_all[1].reshape(units, -1), nt, preferred_element_type=f32)
        return (gate / (1.0 + jnp.exp(-gate)) * up).astype(bf16)

    def project(xx, hidden):
        got = jnp.dot(hidden, w_all[2].reshape(units, -1), preferred_element_type=f32)
        part[xx] = got.astype(bf16).reshape(depth, own, -1)

    table = ((2, 1, 3), (3, 0, 2), (0, 1, 3), (0, 1, 2))
    ends = [sum(jnp.where(z == a, table[a][n], 0) for a in range(depth)) for n in range(depth - 1)]
    hidden = hidden_of(ox)
    for p in in_turn[4:]:
        arrived(w_slot(other, p, last), f_recv.at[2, p])
        arrived(w_slot(other_across, p, last), f_recv.at[3, p])
    project(ox, hidden)
    for zz in ends + [z]:
        send(part.at[ox, zz], r1.at[zz], e_send.at[zz], e_recv.at[zz], x_peer)
    project(x, hidden_of(x))
    for zz in ends:
        arrived(r1.at[zz], e_recv.at[zz])
        s2[zz] = (part[x, zz].astype(f32) + r1[zz].astype(f32)).astype(bf16)
        send(s2.at[zz], r3.at[z], z_send.at[zz], z_recv.at[z], (2 * zz + x, j))
    arrived(r1.at[z], e_recv.at[z])
    ffn = part[x, z].astype(f32) + r1[z].astype(f32)
    for zz in ends:
        arrived(r3.at[zz], z_recv.at[zz])
        ffn = ffn + r3[zz].astype(f32)
    out[...] = (stream + 0.5 * ffn).astype(out.dtype)

    for k in range(size - 1):
        sent(kv_all.at[0], kv_send.at[k])
        sent(info.at[0], in_send.at[k])
    sent(st_out, st_send.at[0])
    sent(sn_out, st_send.at[1])
    sent(st_out, st_send.at[2])
    sent(sn_out, st_send.at[3])
    for zz in range(depth):
        slot = x_all.at[x, zz]
        sent(slot, x_send.at[1, zz])
        sent(r1.at[0], e_send.at[zz])
    for n in range(4):
        sent(x_all.at[0, 0], x_send.at[0, n], None if n < 2 else middle)
    late = wt.at[2:3, mine, :]
    early = wt.at[0:2, mine, :]
    for p in straight + crossed[:1]:
        sent(block, w_send.at[0, p])
    for p in crossed[1:]:
        sent(early, w_send.at[0, p])
        sent(late, w_send.at[1, p])
    for p in [i] + in_turn[:4]:
        for ref in (g_send.at[0, p], f_send.at[0, p], f_send.at[1, p]):
            sent(block, ref)
    for p in in_turn[4:]:
        for ref in (g_send.at[0, p], f_send.at[0, p], f_send.at[1, p]):
            sent(early, ref)
        for ref in (g_send.at[1, p], f_send.at[2, p], f_send.at[3, p]):
            sent(late, ref)
    for k in range(1, members):
        sent(rs.at[0], p_send.at[(j + k) % members])
    for zz in ends:
        sent(s2.at[0], z_send.at[zz])


def fused_shards(*args):
    (res, qn, kn, vn, on, gn, qb, kb, vb, ob, gb, opn, opb, gain, gw, uw, dw) = args
    spread, members = lax.axis_size("sp"), lax.axis_size("tp")
    rows, wide = res.shape
    own, depth = rows // members, spread // 2
    chan, hid = gw.shape
    piece = hid // spread
    kvw = 2 * (kn.shape[1] + kb.shape[1])
    bf16, f32 = jnp.bfloat16, jnp.float32
    state_rows = DH_A + DH_B
    v = pltpu.VMEM
    dma = pltpu.SemaphoreType.DMA
    scratch = [
        v((spread // 2, rows, kvw), bf16),
        v((spread // 2, 2, 16, rows), f32),
        v((2, 16, rows), f32),
        v((3, hid, chan), bf16),
        v((3, members, piece, wide), bf16),
        v((members, own, wide), bf16),
        v((members, own, wide), bf16),
        v((2, depth, own, wide), bf16),
        v((2, depth, own, wide), bf16),
        v((depth, own, wide), bf16),
        v((depth, own, wide), bf16),
        v((depth, own, wide), bf16),
        v((state_rows, 128), bf16),
        v((8, rows), f32),
        v((2, state_rows, 128), bf16),
        v((2, 8, rows), f32),
        dma((spread // 2,)),
        dma((spread // 2,)),
        dma((spread // 2,)),
        dma((spread // 2,)),
        dma((2, spread)),
        dma((2, spread)),
        dma((4, spread)),
        dma((4, spread)),
        dma((2, spread)),
        dma((2, spread)),
        dma((members,)),
        dma((members,)),
        dma((2, depth)),
        dma((2, depth)),
        dma((depth,)),
        dma((depth,)),
        dma((depth,)),
        dma((depth,)),
        dma((4,)),
        dma((2,)),
        dma((2,)),
        dma((17,)),
    ]
    scratch += [v(a.shape, a.dtype) for a in (res, qn, on, gn, qb, ob, gb, opn, opb, gain, gw, uw, dw)]
    geometry = (spread, members, wide, gn.shape[1], gb.shape[1])
    return pl.pallas_call(
        functools.partial(fused_kernel, geometry),
        out_shape=jax.ShapeDtypeStruct((own, wide), bf16),
        in_specs=[pl.BlockSpec(memory_space=pltpu.HBM)] * 17,
        out_specs=pl.BlockSpec(memory_space=pltpu.VMEM),
        scratch_shapes=scratch,
        compiler_params=pltpu.CompilerParams(
            collective_id=0, has_side_effects=True, vmem_limit_bytes=40 * 1024 * 1024
        ),
        name="fused",
    )(*[pltpu.with_memory_space_constraint(a, pltpu.HBM) for a in args])


def pick(*args):
    res, kn, gn, gb, gw = args[0], args[2], args[5], args[10], args[14]
    spread, members = lax.axis_size("sp"), lax.axis_size("tp")
    rows = res.shape[0]
    chan, hid = gw.shape
    fits = (
        spread == 8
        and members == 4
        and rows == 128
        and spread * rows <= 2048
        and chan % 128 == 0
        and hid % (16 * spread) == 0
        and hid % 128 == 0
        and (gn.shape[1], gb.shape[1]) == (2, 1)
        and kn.shape[1] == 2 * DH_A
        and DH_A == 128
        and DH_B == 256
    )
    return fused_shards(*args) if fits else shards(*args)


def solution(mesh):
    in_specs = (
        P("sp", None),
        P("sp", "tp"),
        P("sp", "tp"),
        P("sp", "tp"),
        P("sp", "tp"),
        P(None, "tp", "sp"),
        P("sp", "tp"),
        P("sp", "tp"),
        P("sp", "tp"),
        P("sp", "tp"),
        P(None, "tp", "sp"),
        P("tp", None),
        P("tp", None),
        P(),
        P("sp", "tp"),
        P("sp", "tp"),
        P("sp", "tp"),
    )
    out_specs = P(("sp", "tp"), None)
    return jax.shard_map(pick, mesh=mesh, in_specs=in_specs, out_specs=out_specs, check_vma=False)
```

```python
import functools

import jax
import jax.numpy as jnp
from jax import lax
from jax.experimental import pallas as pl
from jax.experimental.pallas import tpu as pltpu
from jax.sharding import PartitionSpec as P

DH_A = 128
DH_B = 256

EPSILON = 1e-06
FAR = -1e30
MESH = pl.DeviceIdType.MESH


def direction_columns(in_gate, log_forget, reverse):
    place, length = lax.axis_index("sp"), lax.axis_size("sp")
    cumulative = lax.cumsum(log_forget, axis=1, reverse=reverse)
    total = cumulative[:, 0] if reverse else cumulative[:, -1]
    toward_end = total[:, None] - cumulative + in_gate
    packed = jnp.concatenate([toward_end, total[:, None]], axis=1)
    every = lax.all_gather(packed, "sp")
    ends, totals = every[:, :, :-1], every[:, :, -1]
    index = jnp.arange(length)
    if reverse:
        between = (index[None, :] > place) & (index[None, :] < index[:, None])
        valid = index > place
    else:
        between = (index[None, :] < place) & (index[None, :] > index[:, None])
        valid = index < place
    offset = jnp.sum(jnp.where(between[:, :, None], totals[None], 0.0), axis=1)
    columns = jnp.where(valid[:, None, None], offset[:, :, None] + ends, FAR)
    own = (in_gate - cumulative)[None]
    columns = jnp.where((index == place)[:, None, None], own, columns)
    return jnp.moveaxis(columns, 0, 1).reshape(in_gate.shape[0], -1)


def group_cell(query, keys, values, outgate, gates, width):
    rows, every = query.shape[0], keys.shape[0]
    place = lax.axis_index("sp")
    heads = query.shape[1] // width
    q = query.reshape(rows, heads, width)
    k = keys.reshape(every, heads, width)
    v = values.reshape(every, heads, width)
    scores = jnp.einsum("thd,shd->hts", q, k, preferred_element_type=jnp.float32) * width ** (-0.5)
    t_at = (place * rows + jnp.arange(rows))[:, None]
    s_at = jnp.arange(every)[None, :]
    summed = 0.0
    for direction in range(2):
        columns = direction_columns(
            gates[direction], jax.nn.log_sigmoid(gates[2 + direction]), direction == 1
        )
        mask = s_at >= t_at if direction else s_at <= t_at
        log_weight = jnp.where(mask[None], columns[:, None, :], FAR)
        top = jnp.max(log_weight, axis=2, keepdims=True)
        weighted = jnp.exp(log_weight - top) * scores
        den = jnp.sum(weighted, axis=2)
        num = jnp.einsum(
            "hts,shd->thd", weighted.astype(jnp.bfloat16), v, preferred_element_type=jnp.float32
        )
        summed = summed + num / jnp.maximum(jnp.abs(jnp.transpose(den)), 1.0)[:, :, None]
    normed = summed * lax.rsqrt(jnp.mean(summed * summed, axis=2, keepdims=True) + EPSILON)
    return (normed.reshape(rows, -1) * jax.nn.sigmoid(outgate.astype(jnp.float32))).astype(
        jnp.bfloat16
    )


def shards(
    residual,
    query_narrow,
    keys_narrow,
    values_narrow,
    outgate_narrow,
    gates_narrow,
    query_broad,
    keys_broad,
    values_broad,
    outgate_broad,
    gates_broad,
    outproj_narrow,
    outproj_broad,
    norm_gain,
    gate_weight,
    up_weight,
    down_weight,
):
    spread = lax.axis_size("sp")
    channels, hidden_own = gate_weight.shape
    stacked = jnp.stack([gate_weight.T, up_weight.T, down_weight.T])
    pieces = stacked.reshape(3, spread, hidden_own // spread, channels)
    pieces = lax.all_to_all(pieces, "sp", split_axis=1, concat_axis=1)
    weights = jnp.swapaxes(pieces, 1, 2).reshape(3, hidden_own // spread, -1)

    narrow, broad = keys_narrow.shape[1], keys_broad.shape[1]
    memory = lax.all_gather(
        jnp.concatenate([keys_narrow, values_narrow, keys_broad, values_broad], axis=1),
        "sp",
        axis=0,
        tiled=True,
    )
    kn, vn = memory[:, :narrow], memory[:, narrow : 2 * narrow]
    kb, vb = memory[:, 2 * narrow : 2 * narrow + broad], memory[:, 2 * narrow + broad :]
    cell_narrow = group_cell(query_narrow, kn, vn, outgate_narrow, gates_narrow, DH_A)
    cell_broad = group_cell(query_broad, kb, vb, outgate_broad, gates_broad, DH_B)

    own_count = residual.shape[0] // lax.axis_size("tp")
    proj = lax.psum_scatter(
        (
            jnp.dot(cell_narrow, outproj_narrow, preferred_element_type=jnp.float32)
            + jnp.dot(cell_broad, outproj_broad, preferred_element_type=jnp.float32)
        ).astype(jnp.bfloat16),
        "tp",
        scatter_dimension=0,
        tiled=True,
    ).astype(jnp.float32)
    offset = lax.axis_index("tp") * own_count
    stream = lax.dynamic_slice_in_dim(residual, offset, own_count, 0).astype(jnp.float32) + proj
    scaled = stream * lax.rsqrt(jnp.mean(stream * stream, axis=1, keepdims=True) + EPSILON)
    normed = (scaled * norm_gain.astype(jnp.float32)).astype(jnp.bfloat16)
    normed = lax.all_gather(normed, ("sp", "tp"), axis=0, tiled=True)
    nt = (((1,), (1,)), ((), ()))
    gate = lax.dot_general(normed, weights[0], nt, preferred_element_type=jnp.float32)
    upward = lax.dot_general(normed, weights[1], nt, preferred_element_type=jnp.float32)
    hidden = (jax.nn.silu(gate) * upward).astype(jnp.bfloat16)
    partial_value = jnp.dot(hidden, weights[2], preferred_element_type=jnp.float32)
    ffn = lax.psum_scatter(
        partial_value.astype(jnp.bfloat16), ("sp", "tp"), scatter_dimension=0, tiled=True
    ).astype(jnp.float32)
    return (stream + 0.5 * ffn).astype(jnp.bfloat16)


def fused_kernel(geometry, *refs):
    spread, members, wide, narrow_heads, broad_heads = geometry
    held, out = refs[:17], refs[17]
    (kv_all, info, gates, wt, w_all, pp, rs, x_all, part, r1, s2, r3) = refs[18:30]
    (st_out, sn_out, st_in, sn_in) = refs[30:34]
    (kv_send, kv_recv, in_send, in_recv, w_send, w_recv, f_send, f_recv, g_send, g_recv) = refs[34:44]
    (p_send, p_recv, x_send, x_recv, e_send, e_recv, z_send, z_recv) = refs[44:52]
    (st_send, st_recv, sn_recv, load_sem) = refs[52:56]
    (res, qn, on, gn, qb, ob, gb, opn, opb, gain, gw, uw, dw) = refs[56:69]
    rows = res.shape[0]
    own = rows // members
    depth = spread // 2
    chan, hid = gw.shape
    piece = hid // spread
    ca, cb = held[2].shape[1], held[7].shape[1]
    i, j = lax.axis_index("sp"), lax.axis_index("tp")
    z, x = i // 2, i % 2
    y, c = j // 2, j % 2
    ox = 1 - x
    size = spread // 2
    half, local = i // size, i % size
    f32, bf16 = jnp.float32, jnp.bfloat16
    sibling, x_peer = (i, j + 1 - 2 * c), (2 * z + ox, j)
    across = (1 - y) * 2 + c
    y_peer = (i, across)

    def ranked(n):
        pick = 0
        for a in range(depth):
            others = sorted(
                (b for b in range(depth) if b != a),
                key=lambda b: (abs(a - b), (a < depth // 2) == (b < depth // 2)),
            )
            pick = pick + jnp.where(z == a, others[n], 0)
        return pick

    def send(src, dst, s_sem, r_sem, to):
        copy = pltpu.make_async_remote_copy(
            src_ref=src, dst_ref=dst, send_sem=s_sem, recv_sem=r_sem, device_id=to, device_id_type=MESH
        )
        copy.start()
        return copy

    def arrived(ref, sem):
        pltpu.make_async_remote_copy(
            src_ref=ref, dst_ref=ref, send_sem=sem, recv_sem=sem, device_id=(i, j), device_id_type=MESH
        ).wait_recv()

    def sent(ref, sem, cond=None):
        def wait():
            pltpu.make_async_remote_copy(
                src_ref=ref, dst_ref=ref, send_sem=sem, recv_sem=sem, device_id=(i, j), device_id_type=MESH
            ).wait_send()

        if cond is None:
            wait()
        else:
            pl.when(cond)(wait)

    barrier = pltpu.get_barrier_semaphore()
    for k in range(1, spread):
        pl.semaphore_signal(barrier, inc=1, device_id=((i + k) % spread, j), device_id_type=MESH)
    for k in range(1, members):
        pl.semaphore_signal(barrier, inc=1, device_id=(i, (j + k) % members), device_id_type=MESH)

    mine_kv = kv_all.at[local]
    targets = {
        5: gn,
        10: gb,
        2: mine_kv.at[:, 0:ca],
        3: mine_kv.at[:, ca : 2 * ca],
        7: mine_kv.at[:, 2 * ca : 2 * ca + cb],
        8: mine_kv.at[:, 2 * ca + cb : 2 * ca + 2 * cb],
        14: gw,
        15: uw,
        16: dw,
        1: qn,
        6: qb,
        4: on,
        9: ob,
        11: opn,
        12: opb,
        0: res,
        13: gain,
    }
    loads = {n: pltpu.make_async_copy(held[n], ref, load_sem.at[n]) for n, ref in targets.items()}
    for load in loads.values():
        load.start()

    def loaded(*numbers):
        for n in numbers:
            loads[n].wait()

    loaded(5, 10)
    gates[...] = jnp.zeros_like(gates)
    for role in range(4):
        at = 8 * (role % 2)
        gates[role // 2, at : at + narrow_heads, :] = gn[role]
        gates[role // 2, at + narrow_heads : at + narrow_heads + broad_heads, :] = gb[role]
    in_gate, pre = gates[0], gates[1]
    forget = jnp.minimum(pre, 0.0) - jnp.log1p(jnp.exp(-jnp.abs(pre)))
    r_at = lax.broadcasted_iota(jnp.int32, (rows, rows), 0)
    c_at = lax.broadcasted_iota(jnp.int32, (rows, rows), 1)
    run = lambda m: jnp.dot(
        forget, m.astype(f32), preferred_element_type=f32, precision=lax.Precision.HIGHEST
    )
    forward_row = lax.broadcasted_iota(jnp.int32, in_gate.shape, 0) < 8
    cumulative = jnp.where(forward_row, run(r_at <= c_at), run(r_at >= c_at))
    total = jnp.where(
        forward_row,
        jnp.broadcast_to(cumulative[:, rows - 1 : rows], in_gate.shape),
        jnp.broadcast_to(cumulative[:, 0:1], in_gate.shape),
    )
    own_column = in_gate - cumulative
    info[local, 0] = total + own_column
    info[local, 1] = total
    pl.semaphore_wait(barrier, spread + members - 2)

    loaded(2, 3, 7, 8)
    mates = [(local + k) % size for k in range(1, size)]
    for k, mate in enumerate(mates):
        to = (half * size + mate, j)
        send(kv_all.at[local], kv_all.at[local], kv_send.at[k], kv_recv.at[local], to)
        send(info.at[local], info.at[local], in_send.at[k], in_recv.at[local], to)

    loaded(14, 15, 16)
    for m, ref in enumerate((gw, uw, dw)):
        for k in range(hid // 128):
            wt[m, k * 128 : (k + 1) * 128, :] = ref[:, k * 128 : (k + 1) * 128].T
    mine = pl.ds(pl.multiple_of(i * piece, 16), piece)

    whole, first, last = (0, 0, 3), (0, 0, 2), (1, 2, 3)

    def w_slot(jj, p, cut):
        return w_all.at[cut[1] : cut[2], jj, :, pl.ds(pl.multiple_of(p * chan, 128), chan)]

    def send_weights(p, part=whole):
        theirs = pl.ds(pl.multiple_of(p * piece, 16), piece)
        n = part[0]
        source = wt.at[part[1] : part[2], theirs, :]
        send(source, w_slot(j, i, part), w_send.at[n, p], w_recv.at[n, i], (p, j))

    def share_weights(p, part=whole):
        slot, n = w_slot(j, p, part), part[0]
        arrived(slot, w_recv.at[n, p])
        send(slot, slot, f_send.at[2 * n, p], f_recv.at[2 * n, p], sibling)
        send(slot, slot, g_send.at[n, p], g_recv.at[n, p], y_peer)

    def share_across(p, part=whole):
        slot, n = w_slot(across, p, part), part[0]
        arrived(slot, g_recv.at[n, p])
        send(slot, slot, f_send.at[2 * n + 1, p], f_recv.at[2 * n + 1, p], sibling)

    columns = pl.ds(pl.multiple_of(i * chan, 128), chan)
    block = wt.at[:, mine, :]
    send(block, w_slot(j, i, whole), g_send.at[0, i], g_recv.at[0, i], y_peer)
    send(block, w_slot(j, i, whole), f_send.at[0, i], f_recv.at[0, i], sibling)
    w_all[:, j, :, columns] = wt[:, mine, :]
    straight = [2 * ranked(n) + x for n in range(depth - 1)]
    crossed = [2 * z + ox] + [2 * ranked(n) + ox for n in range(depth - 1)]
    middle = jnp.logical_or(z == depth // 2 - 1, z == depth // 2)

    @pl.when(middle)
    def _():
        for p in (straight[2], straight[0], straight[1]):
            send_weights(p)

    @pl.when(jnp.logical_not(middle))
    def _():
        send_weights(straight[1])

    send_weights(crossed[0])

    @pl.when(middle)
    def _():
        send_weights(crossed[2], first)

    in_turn = [
        jnp.where(middle, a, b)
        for a, b in zip(
            [straight[0], straight[2], crossed[0], straight[1], crossed[1], crossed[3], crossed[2]],
            [straight[1], crossed[0], straight[0], straight[2], crossed[1], crossed[3], crossed[2]],
        )
    ]

    share_weights(in_turn[0])
    for mate in mates:
        arrived(kv_all.at[mate], kv_recv.at[mate])
        arrived(info.at[mate], in_recv.at[mate])

    before, after = [], [None] * size
    passed = jnp.zeros_like(total)
    for k in range(size):
        before.append(passed)
        passed = passed + info[k, 1]
    passed = jnp.zeros_like(total)
    for k in reversed(range(size)):
        after[k] = passed
        passed = passed + info[k, 1]
    to_end = jnp.concatenate(
        [info[k, 0] + jnp.where(forward_row, after[k], before[k]) for k in range(size)], axis=1
    )
    to_end = jnp.where(half == 0, to_end[0:8], to_end[8:16])
    end_max = jnp.max(to_end, axis=1, keepdims=True)
    share = jnp.transpose(
        jnp.concatenate([jnp.exp(to_end - end_max), jnp.zeros((rows - 8, size * rows), f32)], axis=0)
    )
    share_a = jnp.where(x == 0, share[:, 0:1], share[:, 1:2])
    share_b = share[:, narrow_heads : narrow_heads + 1]
    wa, wb = ca // narrow_heads, cb // 2

    def kv_lanes(start, width):
        return kv_all[:, :, pl.ds(pl.multiple_of(start, 128), width)].reshape(size * rows, width)

    tn = (((0,), (0,)), ((), ()))
    keys_a, keys_b = kv_lanes(x * wa, wa), kv_lanes(2 * ca, cb)
    values_a = (share_a * kv_lanes(ca + x * wa, wa).astype(f32)).astype(bf16)
    values_b = (share_b * kv_lanes(2 * ca + cb + x * wb, wb).astype(f32)).astype(bf16)
    st_out[0:wa, :] = lax.dot_general(keys_a, values_a, tn, preferred_element_type=f32).astype(bf16)
    st_out[wa : wa + cb, :] = lax.dot_general(keys_b, values_b, tn, preferred_element_type=f32).astype(bf16)
    norm_a = jnp.sum(share_a * keys_a.astype(f32), axis=0, keepdims=True)
    norm_b = jnp.sum(share_b * keys_b.astype(f32), axis=0, keepdims=True)
    sn_out[0:1, :] = norm_a
    sn_out[1:2, :] = norm_b[:, 0:wa]
    sn_out[2:3, :] = norm_b[:, wa:]
    sn_out[3:8, :] = jnp.broadcast_to(end_max[0:5], (5, rows))
    mirror = ((i + size) % spread, j)
    send(sn_out, sn_in.at[x], st_send.at[1], sn_recv.at[x], mirror)
    send(st_out, st_in.at[x], st_send.at[0], st_recv.at[x], mirror)

    @pl.when(middle)
    def _():
        for p in (crossed[1], crossed[3]):
            send_weights(p, first)

    @pl.when(jnp.logical_not(middle))
    def _():
        send_weights(straight[0])

    share_weights(in_turn[1])
    arrived(sn_in.at[x], sn_recv.at[x])
    arrived(st_in.at[x], st_recv.at[x])
    send(sn_in.at[x], sn_in.at[x], st_send.at[3], sn_recv.at[x], x_peer)
    send(st_in.at[x], st_in.at[x], st_send.at[2], st_recv.at[x], x_peer)

    @pl.when(jnp.logical_not(middle))
    def _():
        send_weights(straight[2])
        for p in (crossed[2], crossed[3], crossed[1]):
            send_weights(p, first)

    share_weights(in_turn[2])
    arrived(sn_in.at[ox], sn_recv.at[ox])
    arrived(st_in.at[ox], st_recv.at[ox])

    loaded(1, 6, 4, 9, 11, 12, 0, 13)
    pieces = [None] * size
    forward_sum = jnp.zeros_like(total)
    ahead = [None] * size
    for k in reversed(range(size)):
        ahead[k] = forward_sum
        forward_sum = forward_sum + jnp.where(k < local, info[k, 1], 0.0)
    backward_sum = jnp.zeros_like(total)
    for k in range(size):
        reach = jnp.where(forward_row, ahead[k], backward_sum) + info[k, 0]
        seen = jnp.logical_or(
            jnp.logical_and(forward_row, k < local),
            jnp.logical_and(jnp.logical_not(forward_row), k > local),
        )
        pieces[k] = jnp.where(k == local, own_column, jnp.where(seen, reach, FAR))
        backward_sum = backward_sum + jnp.where(k > local, info[k, 1], 0.0)
    column = jnp.concatenate(pieces, axis=1)
    past = sn_in[x, 3:8, :] + jnp.where(half == 1, forward_sum[0:5], backward_sum[8:13])
    t_at = lax.broadcasted_iota(jnp.int32, (rows, size * rows), 0) + local * rows
    s_at = lax.broadcasted_iota(jnp.int32, (rows, size * rows), 1)
    masks = (s_at <= t_at, s_at >= t_at)
    nt = (((1,), (1,)), ((), ()))
    proj = jnp.zeros((rows, res.shape[1]), f32)
    heads = [(qn, on, opn, 0, ca, h, ca // narrow_heads, h) for h in range(narrow_heads)]
    heads += [
        (qb, ob, opb, 2 * ca, cb, h, cb // broad_heads, narrow_heads + h) for h in range(broad_heads)
    ]
    for query, outgate, outproj, base, group, h, width, row in heads:
        lanes = slice(h * width, (h + 1) * width)
        keys = kv_all[:, :, base + h * width : base + (h + 1) * width].reshape(size * rows, width)
        vals = kv_all[:, :, base + group + h * width : base + group + (h + 1) * width].reshape(
            size * rows, width
        )
        queries = query[:, lanes]
        scores = lax.dot_general(queries, keys, nt, preferred_element_type=f32) * width ** (-0.5)
        if row < narrow_heads:
            memory, normer = st_in[row, 0:wa, :], sn_in[row, 0:1, :]
        else:
            memory = jnp.concatenate([st_in[0, wa:, :], st_in[1, wa:, :]], axis=1)
            normer = jnp.concatenate([sn_in[0, 1:2, :], sn_in[0, 2:3, :]], axis=1)
        recalled = jnp.dot(queries, memory, preferred_element_type=f32) * width ** (-0.5)
        recall_den = jnp.sum(queries.astype(f32) * normer, axis=1, keepdims=True) * width ** (-0.5)
        summed = jnp.zeros((rows, width), f32)
        for direction in range(2):
            at = 8 * direction + row
            weight = jnp.where(
                masks[direction],
                jnp.broadcast_to(column[at : at + 1, :], scores.shape),
                FAR,
            )
            carried = jnp.where(half == 1 - direction, past[row : row + 1, 0:1], FAR)
            top = jnp.maximum(jnp.max(weight, axis=1, keepdims=True), carried)
            kept = jnp.exp(carried - top)
            p = jnp.exp(weight - top) * scores
            den = jnp.sum(p, axis=1, keepdims=True) + kept * recall_den
            num = jnp.dot(p.astype(bf16), vals, preferred_element_type=f32) + kept * recalled
            summed = summed + num / jnp.maximum(jnp.abs(den), 1.0)
        normed = summed * lax.rsqrt(jnp.mean(summed * summed, axis=1, keepdims=True) + EPSILON)
        opened = 1.0 / (1.0 + jnp.exp(-outgate[:, lanes].astype(f32)))
        cell = (normed * opened).astype(bf16)
        proj = proj + jnp.dot(cell, outproj[lanes, :], preferred_element_type=f32)
    pp[...] = proj.astype(bf16).reshape(pp.shape)

    for k in range(1, members):
        q = (j + k) % members
        send(pp.at[q], rs.at[j], p_send.at[q], p_recv.at[j], (i, q))
    stream = res[pl.ds(pl.multiple_of(j * own, own), own), :].astype(f32) + pp[j].astype(f32)
    for k in range(1, members):
        q = (j + k) % members
        arrived(rs.at[q], p_recv.at[q])
        stream = stream + rs[q].astype(f32)
    scaled = stream * lax.rsqrt(jnp.mean(stream * stream, axis=1, keepdims=True) + EPSILON)
    x_all[x, z] = (scaled * gain[...].astype(f32).reshape(1, wide)).astype(bf16)

    def pass_x(zz, sem, to):
        slot = x_all.at[x, zz]
        send(slot, slot, sem, x_recv.at[x, zz], to)

    def x_arrived(xx, zz):
        arrived(x_all.at[xx, zz], x_recv.at[xx, zz])

    for n in range(2):
        pass_x(z, x_send.at[0, n], (2 * ranked(n) + x, j))
    pass_x(z, x_send.at[1, z], x_peer)

    def forward_x(n):
        zz = ranked(n)
        x_arrived(x, zz)
        if n != 1:

            @pl.when(middle)
            def _():
                pass_x(zz, x_send.at[0, 2 + n // 2], (2 * ranked(1) + x, j))

        pass_x(zz, x_send.at[1, zz], x_peer)

    for p in (crossed[1], crossed[3], crossed[2]):
        send_weights(p, last)
    share_weights(in_turn[3])
    share_across(i)
    share_across(in_turn[0])
    share_weights(in_turn[4], first)
    share_across(in_turn[1])
    share_weights(in_turn[5], first)
    share_across(in_turn[2])
    share_weights(in_turn[6], first)
    share_across(in_turn[3])
    forward_x(2)
    forward_x(0)
    forward_x(1)
    for p in in_turn[4:]:
        share_weights(p, last)
    for p in in_turn[4:]:
        share_across(p, first)
    for zz in range(depth):
        x_arrived(ox, zz)
    for p in in_turn[4:]:
        share_across(p, last)
    other, other_across = 2 * y + 1 - c, 2 * (1 - y) + 1 - c
    for p, cut in [(i, whole)] + [(p, whole) for p in in_turn[:4]] + [(p, first) for p in in_turn[4:]]:
        arrived(w_slot(other, p, cut), f_recv.at[0, p])
        arrived(w_slot(other_across, p, cut), f_recv.at[1, p])

    units = members * piece

    def hidden_of(xx):
        a = x_all[xx].reshape(depth * own, -1)
        gate = lax.dot_general(a, w_all[0].reshape(units, -1), nt, preferred_element_type=f32)
        up = lax.dot_general(a, w_all[1].reshape(units, -1), nt, preferred_element_type=f32)
        return (gate / (1.0 + jnp.exp(-gate)) * up).astype(bf16)

    def project(xx, hidden):
        got = jnp.dot(hidden, w_all[2].reshape(units, -1), preferred_element_type=f32)
        part[xx] = got.astype(bf16).reshape(depth, own, -1)

    table = ((2, 3, 1), (3, 0, 2), (0, 1, 3), (0, 1, 2))
    ends = [sum(jnp.where(z == a, table[a][n], 0) for a in range(depth)) for n in range(depth - 1)]
    hidden = hidden_of(ox)
    for p in in_turn[4:]:
        arrived(w_slot(other, p, last), f_recv.at[2, p])
        arrived(w_slot(other_across, p, last), f_recv.at[3, p])
    project(ox, hidden)
    for zz in ends + [z]:
        send(part.at[ox, zz], r1.at[zz], e_send.at[zz], e_recv.at[zz], x_peer)
    project(x, hidden_of(x))
    for zz in ends:
        arrived(r1.at[zz], e_recv.at[zz])
        s2[zz] = (part[x, zz].astype(f32) + r1[zz].astype(f32)).astype(bf16)
        send(s2.at[zz], r3.at[z], z_send.at[zz], z_recv.at[z], (2 * zz + x, j))
    arrived(r1.at[z], e_recv.at[z])
    ffn = part[x, z].astype(f32) + r1[z].astype(f32)
    for zz in ends:
        arrived(r3.at[zz], z_recv.at[zz])
        ffn = ffn + r3[zz].astype(f32)
    out[...] = (stream + 0.5 * ffn).astype(out.dtype)

    for k in range(size - 1):
        sent(kv_all.at[0], kv_send.at[k])
        sent(info.at[0], in_send.at[k])
    sent(st_out, st_send.at[0])
    sent(sn_out, st_send.at[1])
    sent(st_out, st_send.at[2])
    sent(sn_out, st_send.at[3])
    for zz in range(depth):
        slot = x_all.at[x, zz]
        sent(slot, x_send.at[1, zz])
        sent(r1.at[0], e_send.at[zz])
    for n in range(4):
        sent(x_all.at[0, 0], x_send.at[0, n], None if n < 2 else middle)
    late = wt.at[2:3, mine, :]
    early = wt.at[0:2, mine, :]
    for p in straight + crossed[:1]:
        sent(block, w_send.at[0, p])
    for p in crossed[1:]:
        sent(early, w_send.at[0, p])
        sent(late, w_send.at[1, p])
    for p in [i] + in_turn[:4]:
        for ref in (g_send.at[0, p], f_send.at[0, p], f_send.at[1, p]):
            sent(block, ref)
    for p in in_turn[4:]:
        for ref in (g_send.at[0, p], f_send.at[0, p], f_send.at[1, p]):
            sent(early, ref)
        for ref in (g_send.at[1, p], f_send.at[2, p], f_send.at[3, p]):
            sent(late, ref)
    for k in range(1, members):
        sent(rs.at[0], p_send.at[(j + k) % members])
    for zz in ends:
        sent(s2.at[0], z_send.at[zz])


def fused_shards(*args):
    (res, qn, kn, vn, on, gn, qb, kb, vb, ob, gb, opn, opb, gain, gw, uw, dw) = args
    spread, members = lax.axis_size("sp"), lax.axis_size("tp")
    rows, wide = res.shape
    own, depth = rows // members, spread // 2
    chan, hid = gw.shape
    piece = hid // spread
    kvw = 2 * (kn.shape[1] + kb.shape[1])
    bf16, f32 = jnp.bfloat16, jnp.float32
    state_rows = DH_A + DH_B
    v = pltpu.VMEM
    dma = pltpu.SemaphoreType.DMA
    scratch = [
        v((spread // 2, rows, kvw), bf16),
        v((spread // 2, 2, 16, rows), f32),
        v((2, 16, rows), f32),
        v((3, hid, chan), bf16),
        v((3, members, piece, wide), bf16),
        v((members, own, wide), bf16),
        v((members, own, wide), bf16),
        v((2, depth, own, wide), bf16),
        v((2, depth, own, wide), bf16),
        v((depth, own, wide), bf16),
        v((depth, own, wide), bf16),
        v((depth, own, wide), bf16),
        v((state_rows, 128), bf16),
        v((8, rows), f32),
        v((2, state_rows, 128), bf16),
        v((2, 8, rows), f32),
        dma((spread // 2,)),
        dma((spread // 2,)),
        dma((spread // 2,)),
        dma((spread // 2,)),
        dma((2, spread)),
        dma((2, spread)),
        dma((4, spread)),
        dma((4, spread)),
        dma((2, spread)),
        dma((2, spread)),
        dma((members,)),
        dma((members,)),
        dma((2, depth)),
        dma((2, depth)),
        dma((depth,)),
        dma((depth,)),
        dma((depth,)),
        dma((depth,)),
        dma((4,)),
        dma((2,)),
        dma((2,)),
        dma((17,)),
    ]
    scratch += [v(a.shape, a.dtype) for a in (res, qn, on, gn, qb, ob, gb, opn, opb, gain, gw, uw, dw)]
    geometry = (spread, members, wide, gn.shape[1], gb.shape[1])
    return pl.pallas_call(
        functools.partial(fused_kernel, geometry),
        out_shape=jax.ShapeDtypeStruct((own, wide), bf16),
        in_specs=[pl.BlockSpec(memory_space=pltpu.HBM)] * 17,
        out_specs=pl.BlockSpec(memory_space=pltpu.VMEM),
        scratch_shapes=scratch,
        compiler_params=pltpu.CompilerParams(
            collective_id=0, has_side_effects=True, vmem_limit_bytes=40 * 1024 * 1024
        ),
        name="fused",
    )(*[pltpu.with_memory_space_constraint(a, pltpu.HBM) for a in args])


def pick(*args):
    res, kn, gn, gb, gw = args[0], args[2], args[5], args[10], args[14]
    spread, members = lax.axis_size("sp"), lax.axis_size("tp")
    rows = res.shape[0]
    chan, hid = gw.shape
    fits = (
        spread == 8
        and members == 4
        and rows == 128
        and spread * rows <= 2048
        and chan % 128 == 0
        and hid % (16 * spread) == 0
        and hid % 128 == 0
        and (gn.shape[1], gb.shape[1]) == (2, 1)
        and kn.shape[1] == 2 * DH_A
        and DH_A == 128
        and DH_B == 256
    )
    return fused_shards(*args) if fits else shards(*args)


def solution(mesh):
    in_specs = (
        P("sp", None),
        P("sp", "tp"),
        P("sp", "tp"),
        P("sp", "tp"),
        P("sp", "tp"),
        P(None, "tp", "sp"),
        P("sp", "tp"),
        P("sp", "tp"),
        P("sp", "tp"),
        P("sp", "tp"),
        P(None, "tp", "sp"),
        P("tp", None),
        P("tp", None),
        P(),
        P("sp", "tp"),
        P("sp", "tp"),
        P("sp", "tp"),
    )
    out_specs = P(("sp", "tp"), None)
    return jax.shard_map(pick, mesh=mesh, in_specs=in_specs, out_specs=out_specs, check_vma=False)
```
